256 devices in a mesh: sp: 32 (over z, x), tp: 8 (over y, core).
Axes of the slice: x: 4, y: 4, z: 8, core: 2. Of those that a mesh axis runs over, the one named last changes fastest.
Arguments:
- tokens: bfloat16 [8192, 4096], P('sp', 'tp'), may hold values from -6 to 6
- pre_gain: float32 [4096], replicated, may hold values from 0.1 to 1.9
- rate_factor: float32 [8192], P('sp'), may hold values from 0.5 to 2, as said below
- w_rec_in: bfloat16 [4096, 1024], P(None, 'tp'), may hold values from -0.09375 to 0.09375
- w_rec_gate: bfloat16 [4096, 1024], P(None, 'tp')
- conv_taps: float32 [4, 1024], P(None, 'tp'), may hold values from -3 to 3
- rate_maps: bfloat16 [8, 128, 128], P('tp'), may hold values from -0.5 to 0.5
- input_maps: bfloat16 [8, 128, 128], P('tp'), may hold values from -0.5 to 0.5
- decay_param: float32 [1024], P('tp'), as said below
- w_query: bfloat16 [4096, 1536], P(None, 'tp'), may hold values from -0.09375 to 0.09375
- w_latent: bfloat16 [4096, 512], replicated, may hold values from -0.09375 to 0.09375
- w_rope_key: bfloat16 [4096, 64], replicated, may hold values from -0.09375 to 0.09375
- latent_gain: float32 [512], replicated, may hold values from 0.7 to 100, as said below
- w_expand: bfloat16 [512, 2048], P(None, 'tp')
- rec_gain: float32 [1024], P('tp'), may hold values from 0.1 to 1.9
- att_gain: float32 [1024], P('tp'), may hold values from 0.1 to 1.9
- w_out_rec: bfloat16 [1024, 4096], P('tp'), may hold values from -0.125 to 0.125
- w_out_att: bfloat16 [1024, 4096], P('tp'), may hold values from -0.125 to 0.125
- post_gain: float32 [4096], replicated, may hold values from 0.1 to 1.9
Outputs:
- layer_out: bfloat16 [8192, 4096], P(('sp', 'tp'))
The draws below stay inside these ranges and needn't reach their ends.
Inputs may be any that keep to these rules, and one draw needn't show every extreme that they name: `rate_factor`: one positive factor for each position. `decay_param`: one parameter for each recurrent channel. `latent_gain`: one positive gain for each latent entry.
All inputs are finite; a program needn't handle non-finite values.
Results may differ from the reference program's by a relative error of at most 0.017.
The reference program's roundings to bfloat16 on the way count: a program that leaves them out, or rounds other values in their place, can miss the bound.
Values may be sent and summed in bfloat16 or wider, within the bound.
A program may use at most 128 MiB of HBM per device.

```python
import math
import jax
import jax.numpy as jnp
from jax import lax

D = 4096
LRU_W = 1024
LRU_BLK = 128
CONV = 4
HEADS = 8
NOPE = 128
ROPE = 64
VDIM = 128
LATENT = 512
TOK_DEV = 256
SEQ = 8192
N_TP = 8


def draw_rate_factor(key, part):
    span_rows = max(TOK_DEV // 2, 1)
    levels = jnp.exp(jax.random.uniform(key, (SEQ // span_rows,), jnp.float32, math.log(0.5), math.log(2.0)))
    return jnp.repeat(levels, span_rows, total_repeat_length=SEQ)


def draw_decay_param(key, part):
    choose_key, slow_key, fast_key = jax.random.split(key, 3)
    share = 0.5
    slow_mask = jax.random.uniform(choose_key, (LRU_W,), jnp.float32) < share
    slow_value = math.log(8.0 * SEQ) + jax.random.uniform(slow_key, (LRU_W,), jnp.float32, 0.5, 2.0)
    fast_value = jax.random.uniform(fast_key, (LRU_W,), jnp.float32, 4.5, 6.0)
    return jnp.where(slow_mask, slow_value, fast_value)


def draw_latent_gain(key, part):
    return jax.random.uniform(key, (LATENT,), jnp.float32, 0.7, 1.3)


def draw_w_rec_gate(key, part):
    base_key, factor_key = jax.random.split(key)
    base = jax.random.normal(base_key, (D, LRU_W), jnp.float32) / math.sqrt(D)
    factors = jnp.exp(jax.random.uniform(factor_key, (LRU_W // LRU_BLK,), jnp.float32, math.log(1.0 / 3.0), math.log(3.0)))
    return (base * jnp.repeat(factors, LRU_BLK, total_repeat_length=LRU_W)[None, :]).astype(jnp.bfloat16)


def draw_w_expand(key, part):
    base_key, factor_key = jax.random.split(key)
    base = jax.random.normal(base_key, (LATENT, HEADS, NOPE + VDIM), jnp.float32) / math.sqrt(LATENT)
    factors = jnp.exp(jax.random.uniform(factor_key, (HEADS,), jnp.float32, math.log(1.0 / 3.0), math.log(3.0)))
    columns = jnp.arange(NOPE + VDIM)
    scaling = jnp.where(columns[None, :] >= NOPE, factors[:, None], 1.0)
    return (base * scaling[None, :, :]).reshape(LATENT, HEADS * (NOPE + VDIM)).astype(jnp.bfloat16)


def level_of(own_key, dims, cuts, low, high):
    level = 1.0
    for dim, shards_of in cuts:
        steps = jax.random.uniform(jax.random.fold_in(jax.random.fold_in(own_key, 6), dim), (shards_of,), jnp.float32, low / len(cuts), high / len(cuts))
        level = level * jnp.repeat(jnp.exp(steps), dims[dim] // shards_of).reshape((-1,) + (1,) * (len(dims) - 1 - dim))
    return level


def scatter_about(stream_key, shape, width, reach, shards=(), held_as=jnp.bfloat16):
    drawn = jax.random.normal(stream_key, shape, jnp.float32) * width
    if len(shards) > 0:
        drawn = level_of(stream_key, shape, shards, -0.22, 0.18) * drawn
    return jnp.clip(drawn, min=-reach, max=reach).astype(held_as)


def setup_inputs(seed: int = 0) -> dict:
    key_list = jax.random.split(jax.random.key(seed), 20)
    tokens = scatter_about(key_list[0], (SEQ, D), 1.0, 6.0, ((0, 32), (1, 8)))
    pre_gain = jnp.clip(1.0 + 0.18 * jax.random.normal(key_list[1], (D,), jnp.float32), 0.1, 1.9)
    rate_factor = draw_rate_factor(jax.random.fold_in(key_list[19], 71), 0)
    w_rec_in = scatter_about(key_list[3], (D, LRU_W), D ** -0.5, 0.09375, ((1, 8),))
    w_rec_gate = draw_w_rec_gate(jax.random.fold_in(key_list[19], 71), 0)
    conv_taps = scatter_about(key_list[5], (CONV, LRU_W), 0.5, 3.0, ((1, 8),), jnp.float32)
    rate_maps = scatter_about(key_list[6], (LRU_W // LRU_BLK, LRU_BLK, LRU_BLK), LRU_BLK ** -0.5, 0.5, ((0, 8),))
    input_maps = scatter_about(key_list[7], (LRU_W // LRU_BLK, LRU_BLK, LRU_BLK), LRU_BLK ** -0.5, 0.5, ((0, 8),))
    decay_param = draw_decay_param(jax.random.fold_in(key_list[19], 71), 0)
    w_query = scatter_about(key_list[9], (D, HEADS * (NOPE + ROPE)), D ** -0.5, 0.09375, ((1, 8),))
    w_latent = scatter_about(key_list[10], (D, LATENT), D ** -0.5, 0.09375)
    w_rope_key = scatter_about(key_list[11], (D, ROPE), D ** -0.5, 0.09375)
    latent_gain = draw_latent_gain(jax.random.fold_in(key_list[19], 71), 0)
    w_expand = draw_w_expand(jax.random.fold_in(key_list[19], 71), 0)
    rec_gain = jnp.clip(1.0 + 0.18 * jax.random.normal(key_list[14], (LRU_W,), jnp.float32), 0.1, 1.9)
    att_gain = jnp.clip(1.0 + 0.18 * jax.random.normal(key_list[15], (HEADS * VDIM,), jnp.float32), 0.1, 1.9)
    w_out_rec = scatter_about(key_list[16], (LRU_W, D), (LRU_W + HEADS * VDIM) ** -0.5, 0.125, ((0, 8),))
    w_out_att = scatter_about(key_list[17], (HEADS * VDIM, D), (LRU_W + HEADS * VDIM) ** -0.5, 0.125, ((0, 8),))
    post_gain = jnp.clip(1.0 + 0.18 * jax.random.normal(key_list[18], (D,), jnp.float32), 0.1, 1.9)
    return {"tokens": tokens, "pre_gain": pre_gain, "rate_factor": rate_factor, "w_rec_in": w_rec_in, "w_rec_gate": w_rec_gate, "conv_taps": conv_taps, "rate_maps": rate_maps, "input_maps": input_maps, "decay_param": decay_param, "w_query": w_query, "w_latent": w_latent, "w_rope_key": w_rope_key, "latent_gain": latent_gain, "w_expand": w_expand, "rec_gain": rec_gain, "att_gain": att_gain, "w_out_rec": w_out_rec, "w_out_att": w_out_att, "post_gain": post_gain}


EPS = 1e-06
RATE_C = 8.0
THETA = 10000.0

def rms_inverse(values):
    return lax.rsqrt(lax.optimization_barrier(jnp.mean(values * values, axis=-1, keepdims=True)) + EPS)

def rotate(values, cosine, sine_part):
    half_width = values.shape[-1] // 2
    leading = values[..., :half_width]
    trailing = values[..., half_width:]
    return jnp.concatenate([leading * cosine - trailing * sine_part, trailing * cosine + leading * sine_part], axis=-1)

def angles(length, offset, span_width):
    frequency = 1.0 / THETA ** (jnp.arange(0, span_width, 2).astype(jnp.float32) / span_width)
    places = (offset + jnp.arange(length).astype(jnp.int32)).astype(jnp.float32)
    turned = places[:, None] * frequency[None, :]
    return (jnp.cos(turned), jnp.sin(turned))

def combine_steps(earlier, later):
    return (earlier[0] * later[0], later[0] * earlier[1] + later[1])

def attend_block(state_now, query_nope, query_rope, places, keys_nope, key_rope, values, key_root):
    maxima, totals, accumulated = state_now
    scaling = 1.0 / math.sqrt(query_nope.shape[-1] + query_rope.shape[-1])
    scores = jnp.einsum('qhd,khd->hqk', query_nope.astype(jnp.float32), keys_nope.astype(jnp.float32))
    scores = scores + jnp.einsum('qhd,kd->hqk', query_rope.astype(jnp.float32), key_rope.astype(jnp.float32))
    scores = scores * scaling
    key_places = key_root + jnp.arange(keys_nope.shape[0]).astype(jnp.int32)
    visible = key_places[None, :] <= places[:, None]
    scores = jnp.where(visible[None], scores, -jnp.inf)
    largest = jnp.maximum(maxima, lax.optimization_barrier(jnp.max(scores, axis=-1)))
    anchor = jnp.where(largest == -jnp.inf, 0.0, largest)
    weights = jnp.exp(scores - anchor[..., None])
    shrink = jnp.exp(maxima - anchor)
    totals = totals * shrink + lax.optimization_barrier(jnp.sum(weights, axis=-1))
    rounded = weights.astype(jnp.bfloat16).astype(jnp.float32)
    accumulated = accumulated * shrink[..., None] + jnp.einsum('hqk,khd->hqd', rounded, values.astype(jnp.float32))
    return (largest, totals, accumulated)

def reference(tokens, pre_gain, rate_factor, w_rec_in, w_rec_gate, conv_taps, rate_maps, input_maps, decay_param, w_query, w_latent, w_rope_key, latent_gain, w_expand, rec_gain, att_gain, w_out_rec, w_out_att, post_gain):
    tokens_wide = tokens.astype(jnp.float32)
    inverse = rms_inverse(tokens_wide)
    scaled = (tokens_wide * pre_gain).astype(jnp.bfloat16)

    def project(weight):
        return inverse * jnp.dot(scaled, weight, preferred_element_type=jnp.float32)
    rec_input = project(w_rec_in).astype(jnp.bfloat16)
    gate_value = project(w_rec_gate)
    query_raw = project(w_query)
    latent_raw = project(w_latent)
    rope_raw = project(w_rope_key)
    padded = jnp.concatenate([jnp.zeros((CONV - 1, LRU_W), jnp.bfloat16), rec_input], axis=0)
    convolved = conv_taps[0] * padded[0:SEQ].astype(jnp.float32)
    for tap_index in range(1, CONV):
        convolved = convolved + conv_taps[tap_index] * padded[tap_index:tap_index + SEQ].astype(jnp.float32)
    conv_low = lax.optimization_barrier(convolved.astype(jnp.bfloat16)).astype(jnp.float32)
    blocks = conv_low.reshape(SEQ, LRU_W // LRU_BLK, LRU_BLK)
    rate_gate = jax.nn.sigmoid(jnp.einsum('sbi,bij->sbj', blocks, rate_maps.astype(jnp.float32))).reshape(SEQ, LRU_W)
    entry_gate = jax.nn.sigmoid(jnp.einsum('sbi,bij->sbj', blocks, input_maps.astype(jnp.float32))).reshape(SEQ, LRU_W)
    log_keep = -RATE_C * rate_factor[:, None] * rate_gate * jax.nn.softplus(-decay_param)
    keep_rate = jnp.exp(log_keep)
    driven = jnp.sqrt(-jnp.expm1(2.0 * log_keep)) * entry_gate * convolved
    state_seq = lax.associative_scan(combine_steps, (keep_rate, driven), axis=0)[1]
    rec_out = state_seq * jax.nn.gelu(gate_value)
    rec_norm = (rec_out * rms_inverse(rec_out) * rec_gain).astype(jnp.bfloat16)
    cosine, sine_part = angles(SEQ, 0, ROPE)
    query_heads = query_raw.reshape(SEQ, HEADS, NOPE + ROPE)
    query_nope = query_heads[:, :, :NOPE].astype(jnp.bfloat16)
    query_rope = rotate(query_heads[:, :, NOPE:], cosine[:, None, :], sine_part[:, None, :]).astype(jnp.bfloat16)
    latent_norm = (latent_raw * rms_inverse(latent_raw) * latent_gain).astype(jnp.bfloat16)
    rope_key = rotate(rope_raw, cosine, sine_part).astype(jnp.bfloat16)
    expanded = jnp.dot(latent_norm, w_expand, preferred_element_type=jnp.float32).astype(jnp.bfloat16)
    expanded = expanded.reshape(SEQ, HEADS, NOPE + VDIM)
    keys_nope = expanded[:, :, :NOPE]
    values = expanded[:, :, NOPE:]
    query_span = math.gcd(SEQ, 256)
    block_count = SEQ // query_span

    def one_block(block_index):
        root = block_index * query_span
        block_nope = lax.dynamic_slice_in_dim(query_nope, root, query_span, 0)
        block_rope = lax.dynamic_slice_in_dim(query_rope, root, query_span, 0)
        places = root + jnp.arange(query_span).astype(jnp.int32)
        initial = (jnp.full((HEADS, query_span), -jnp.inf, jnp.float32), jnp.zeros((HEADS, query_span), jnp.float32), jnp.zeros((HEADS, query_span, VDIM), jnp.float32))
        maxima, totals, accumulated = attend_block(initial, block_nope, block_rope, places, keys_nope, rope_key, values, 0)
        return (accumulated / totals[..., None]).transpose(1, 0, 2)
    att_out = lax.map(one_block, jnp.arange(block_count).astype(jnp.int32)).reshape(SEQ, HEADS * VDIM)
    att_norm = (att_out * rms_inverse(att_out) * att_gain).astype(jnp.bfloat16)
    rec_width = LRU_W // N_TP
    att_width = HEADS * VDIM // N_TP
    mixed_sum = jnp.zeros((SEQ, D), jnp.float32)
    for member in range(N_TP):
        partial_value = jnp.dot(rec_norm[:, member * rec_width:(member + 1) * rec_width], w_out_rec[member * rec_width:(member + 1) * rec_width], preferred_element_type=jnp.float32)
        partial_value = partial_value + jnp.dot(att_norm[:, member * att_width:(member + 1) * att_width], w_out_att[member * att_width:(member + 1) * att_width], preferred_element_type=jnp.float32)
        mixed_sum = mixed_sum + lax.optimization_barrier(partial_value.astype(jnp.bfloat16)).astype(jnp.float32)
    return (mixed_sum * rms_inverse(mixed_sum) * post_gain).astype(jnp.bfloat16)
```

```python
import functools
import math

import jax
import jax.numpy as jnp
from jax import lax
from jax.experimental import pallas as pl
from jax.experimental.pallas import tpu as pltpu
from jax.sharding import PartitionSpec as P

NOPE = 128
ROPE = 64
VDIM = 128
EPS = 1e-06
RATE_C = 8.0
THETA = 10000.0
NY, NX, NZ = 4, 4, 8
MESH = pl.DeviceIdType.MESH
F32, BF16 = jnp.float32, jnp.bfloat16
VM = pl.BlockSpec(memory_space=pltpu.VMEM)
ANY = pl.BlockSpec(memory_space=pl.ANY)


def remote(src, dst, send, recv, where):
    return pltpu.make_async_remote_copy(
        src_ref=src, dst_ref=dst, send_sem=send, recv_sem=recv, device_id=where, device_id_type=MESH
    )


def greet(partners):
    barrier = pltpu.get_barrier_semaphore()
    for where in partners:
        pl.semaphore_signal(barrier, inc=1, device_id=where, device_id_type=MESH)
    pl.semaphore_wait(barrier, len(partners))


def mm(a, b):
    return jnp.dot(a, b, preferred_element_type=F32)


def kernel_a(
    tok_ref, gain_ref, w_in, w_gate, w_q, w_lat, w_rope, lat_gain, w_exp, cos_ref, sin_ref,
    q_out, kv_out, rec_out, gate_out,
    tok, v_ig, v_q, v_lat, v_rope, v_exp, a_ig, a_q, a_lat, a_rope, sq,
    wsem, ssem, rsem,
):
    tp = lax.axis_index("tp")
    y, c = tp // 2, tp % 2
    sib = y * 2 + 1 - c
    up = ((y + 1) % NY) * 2 + c
    dn = ((y + 3) % NY) * 2 + c
    far = ((y + 2) % NY) * 2 + c
    rows = tok_ref.shape[0]
    half = rows // 2
    depth = tok_ref.shape[1]
    model = depth * 2 * NY

    loads = [
        pltpu.make_async_copy(w_in, v_ig.at[:, pl.ds(0, 128)], wsem.at[0]),
        pltpu.make_async_copy(w_gate, v_ig.at[:, pl.ds(128, 128)], wsem.at[1]),
        pltpu.make_async_copy(w_q, v_q, wsem.at[2]),
        pltpu.make_async_copy(w_lat, v_lat, wsem.at[3]),
        pltpu.make_async_copy(w_rope, v_rope, wsem.at[4]),
        pltpu.make_async_copy(w_exp, v_exp, wsem.at[5]),
    ]
    for load in loads:
        load.start()
    greet([{"tp": sib}, {"tp": up}, {"tp": dn}])

    h0, h1 = pl.ds(0, half), pl.ds(half, half)

    def msg(k, src, slot, part, where):
        return remote(src, tok.at[slot, part], ssem.at[k], rsem.at[k], {"tp": where})

    sent = []

    def send(k, src, slot, part, where):
        copy = msg(k, src, slot, part, where)
        copy.start()
        sent.append(copy)

    def arrived(k, slot, part):
        msg(k, tok.at[slot, part], slot, part, sib).wait_recv()

    def own(part):
        return tok_ref.at[part]

    send(1, own(h0), tp, h0, up)
    send(3, own(h1), tp, h1, dn)
    send(0, tok_ref, tp, pl.ds(0, rows), sib)
    send(2, own(h1), tp, h1, up)
    send(4, own(h0), tp, h0, dn)

    def chunk(block, source, first):
        wide = block.astype(F32)
        square = wide * wide
        folded = square[:, 0:128]
        for k in range(1, depth // 128):
            folded = folded + square[:, k * 128 : (k + 1) * 128]
        at = pl.ds(pl.multiple_of(source * depth, depth), depth)
        low = (wide * gain_ref[:, at]).astype(BF16)
        parts = ((a_ig, v_ig), (a_q, v_q), (a_lat, v_lat), (a_rope, v_rope))
        if first:
            sq[...] = folded
            for acc, weight in parts:
                acc[...] = mm(low, weight[at, :])
        else:
            sq[...] += folded
            for acc, weight in parts:
                acc[...] += mm(low, weight[at, :])

    for load in loads[:5]:
        load.wait()
    chunk(tok_ref[...], tp, True)
    arrived(0, sib, pl.ds(0, rows))
    chunk(tok[sib], sib, False)

    arrived(1, dn, h0)
    send(5, tok.at[dn, h0], dn, h0, up)
    send(7, tok.at[dn, h0], dn, h0, sib)
    arrived(3, up, h1)
    send(6, tok.at[up, h1], up, h1, dn)
    send(9, tok.at[up, h1], up, h1, sib)
    arrived(2, dn, h1)
    send(8, tok.at[dn, h1], dn, h1, sib)
    arrived(4, up, h0)
    send(10, tok.at[up, h0], up, h0, sib)
    chunk(tok[dn], dn, False)
    chunk(tok[up], up, False)
    dn_sib = ((y + 3) % NY) * 2 + 1 - c
    up_sib = ((y + 1) % NY) * 2 + 1 - c
    far_sib = ((y + 2) % NY) * 2 + 1 - c
    arrived(7, dn_sib, h0)
    arrived(8, dn_sib, h1)
    chunk(tok[dn_sib], dn_sib, False)
    arrived(9, up_sib, h1)
    arrived(10, up_sib, h0)
    chunk(tok[up_sib], up_sib, False)
    arrived(5, far, h0)
    send(11, tok.at[far, h0], far, h0, sib)
    arrived(6, far, h1)
    send(12, tok.at[far, h1], far, h1, sib)
    chunk(tok[far], far, False)
    arrived(11, far_sib, h0)
    arrived(12, far_sib, h1)
    chunk(tok[far_sib], far_sib, False)
    loads[5].wait()

    inverse = lax.rsqrt(jnp.sum(sq[...], axis=1, keepdims=True) / model + EPS)
    latent = inverse * a_lat[...]
    spread = lax.rsqrt(jnp.mean(latent * latent, axis=1, keepdims=True) + EPS)
    latent = (latent * spread * lat_gain[...]).astype(BF16)
    expanded = mm(latent, v_exp[...]).T
    kv_out[0:NOPE, :] = expanded[0:NOPE].astype(BF16)
    kv_out[NOPE + ROPE :, :] = expanded[NOPE:].astype(BF16)
    query = inverse * a_q[...]
    turned = jnp.concatenate([query[:, NOPE:], inverse * a_rope[...]], axis=1).T
    cosine, sine = cos_ref[...], sin_ref[...]
    hr = ROPE // 2
    u, w = turned[0:hr], turned[hr:ROPE]
    q_out[0:NOPE, :] = query[:, 0:NOPE].T.astype(BF16)
    q_out[NOPE : NOPE + hr, :] = (u * cosine - w * sine).astype(BF16)
    q_out[NOPE + hr :, :] = (w * cosine + u * sine).astype(BF16)
    u, w = turned[ROPE : ROPE + hr], turned[ROPE + hr :]
    kv_out[NOPE : NOPE + hr, :] = (u * cosine - w * sine).astype(BF16)
    kv_out[NOPE + hr : NOPE + ROPE, :] = (w * cosine + u * sine).astype(BF16)
    ig = inverse * a_ig[...]
    rec_out[...] = ig[:, 0:128].astype(BF16)
    gate_out[...] = ig[:, 128:256]
    for copy in sent:
        copy.wait_send()


def call_a(tokens, pre_gain, w_in, w_gate, w_q, w_lat, w_rope, lat_gain, w_exp, cosine, sine):
    rows, depth = tokens.shape
    model = w_in.shape[0]
    return pl.pallas_call(
        kernel_a,
        name="gather_project",
        out_shape=(
            jax.ShapeDtypeStruct((NOPE + ROPE, rows), BF16),
            jax.ShapeDtypeStruct((NOPE + ROPE + VDIM, rows), BF16),
            jax.ShapeDtypeStruct((rows, 128), BF16),
            jax.ShapeDtypeStruct((rows, 128), F32),
        ),
        in_specs=[VM, VM, ANY, ANY, ANY, ANY, ANY, VM, ANY, VM, VM],
        out_specs=(VM, VM, VM, VM),
        scratch_shapes=[
            pltpu.VMEM((2 * NY, rows, depth), BF16),
            pltpu.VMEM((model, 256), BF16),
            pltpu.VMEM((model, NOPE + ROPE), BF16),
            pltpu.VMEM((model, 512), BF16),
            pltpu.VMEM((model, ROPE), BF16),
            pltpu.VMEM((512, NOPE + VDIM), BF16),
            pltpu.VMEM((rows, 256), F32),
            pltpu.VMEM((rows, NOPE + ROPE), F32),
            pltpu.VMEM((rows, 512), F32),
            pltpu.VMEM((rows, ROPE), F32),
            pltpu.VMEM((rows, 128), F32),
            pltpu.SemaphoreType.DMA((6,)),
            pltpu.SemaphoreType.DMA((13,)),
            pltpu.SemaphoreType.DMA((13,)),
        ],
        compiler_params=pltpu.CompilerParams(
            collective_id=0, has_side_effects=True, vmem_limit_bytes=48 * 1024 * 1024
        ),
    )(tokens, pre_gain, w_in, w_gate, w_q, w_lat, w_rope, lat_gain, w_exp, cosine, sine)


def shifted(values, by, fill):
    row = lax.broadcasted_iota(jnp.int32, values.shape, 0)
    return jnp.where(row < by, fill, pltpu.roll(values, by, 0))


def minus_expm1(x):
    series = 1.0 + x * (1.0 / 7.0)
    for n in (6.0, 5.0, 4.0, 3.0, 2.0):
        series = 1.0 + (x * (1.0 / n)) * series
    return jnp.where(x > -0.25, -x * series, 1.0 - jnp.exp(x))


def softplus(x):
    small = jnp.exp(-jnp.abs(x))
    t = small / (2.0 + small)
    t2 = t * t
    series = 1.0 / 17.0
    for n in (15.0, 13.0, 11.0, 9.0, 7.0, 5.0, 3.0, 1.0):
        series = 1.0 / n + t2 * series
    return jnp.maximum(x, 0.0) + 2.0 * t * series


def kernel_b(
    q_ref, kv_ref, rec_ref, gate_ref, rf_ref, taps_ref, rmap_ref, imap_ref, decay_ref,
    rec_t, att_t, sums,
    kv, kn, qs, halo, ext, m_s, l_s, o_s, cum_s, loc_s, cx, cz, mine_x, mine_z, po, ps, go, gs,
    kss, krs, qss, qrs, hsem, xss, xrs, zss, zrs, oss, ors, tss, trs,
):
    sp = lax.axis_index("sp")
    z, x = sp // NX, sp % NX
    keys = q_ref.shape[1]

    def at_zx(zz, xx):
        return {"sp": zz * NX + xx}

    zup, zdn = (z + 1) % NZ, (z + NZ - 1) % NZ
    succ = (sp + 1) % (NX * NZ)
    pred = (sp + NX * NZ - 1) % (NX * NZ)
    xs_other = [(x + d) % NX for d in range(1, NX)]
    zs_other = [(z + d) % NZ for d in range(1, NZ)]
    greet(
        [at_zx(z, xx) for xx in xs_other]
        + [at_zx(zz, x) for zz in zs_other]
        + [{"sp": succ}, {"sp": pred}]
    )
    sent = []

    def go_send(copy):
        copy.start()
        sent.append(copy)

    kpart, vpart = pl.ds(0, NOPE + ROPE), pl.ds(NOPE + ROPE, VDIM)
    parts = (kpart, vpart)

    def kv_msg(src, slot, part, k, where_z):
        return remote(src, kv.at[slot, parts[part]], kss.at[k], krs.at[k], at_zx(where_z, x))

    def kid(direction, hop, part):
        return direction * 8 + (hop - 1) * 2 + part

    go_send(kv_msg(kv_ref.at[kpart], z, 0, kid(0, 1, 0), zup))
    go_send(kv_msg(kv_ref.at[kpart], z, 0, kid(1, 1, 0), zdn))
    go_send(kv_msg(kv_ref.at[vpart], z, 1, kid(0, 1, 1), zup))
    go_send(kv_msg(kv_ref.at[vpart], z, 1, kid(1, 1, 1), zdn))
    tail = rec_ref.shape[0] - 16
    go_send(remote(rec_ref.at[pl.ds(tail, 16)], halo, hsem.at[0], hsem.at[1], {"sp": succ}))
    for d in range(1, NX):
        go_send(remote(q_ref, qs.at[x], qss.at[d - 1], qrs.at[d - 1], at_zx(z, (x + d) % NX)))

    scale = math.log2(math.e) / math.sqrt(NOPE + ROPE)
    low = -1e30

    def begin(slot):
        m_s[slot] = jnp.full((1, keys), low, F32)
        l_s[slot] = jnp.zeros((1, keys), F32)
        o_s[slot] = jnp.zeros((VDIM, keys), F32)

    for xx in range(NX):
        begin(xx)

    def attend(slot, queries, values, masked):
        scores = mm(kn[...], queries) * scale
        if masked:
            key = lax.broadcasted_iota(jnp.int32, scores.shape, 0)
            place = lax.broadcasted_iota(jnp.int32, scores.shape, 1)
            scores = jnp.where(key <= place, scores, low)
        before = m_s[slot]
        largest = jnp.maximum(before, jnp.max(scores, axis=0, keepdims=True))
        weights = jnp.exp2(scores - largest)
        shrink = jnp.exp2(before - largest)
        m_s[slot] = largest
        l_s[slot] = l_s[slot] * shrink + jnp.sum(weights, axis=0, keepdims=True)
        o_s[slot] = o_s[slot] * shrink + mm(values, weights.astype(BF16))

    kn[...] = kv_ref[kpart, :].T
    attend(x, q_ref[...], kv_ref[vpart, :], True)

    remote(halo, halo, hsem.at[0], hsem.at[1], {"sp": succ}).wait_recv()
    first = sp == 0
    rows = rec_ref.shape[0]
    ext[0:16, :] = jnp.where(first, 0.0, halo[...].astype(F32))
    ext[16:, :] = rec_ref[...].astype(F32)
    convolved = taps_ref[0:1, :] * ext[13 : 13 + rows, :]
    for k in range(1, 4):
        convolved = convolved + taps_ref[k : k + 1, :] * ext[13 + k : 13 + k + rows, :]
    conv_low = convolved.astype(BF16)
    rate = jax.nn.sigmoid(mm(conv_low, rmap_ref[...]))
    entry = jax.nn.sigmoid(mm(conv_low, imap_ref[...]))
    factor = jnp.broadcast_to(rf_ref[...], (128, rows)).T
    log_keep = (-RATE_C) * factor * rate * softplus(-decay_ref[...])
    cum = jnp.exp(log_keep)
    local = jnp.sqrt(minus_expm1(2.0 * log_keep)) * entry * convolved
    step = 1
    while step < rows:
        local = local + cum * shifted(local, step, 0.0)
        cum = cum * shifted(cum, step, 1.0)
        step *= 2
    cum_s[...] = cum
    loc_s[...] = local
    mine_x[0:1, :] = cum[rows - 1 :]
    mine_x[1:2, :] = local[rows - 1 :]
    for d in range(1, NX):
        go_send(remote(mine_x, cx.at[x], xss.at[d - 1], xrs.at[d - 1], at_zx(z, (x + d) % NX)))

    def got(slot, part, k):
        kv_msg(kv.at[slot, parts[part]], slot, part, k, zup).wait_recv()

    def take_hop(hop):
        below, above = (z + NZ - hop) % NZ, (z + hop) % NZ
        for part in (0, 1):
            for direction, slot, to in ((0, below, zup), (1, above, zdn)):
                if hop == 4 and direction != part:
                    continue
                got(slot, part, kid(direction, hop, part))
                if hop < 3 or (hop == 3 and direction == part):
                    go_send(kv_msg(kv.at[slot, parts[part]], slot, part, kid(direction, hop + 1, part), to))
        return below, above

    def against(slot):
        kn[...] = kv[slot, 0 : NOPE + ROPE, :].T

        def one(i, carry):
            xx = (x + i) % NX
            attend(xx, qs[xx], kv[slot, NOPE + ROPE :, :], False)
            return carry

        lax.fori_loop(0, NX, one, 0)

    def hop_work(hop):
        below, above = take_hop(hop)
        return below, above

    qs[x] = q_ref[...]
    for d in range(1, NX):
        remote(q_ref, qs.at[(x + NX - d) % NX], qss.at[d - 1], qrs.at[d - 1], at_zx(z, x)).wait_recv()
    for d in range(1, NX):

        @pl.when(x + d < NX)
        def _():
            attend(x + d, qs[jnp.minimum(x + d, NX - 1)], kv_ref[vpart, :], False)

    for hop in range(1, 5):
        below, above = take_hop(hop)

        @pl.when(below < z)
        def _():
            against(below)

        if hop < 4:

            @pl.when(above < z)
            def _():
                against(above)

        if hop == 1:
            cx[x] = mine_x[...]
            for d in range(1, NX):
                remote(mine_x, cx.at[(x + NX - d) % NX], xss.at[d - 1], xrs.at[d - 1], at_zx(z, x)).wait_recv()
            pa, pb = jnp.ones((1, 128), F32), jnp.zeros((1, 128), F32)
            ta, tb = pa, pb
            for i in range(NX):
                a, b = cx[i, 0:1, :], cx[i, 1:2, :]
                ta, tb = ta * a, a * tb + b
                pa = jnp.where(i < x, pa * a, pa)
                pb = jnp.where(i < x, a * pb + b, pb)
            mine_z[0:1, :] = ta
            mine_z[1:2, :] = tb
            for d in range(1, NZ):
                go_send(remote(mine_z, cz.at[z], zss.at[d - 1], zrs.at[d - 1], at_zx((z + d) % NZ, x)))
        if hop == 3:
            cz[z] = mine_z[...]
            for d in range(1, NZ):
                remote(mine_z, cz.at[(z + NZ - d) % NZ], zss.at[d - 1], zrs.at[d - 1], at_zx(z, x)).wait_recv()
            entering = jnp.zeros((1, 128), F32)
            for i in range(NZ):
                entering = jnp.where(i < z, cz[i, 0:1, :] * entering + cz[i, 1:2, :], entering)
            entering = pa * entering + pb
            state = loc_s[...] + cum_s[...] * entering
            turned = (state * jax.nn.gelu(gate_ref[...])).T
            rec_t[...] = turned
            sums[0:1, :] = jnp.sum(turned * turned, axis=0, keepdims=True)

    for d in range(1, NX):
        xx = (x + d) % NX
        total = l_s[xx]
        po[d - 1] = (o_s[xx] / jnp.where(total > 0.0, total, 1.0)).astype(BF16)
        ps[d - 1, 0:1, :] = m_s[xx]
        ps[d - 1, 1:2, :] = total
        go_send(remote(po.at[d - 1], go.at[d - 1], oss.at[d - 1], ors.at[d - 1], at_zx(z, xx)))
        go_send(remote(ps.at[d - 1], gs.at[d - 1], tss.at[d - 1], trs.at[d - 1], at_zx(z, xx)))
    largest = m_s[x]
    for d in range(1, NX):
        remote(ps.at[d - 1], gs.at[d - 1], tss.at[d - 1], trs.at[d - 1], at_zx(z, x)).wait_recv()
        largest = jnp.maximum(largest, gs[d - 1, 0:1, :])
    share = jnp.exp2(m_s[x] - largest)
    total = l_s[x] * share
    out = o_s[x] * share
    for d in range(1, NX):
        remote(po.at[d - 1], go.at[d - 1], oss.at[d - 1], ors.at[d - 1], at_zx(z, x)).wait_recv()
        share = gs[d - 1, 1:2, :] * jnp.exp2(gs[d - 1, 0:1, :] - largest)
        total = total + share
        out = out + go[d - 1].astype(F32) * share
    out = out / total
    att_t[...] = out
    sums[1:2, :] = jnp.sum(out * out, axis=0, keepdims=True)
    for copy in sent:
        copy.wait_send()


def call_b(q, kv, rec, gate, rf, taps, rmap, imap, decay):
    keys = q.shape[1]
    dma = pltpu.SemaphoreType.DMA
    return pl.pallas_call(
        kernel_b,
        name="attend_recur",
        out_shape=(
            jax.ShapeDtypeStruct((128, keys), F32),
            jax.ShapeDtypeStruct((VDIM, keys), F32),
            jax.ShapeDtypeStruct((2, keys), F32),
        ),
        in_specs=[VM] * 9,
        out_specs=(VM, VM, VM),
        scratch_shapes=[
            pltpu.VMEM((NZ, NOPE + ROPE + VDIM, keys), BF16),
            pltpu.VMEM((keys, NOPE + ROPE), BF16),
            pltpu.VMEM((NX, NOPE + ROPE, keys), BF16),
            pltpu.VMEM((16, 128), BF16),
            pltpu.VMEM((16 + keys, 128), F32),
            pltpu.VMEM((NX, 1, keys), F32),
            pltpu.VMEM((NX, 1, keys), F32),
            pltpu.VMEM((NX, VDIM, keys), F32),
            pltpu.VMEM((keys, 128), F32),
            pltpu.VMEM((keys, 128), F32),
            pltpu.VMEM((NX, 2, 128), F32),
            pltpu.VMEM((NZ, 2, 128), F32),
            pltpu.VMEM((2, 128), F32),
            pltpu.VMEM((2, 128), F32),
            pltpu.VMEM((NX - 1, VDIM, keys), BF16),
            pltpu.VMEM((NX - 1, 2, keys), F32),
            pltpu.VMEM((NX - 1, VDIM, keys), BF16),
            pltpu.VMEM((NX - 1, 2, keys), F32),
            dma((16,)), dma((16,)),
            dma((NX - 1,)), dma((NX - 1,)),
            dma((2,)),
            dma((NX - 1,)), dma((NX - 1,)),
            dma((NZ - 1,)), dma((NZ - 1,)),
            dma((NX - 1,)), dma((NX - 1,)),
            dma((NX - 1,)), dma((NX - 1,)),
        ],
        compiler_params=pltpu.CompilerParams(
            collective_id=1, has_side_effects=True, vmem_limit_bytes=32 * 1024 * 1024
        ),
    )(q, kv, rec, gate, rf, taps, rmap, imap, decay)


def kernel_c(
    rec_t, att_t, sums, rgain, again, w_rec, w_att, post,
    out_ref,
    got_s, act, w, pair_out, pair_in, part, f_out, f_in, n_out, n_in,
    wsem, sss, srs, pss, prs, fss, frs, nss, nrs,
):
    tp = lax.axis_index("tp")
    y, c = tp // 2, tp % 2
    sib = y * 2 + 1 - c
    up = ((y + 1) % NY) * 2 + c
    dn = ((y + 3) % NY) * 2 + c
    model = w.shape[1]
    rows = out_ref.shape[0]
    half = model // 2
    loads = [
        pltpu.make_async_copy(w_rec, w.at[pl.ds(0, 128)], wsem.at[0]),
        pltpu.make_async_copy(w_att, w.at[pl.ds(128, 128)], wsem.at[1]),
    ]
    for load in loads:
        load.start()
    n = 2 * NY
    greet([{"tp": (tp + d) % n} for d in range(1, n)])
    sent = []

    def go_send(copy):
        copy.start()
        sent.append(copy)

    for d in range(1, n):
        go_send(remote(sums, got_s.at[d - 1], sss.at[d - 1], srs.at[d - 1], {"tp": (tp + d) % n}))
    total = sums[...]
    for d in range(1, n):
        remote(sums, got_s.at[d - 1], sss.at[d - 1], srs.at[d - 1], {"tp": sib}).wait_recv()
        total = total + got_s[d - 1]
    inverse = lax.rsqrt(total / (128 * n) + EPS)
    act[:, 0:128] = ((rec_t[...] * inverse[0:1, :]).T * rgain[...]).astype(BF16)
    act[:, 128:256] = ((att_t[...] * inverse[1:2, :]).T * again[...]).astype(BF16)
    for load in loads:
        load.wait()

    order = [(y + 2) % NY, (y + 1) % NY, (y + 3) % NY, y]
    for k, yy in enumerate(order):
        block = act[pl.ds(pl.multiple_of(yy * 2 * rows + (1 - c) * rows, rows), rows), :]
        pair_out[k] = mm(block, w[...]).astype(BF16)
        go_send(remote(pair_out.at[k], pair_in.at[k], pss.at[k], prs.at[k], {"tp": sib}))

    def chip_sum(k):
        yy = order[k]
        block = act[pl.ds(pl.multiple_of(yy * 2 * rows + c * rows, rows), rows), :]
        value = mm(block, w[...])
        remote(pair_out.at[k], pair_in.at[k], pss.at[k], prs.at[k], {"tp": sib}).wait_recv()
        return value + pair_in[k].astype(F32)

    f_out[...] = chip_sum(0).astype(BF16)
    left, right = pl.ds(0, half), pl.ds(half, half)
    go_send(remote(f_out.at[:, left], f_in.at[:, left], fss.at[0], frs.at[0], {"tp": up}))
    go_send(remote(f_out.at[:, right], f_in.at[:, right], fss.at[1], frs.at[1], {"tp": dn}))
    part[0] = chip_sum(1)
    n_out[0, :, half:] = part[0, :, half:].astype(BF16)
    go_send(remote(n_out.at[0, :, right], n_in.at[0, :, right], nss.at[0], nrs.at[0], {"tp": up}))
    part[1] = chip_sum(2)
    n_out[1, :, 0:half] = part[1, :, 0:half].astype(BF16)
    go_send(remote(n_out.at[1, :, left], n_in.at[1, :, left], nss.at[1], nrs.at[1], {"tp": dn}))
    own = chip_sum(3)
    remote(f_out.at[:, left], f_in.at[:, left], fss.at[0], frs.at[0], {"tp": up}).wait_recv()
    n_out[0, :, 0:half] = (part[0, :, 0:half] + f_in[:, 0:half].astype(F32)).astype(BF16)
    go_send(remote(n_out.at[0, :, left], n_in.at[0, :, left], nss.at[2], nrs.at[2], {"tp": up}))
    remote(f_out.at[:, right], f_in.at[:, right], fss.at[1], frs.at[1], {"tp": dn}).wait_recv()
    n_out[1, :, half:] = (part[1, :, half:] + f_in[:, half:].astype(F32)).astype(BF16)
    go_send(remote(n_out.at[1, :, right], n_in.at[1, :, right], nss.at[3], nrs.at[3], {"tp": dn}))
    part[0] = own
    for k, (side, cols) in enumerate(((0, right), (1, left), (0, left), (1, right))):
        remote(n_out.at[side, :, cols], n_in.at[side, :, cols], nss.at[k], nrs.at[k], {"tp": up}).wait_recv()
    mixed = part[0] + n_in[0].astype(F32) + n_in[1].astype(F32)
    spread = lax.rsqrt(jnp.mean(mixed * mixed, axis=1, keepdims=True) + EPS)
    out_ref[...] = (mixed * spread * post[...]).astype(BF16)
    for copy in sent:
        copy.wait_send()


def call_c(rec_t, att_t, sums, rgain, again, w_rec, w_att, post):
    keys = rec_t.shape[1]
    n = 2 * NY
    rows = keys // n
    model = w_rec.shape[1]
    dma = pltpu.SemaphoreType.DMA
    return pl.pallas_call(
        kernel_c,
        name="project_out",
        out_shape=jax.ShapeDtypeStruct((rows, model), BF16),
        in_specs=[VM, VM, VM, VM, VM, ANY, ANY, VM],
        out_specs=VM,
        scratch_shapes=[
            pltpu.VMEM((n - 1, 2, keys), F32),
            pltpu.VMEM((keys, 256), BF16),
            pltpu.VMEM((256, model), BF16),
            pltpu.VMEM((NY, rows, model), BF16),
            pltpu.VMEM((NY, rows, model), BF16),
            pltpu.VMEM((2, rows, model), F32),
            pltpu.VMEM((rows, model), BF16),
            pltpu.VMEM((rows, model), BF16),
            pltpu.VMEM((2, rows, model), BF16),
            pltpu.VMEM((2, rows, model), BF16),
            dma((2,)),
            dma((n - 1,)), dma((n - 1,)),
            dma((NY,)), dma((NY,)),
            dma((2,)), dma((2,)),
            dma((4,)), dma((4,)),
        ],
        compiler_params=pltpu.CompilerParams(
            collective_id=2, has_side_effects=True, vmem_limit_bytes=32 * 1024 * 1024
        ),
    )(rec_t, att_t, sums, rgain, again, w_rec, w_att, post)


def shards(
    tokens, pre_gain, rate_factor, w_rec_in, w_rec_gate, conv_taps, rate_maps, input_maps,
    decay_param, w_query, w_latent, w_rope_key, latent_gain, w_expand, rec_gain, att_gain,
    w_out_rec, w_out_att, post_gain,
):
    rows = tokens.shape[0]
    frequency = 1.0 / THETA ** (jnp.arange(0, ROPE, 2).astype(F32) / ROPE)
    places = (lax.axis_index("sp") * rows + jnp.arange(rows)).astype(F32)
    turned = places[None, :] * frequency[:, None]
    cosine, sine = jnp.cos(turned), jnp.sin(turned)
    q, kv, rec, gate = call_a(
        tokens, pre_gain[None], w_rec_in, w_rec_gate, w_query, w_latent, w_rope_key,
        latent_gain[None], w_expand, cosine, sine,
    )
    rec_t, att_t, sums = call_b(
        q, kv, rec, gate, rate_factor[None], conv_taps, rate_maps[0], input_maps[0], decay_param[None]
    )
    return call_c(
        rec_t, att_t, sums, rec_gain[None], att_gain[None], w_out_rec, w_out_att, post_gain[None]
    )


def solution(mesh):
    placed = (
        P("sp", "tp"), P(), P("sp"), P(None, "tp"), P(None, "tp"), P(None, "tp"),
        P("tp", None, None), P("tp", None, None), P("tp"), P(None, "tp"), P(), P(), P(),
        P(None, "tp"), P("tp"), P("tp"), P("tp", None), P("tp", None), P(),
    )
    return jax.shard_map(
        shards, mesh=mesh, in_specs=placed, out_specs=P(("sp", "tp"), None), check_vma=False
    )
```

```python
import math

import jax
import jax.numpy as jnp
from jax import lax
from jax.experimental import pallas as pl
from jax.experimental.pallas import tpu as pltpu
from jax.sharding import PartitionSpec as P

NOPE = 128
ROPE = 64
VDIM = 128
EPS = 1e-06
RATE_C = 8.0
THETA = 10000.0
NY, NX, NZ = 4, 4, 8
NT = 2 * NY
PIECES = 4
LOW = -1e30
MESH = pl.DeviceIdType.MESH
F32, BF16 = jnp.float32, jnp.bfloat16
QK = NOPE + ROPE


def remote(src, dst, send, recv, where):
    return pltpu.make_async_remote_copy(
        src_ref=src, dst_ref=dst, send_sem=send, recv_sem=recv, device_id=where, device_id_type=MESH
    )


def greet(partners):
    barrier = pltpu.get_barrier_semaphore()
    for where in partners:
        pl.semaphore_signal(barrier, inc=1, device_id=where, device_id_type=MESH)
    pl.semaphore_wait(barrier, len(partners))


def hello(sem, where):
    pl.semaphore_signal(sem, inc=1, device_id=where, device_id_type=MESH)


def mm(a, b):
    return jnp.dot(a, b, preferred_element_type=F32)


def mm_t(a, b):
    return lax.dot_general(a, b, (((1,), (1,)), ((), ())), preferred_element_type=F32)


def shifted(values, by, fill):
    row = lax.broadcasted_iota(jnp.int32, values.shape, 0)
    return jnp.where(row < by, fill, pltpu.roll(values, by, 0))


def minus_expm1(x):
    series = 1.0 + x * (1.0 / 7.0)
    for n in (6.0, 5.0, 4.0, 3.0, 2.0):
        series = 1.0 + (x * (1.0 / n)) * series
    return jnp.where(x > -0.25, -x * series, 1.0 - jnp.exp(x))


def softplus(x):
    small = jnp.exp(-jnp.abs(x))
    t = small / (2.0 + small)
    t2 = t * t
    series = 1.0 / 17.0
    for n in (15.0, 13.0, 11.0, 9.0, 7.0, 5.0, 3.0, 1.0):
        series = 1.0 / n + t2 * series
    return jnp.maximum(x, 0.0) + 2.0 * t * series


LOADS = (
    "tok", "gain", "w_in", "w_gate", "w_q", "w_rope", "w_lat", "w_exp", "lat_gain", "cos", "sin",
    "rf", "taps", "rmap", "imap", "decay", "rgain", "again", "w_rec", "w_att", "post",
)


def layer(*refs):
    n_in = len(LOADS)
    src = dict(zip(LOADS, refs[:n_in]))
    out_ref = refs[n_in]
    (
        tok, gain, v_ig, v_qr, v_lat, v_exp, lat_gain, cos_s, sin_s, rf, taps, rmap, imap, decay,
        rgain, again, w_rec, w_att, post,
        a_ig, a_qr, a_lat, sq,
        own_kv, own_q, rec_s, gate_s, kv, qs, halo, ext, m_s, l_s, o_s, cum_s, loc_s,
        mine_x, cx, mine_z, cz, po, ps, go, gs,
        act_r, act_t, sums, got_s, inv_s, r_out, r_in, r_own, t_out, t_in, t_own,
        part, f_out, f_in, n_out, n_in_s,
        lsem, hi, ass, ars, kss, krs, qss, qrs, hsem, xss, xrs, zss, zrs, oss, ors, tss, trs,
        sss, srs, rss, rrs, pss, prs, fss, frs, nss, nrs,
    ) = refs[n_in + 1 :]

    sp, tp = lax.axis_index("sp"), lax.axis_index("tp")
    z, x = sp // NX, sp % NX
    y, c = tp // 2, tp % 2

    def at_tp(yy, cc):
        return yy * 2 + cc

    sib = at_tp(y, 1 - c)
    up, dn, far = (at_tp((y + d) % NY, c) for d in (1, 3, 2))
    up_sib, dn_sib, far_sib = (at_tp((y + d) % NY, 1 - c) for d in (1, 3, 2))

    def at_zx(zz, xx):
        return {"sp": zz * NX + xx}

    zup, zdn = at_zx((z + 1) % NZ, x), at_zx((z + NZ - 1) % NZ, x)
    xs = {d: at_zx(z, (x + d) % NX) for d in range(1, NX)}

    rows, depth = tok.shape[1], tok.shape[2]
    model = depth * NT
    half = rows // 2

    where = {
        "tok": tok.at[tp], "gain": gain, "w_in": v_ig.at[:, pl.ds(0, 128)],
        "w_gate": v_ig.at[:, pl.ds(128, 128)], "w_q": v_qr.at[pl.ds(0, QK)],
        "w_rope": v_qr.at[pl.ds(QK, ROPE)], "w_lat": v_lat, "w_exp": v_exp, "lat_gain": lat_gain,
        "cos": cos_s, "sin": sin_s, "rf": rf, "taps": taps, "rmap": rmap, "imap": imap,
        "decay": decay, "rgain": rgain, "again": again, "w_rec": w_rec, "w_att": w_att, "post": post,
    }
    load = {
        name: pltpu.make_async_copy(src[name], where[name], lsem.at[k])
        for k, name in enumerate(LOADS)
    }
    for name in LOADS:
        load[name].start()
    greet([{"tp": sib}, {"tp": up}, {"tp": dn}, xs[1], xs[3], zup, zdn])
    hello(hi.at[0], xs[3])
    hello(hi.at[1], {"tp": dn})
    hello(hi.at[2], {"tp": sib})

    sent = []

    def go_send(copy):
        copy.start()
        sent.append(copy)

    h0, h1, whole = pl.ds(0, half), pl.ds(half, half), pl.ds(0, rows)

    def tok_msg(k, slot, piece, to):
        at = tok.at[slot, piece]
        return remote(at, at, ass.at[k], ars.at[k], {"tp": to})

    def send(k, slot, piece, to):
        go_send(tok_msg(k, slot, piece, to))

    def arrived(k, slot, piece):
        tok_msg(k, slot, piece, sib).wait_recv()

    load["tok"].wait()
    send(1, tp, h0, up)
    send(3, tp, h1, dn)
    send(0, tp, whole, sib)
    send(2, tp, h1, up)
    send(4, tp, h0, dn)

    def chunk(source, first=False):
        wide = tok[source].astype(F32)
        square = wide * wide
        folded = square[:, 0:128]
        for k in range(1, depth // 128):
            folded = folded + square[:, k * 128 : (k + 1) * 128]
        at = pl.ds(pl.multiple_of(source * depth, depth), depth)
        low = (wide * gain[:, at]).astype(BF16)
        ig, qr, lat = mm(low, v_ig[at, :]), mm_t(low, v_qr[:, at]), mm(low, v_lat[at, :])
        if first:
            sq[...], a_ig[...], a_qr[...], a_lat[...] = folded, ig, qr, lat
        else:
            sq[...] += folded
            a_ig[...] += ig
            a_qr[...] += qr
            a_lat[...] += lat

    for name in ("gain", "w_in", "w_gate", "w_q", "w_rope", "w_lat"):
        load[name].wait()
    chunk(tp, True)
    pl.semaphore_wait(hi.at[2], 1)
    hello(hi.at[3], {"tp": dn})
    arrived(0, sib, whole)
    chunk(sib)
    arrived(1, dn, h0)
    send(5, dn, h0, up)
    send(7, dn, h0, sib)
    arrived(3, up, h1)
    send(6, up, h1, dn)
    send(9, up, h1, sib)
    arrived(2, dn, h1)
    send(8, dn, h1, sib)
    arrived(4, up, h0)
    send(10, up, h0, sib)
    chunk(dn)
    chunk(up)
    arrived(7, dn_sib, h0)
    arrived(8, dn_sib, h1)
    chunk(dn_sib)
    arrived(9, up_sib, h1)
    arrived(10, up_sib, h0)
    chunk(up_sib)
    arrived(5, far, h0)
    send(11, far, h0, sib)
    arrived(6, far, h1)
    send(12, far, h1, sib)
    chunk(far)
    for name in LOADS[7:]:
        load[name].wait()
    arrived(11, far_sib, h0)
    arrived(12, far_sib, h1)
    chunk(far_sib)

    inverse = lax.rsqrt(jnp.sum(sq[...], axis=1, keepdims=True) / model + EPS)
    latent = inverse * a_lat[...]
    spread = lax.rsqrt(jnp.mean(latent * latent, axis=1, keepdims=True) + EPS)
    latent = (latent * spread * lat_gain[...]).astype(BF16)
    expanded = mm(latent, v_exp[...]).T
    turned = (inverse * a_qr[:, NOPE:]).T
    cosine, sine = cos_s[...], sin_s[...]
    hr = ROPE // 2
    u, w = turned[ROPE : ROPE + hr], turned[ROPE + hr :]
    own_kv[0:NOPE, :] = expanded[0:NOPE].astype(BF16)
    own_kv[NOPE : NOPE + hr, :] = (u * cosine - w * sine).astype(BF16)
    own_kv[NOPE + hr : QK, :] = (w * cosine + u * sine).astype(BF16)
    own_kv[QK:, :] = expanded[NOPE:].astype(BF16)

    size = (QK + VDIM) // PIECES

    def piece_at(p):
        return pl.ds(p * size, size)

    def kv_msg(source, direction, hop, p):
        k = (direction * 4 + hop - 1) * PIECES + p
        slot = (z + (NZ - hop + 1 if direction == 0 else hop - 1)) % NZ
        return remote(
            source, kv.at[slot, piece_at(p)], kss.at[k], krs.at[k], zup if direction == 0 else zdn
        )

    def kv_goes(direction, hop, p):
        return hop < 4 or (hop == 4 and (direction == 0) == (p < PIECES // 2))

    for p in range(PIECES):
        for direction in (0, 1):
            go_send(kv_msg(own_kv.at[piece_at(p)], direction, 1, p))

    u, w = turned[0:hr], turned[hr:ROPE]
    own_q[0:NOPE, :] = (inverse * a_qr[:, 0:NOPE]).T.astype(BF16)
    own_q[NOPE : NOPE + hr, :] = (u * cosine - w * sine).astype(BF16)
    own_q[NOPE + hr :, :] = (w * cosine + u * sine).astype(BF16)
    rec_s[...] = (inverse * a_ig[:, 0:128]).astype(BF16)
    gate_s[...] = inverse * a_ig[:, 128:256]
    succ = {"sp": (sp + 1) % (NX * NZ)}
    tail = rows - 16

    pl.semaphore_wait(hi.at[0], 1)
    pl.semaphore_wait(hi.at[1], 1)

    def q_msg(d, slot):
        return remote(own_q, qs.at[slot], qss.at[d - 1], qrs.at[d - 1], xs[d])

    for d in (2, 1, 3):
        go_send(q_msg(d, x))

    for xx in range(NX):
        m_s[xx] = jnp.full((1, rows), LOW, F32)
        l_s[xx] = jnp.zeros((1, rows), F32)
        o_s[xx] = jnp.zeros((VDIM, rows), F32)

    scale = math.log2(math.e) / math.sqrt(QK)

    def attend(slots, queries, keys, values, masked):
        scores = [mm(keys, query) * scale for query in queries]
        if masked:
            key = lax.broadcasted_iota(jnp.int32, scores[0].shape, 0)
            place = lax.broadcasted_iota(jnp.int32, scores[0].shape, 1)
            scores = [jnp.where(key <= place, s, LOW) for s in scores]
        before = [m_s[k] for k in slots]
        most = [jnp.maximum(b, jnp.max(s, axis=0, keepdims=True)) for b, s in zip(before, scores)]
        weights = [jnp.exp2(s - m) for s, m in zip(scores, most)]
        shrink = [jnp.exp2(b - m) for b, m in zip(before, most)]
        for k, m, s, wt in zip(slots, most, shrink, weights):
            m_s[k] = m
            l_s[k] = l_s[k] * s + jnp.sum(wt, axis=0, keepdims=True)
        for k, s, wt in zip(slots, shrink, weights):
            o_s[k] = o_s[k] * s + mm(values, wt.astype(BF16))

    def unit(slot):
        attend(
            range(NX), [qs[k] for k in range(NX)], kv[slot, 0:QK, :].T, kv[slot, QK:, :], False
        )

    def poll(hop, pieces):
        for p in pieces:
            for direction in (0, 1):
                if kv_goes(direction, hop, p):
                    slot = (z + (NZ - hop if direction == 0 else hop)) % NZ
                    here = kv.at[slot, piece_at(p)]
                    k = (direction * 4 + hop - 1) * PIECES + p
                    remote(here, here, kss.at[k], krs.at[k], zup).wait_recv()
                    if kv_goes(direction, hop + 1, p):
                        go_send(kv_msg(here, direction, hop + 1, p))

    first_half, second_half = (0, 1), (2, 3)

    ext[16:, :] = rec_s[...].astype(F32)
    mine_tail = remote(rec_s.at[pl.ds(tail, 16)], halo, hsem.at[0], hsem.at[1], succ)
    go_send(mine_tail)
    own_k = own_kv[0:QK, :].T
    attend((x,), [own_q[...]], own_k, own_kv[QK:, :], True)
    poll(1, first_half)
    mine_tail.wait_recv()
    ext[0:16, :] = jnp.where(sp == 0, 0.0, halo[...].astype(F32))
    convolved = taps[0:1, :] * ext[13 : 13 + rows, :]
    for k in range(1, 4):
        convolved = convolved + taps[k : k + 1, :] * ext[13 + k : 13 + k + rows, :]
    conv_low = convolved.astype(BF16)
    rate = jax.nn.sigmoid(mm(conv_low, rmap[...]))
    entry = jax.nn.sigmoid(mm(conv_low, imap[...]))
    factor = jnp.broadcast_to(rf[...], (128, rows)).T
    log_keep = (-RATE_C) * factor * rate * softplus(-decay[...])
    cum = jnp.exp(log_keep)
    local = jnp.sqrt(minus_expm1(2.0 * log_keep)) * entry * convolved
    step = 1
    while step < rows:
        local = local + cum * shifted(local, step, 0.0)
        cum = cum * shifted(cum, step, 1.0)
        step *= 2
    cum_s[...] = cum
    loc_s[...] = local
    mine_x[0:1, :] = cum[rows - 1 :]
    mine_x[1:2, :] = local[rows - 1 :]

    def x_msg(d, slot):
        return remote(mine_x, cx.at[slot], xss.at[d - 1], xrs.at[d - 1], xs[d])

    for d in range(1, NX):
        go_send(x_msg(d, x))
    poll(1, second_half)

    qs[x] = own_q[...]
    for d in range(1, NX):
        q_msg(d, (x + NX - d) % NX).wait_recv()
    for xx in range(1, NX):

        @pl.when(x < xx)
        def _():
            attend((xx,), [qs[xx]], own_kv[0:QK, :].T, own_kv[QK:, :], False)

    def against(slot):
        @pl.when(slot < z)
        def _():
            unit(slot)

    def z_msg(source, direction, hop):
        slot = (z + (NZ - hop + 1 if direction == 0 else hop - 1)) % NZ
        k = direction * 4 + hop - 1
        return remote(source, cz.at[slot], zss.at[k], zrs.at[k], zup if direction == 0 else zdn)

    def z_step(hop):
        for direction in (0, 1):
            if hop == 4 and direction == 1:
                continue
            slot = (z + (NZ - hop if direction == 0 else hop)) % NZ
            here = cz.at[slot]
            k = direction * 4 + hop - 1
            remote(here, here, zss.at[k], zrs.at[k], zup).wait_recv()
            if hop < 3 or (hop == 3 and direction == 0):
                go_send(z_msg(here, direction, hop + 1))

    for hop in range(2, 5):
        below, above = (z + NZ - hop + 1) % NZ, (z + hop - 1) % NZ
        poll(hop, first_half)
        against(below)
        if hop == 2:
            cx[x] = mine_x[...]
            for d in range(1, NX):
                x_msg(d, (x + NX - d) % NX).wait_recv()
            pa, pb = jnp.ones((1, 128), F32), jnp.zeros((1, 128), F32)
            ta, tb = pa, pb
            for i in range(NX):
                a, b = cx[i, 0:1, :], cx[i, 1:2, :]
                ta, tb = ta * a, a * tb + b
                pa = jnp.where(i < x, pa * a, pa)
                pb = jnp.where(i < x, a * pb + b, pb)
            mine_z[0:1, :] = ta
            mine_z[1:2, :] = tb
            for direction in (0, 1):
                go_send(z_msg(mine_z, direction, 1))
        else:
            z_step(hop - 2)
        poll(hop, second_half)
        against(above)
    against((z + 4) % NZ)

    def o_msg(d):
        return remote(po.at[d - 1], go.at[d - 1], oss.at[d - 1], ors.at[d - 1], xs[d])

    def s_msg(d):
        return remote(ps.at[d - 1], gs.at[d - 1], tss.at[d - 1], trs.at[d - 1], xs[d])

    for d in (2, 1, 3):
        xx = (x + d) % NX
        total = l_s[xx]
        ps[d - 1, 0:1, :] = m_s[xx]
        ps[d - 1, 1:2, :] = total
        po[d - 1] = (o_s[xx] / jnp.where(total > 0.0, total, 1.0)).astype(BF16)
        go_send(s_msg(d))
        go_send(o_msg(d))

    z_step(3)
    cz[z] = mine_z[...]
    z_step(4)
    entering = jnp.zeros((1, 128), F32)
    for i in range(NZ):
        entering = jnp.where(i < z, cz[i, 0:1, :] * entering + cz[i, 1:2, :], entering)
    entering = pa * entering + pb
    state = loc_s[...] + cum_s[...] * entering
    rec = state * jax.nn.gelu(gate_s[...])
    act_r[...] = (rec * rgain[...]).astype(BF16)
    square = (rec * rec).T
    sums[0:1, :] = jnp.sum(square, axis=0, keepdims=True)

    order = [(y + 2) % NY, (y + 1) % NY, (y + 3) % NY, y]
    mine = out_ref.shape[0]

    def rows_of(yy, cc):
        return pl.ds(pl.multiple_of((yy * 2 + cc) * mine, mine), mine)

    def r_msg(k):
        return remote(r_out.at[k], r_in.at[k], rss.at[k], rrs.at[k], {"tp": sib})

    def t_msg(k):
        return remote(t_out.at[k], t_in.at[k], pss.at[k], prs.at[k], {"tp": sib})

    for k, yy in enumerate(order):
        r_out[k] = mm(act_r[rows_of(yy, 1 - c), :], w_rec[...]).astype(BF16)
        go_send(r_msg(k))
    for k, yy in enumerate(order):
        r_own[k] = mm(act_r[rows_of(yy, c), :], w_rec[...])

    most = m_s[x]
    for d in range(1, NX):
        s_msg(d).wait_recv()
        most = jnp.maximum(most, gs[d - 1, 0:1, :])
    share = jnp.exp2(m_s[x] - most)
    total = l_s[x] * share
    out = o_s[x] * share
    for d in range(1, NX):
        o_msg(d).wait_recv()
        share = gs[d - 1, 1:2, :] * jnp.exp2(gs[d - 1, 0:1, :] - most)
        total = total + share
        out = out + go[d - 1].astype(F32) * share
    out = out / total
    sums[1:2, :] = jnp.sum(out * out, axis=0, keepdims=True)

    def sum_msg(d):
        return remote(sums, got_s.at[d - 1], sss.at[d - 1], srs.at[d - 1], {"tp": (tp + d) % NT})

    pl.semaphore_wait(hi.at[3], 1)
    for d in (4, 3, 5, 2, 6, 1, 7):
        go_send(sum_msg(d))
    act_t[...] = (out.T * again[...]).astype(BF16)
    for k, yy in enumerate(order):
        t_out[k] = mm(act_t[rows_of(yy, 1 - c), :], w_att[...]).astype(BF16)
        go_send(t_msg(k))
    for k, yy in enumerate(order):
        t_own[k] = mm(act_t[rows_of(yy, c), :], w_att[...])
    total = sums[...]
    for d in range(1, NT):
        sum_msg(d).wait_recv()
        total = total + got_s[d - 1]
    inverse = lax.rsqrt(total / (128 * NT) + EPS)
    inv_s[0] = jnp.broadcast_to(inverse[0:1, :], (128, rows)).T
    inv_s[1] = jnp.broadcast_to(inverse[1:2, :], (128, rows)).T

    def chip_sum(k):
        at = rows_of(order[k], c)
        r_msg(k).wait_recv()
        t_msg(k).wait_recv()
        value = (r_own[k] + r_in[k].astype(F32)) * inv_s[0, at, :][:, 0:1]
        return value + (t_own[k] + t_in[k].astype(F32)) * inv_s[1, at, :][:, 0:1]

    middle = model // 2
    left, right = pl.ds(0, middle), pl.ds(middle, middle)

    def f_msg(cols, k, to):
        return remote(f_out.at[:, cols], f_in.at[:, cols], fss.at[k], frs.at[k], {"tp": to})

    def n_msg(side, cols, k, to):
        at = (side, slice(None), cols)
        return remote(n_out.at[at], n_in_s.at[at], nss.at[k], nrs.at[k], {"tp": to})

    f_out[...] = chip_sum(0).astype(BF16)
    go_send(f_msg(left, 0, up))
    go_send(f_msg(right, 1, dn))
    part[0] = chip_sum(1)
    n_out[0, :, middle:] = part[0, :, middle:].astype(BF16)
    go_send(n_msg(0, right, 0, up))
    part[1] = chip_sum(2)
    n_out[1, :, 0:middle] = part[1, :, 0:middle].astype(BF16)
    go_send(n_msg(1, left, 1, dn))
    own = chip_sum(3)
    f_msg(left, 0, up).wait_recv()
    n_out[0, :, 0:middle] = (part[0, :, 0:middle] + f_in[:, 0:middle].astype(F32)).astype(BF16)
    go_send(n_msg(0, left, 2, up))
    f_msg(right, 1, dn).wait_recv()
    n_out[1, :, middle:] = (part[1, :, middle:] + f_in[:, middle:].astype(F32)).astype(BF16)
    go_send(n_msg(1, right, 3, dn))
    part[0] = own
    for k, (side, cols) in enumerate(((0, right), (1, left), (0, left), (1, right))):
        n_msg(side, cols, k, up).wait_recv()
    mixed = part[0] + n_in_s[0].astype(F32) + n_in_s[1].astype(F32)
    spread = lax.rsqrt(jnp.mean(mixed * mixed, axis=1, keepdims=True) + EPS)
    out_ref[...] = (mixed * spread * post[...]).astype(BF16)
    for copy in sent:
        copy.wait_send()


def call_layer(*operands):
    rows, depth = operands[0].shape
    model = depth * NT
    mine = rows // NT
    dma = pltpu.SemaphoreType.DMA
    vm = pltpu.VMEM
    scratch = [
        vm((NT, rows, depth), BF16), vm((1, model), F32), vm((model, 256), BF16),
        vm((QK + ROPE, model), BF16), vm((model, 512), BF16), vm((512, NOPE + VDIM), BF16),
        vm((1, 512), F32), vm((ROPE // 2, rows), F32), vm((ROPE // 2, rows), F32),
        vm((1, rows), F32), vm((4, 128), F32), vm((128, 128), BF16), vm((128, 128), BF16),
        vm((1, 128), F32), vm((1, 128), F32), vm((1, 128), F32), vm((128, model), BF16),
        vm((128, model), BF16), vm((1, model), F32),
        vm((rows, 256), F32), vm((rows, 256), F32), vm((rows, 512), F32), vm((rows, 128), F32),
        vm((QK + VDIM, rows), BF16), vm((QK, rows), BF16), vm((rows, 128), BF16),
        vm((rows, 128), F32), vm((NZ, QK + VDIM, rows), BF16), vm((NX, QK, rows), BF16),
        vm((16, 128), BF16), vm((16 + rows, 128), F32), vm((NX, 1, rows), F32),
        vm((NX, 1, rows), F32), vm((NX, VDIM, rows), F32), vm((rows, 128), F32),
        vm((rows, 128), F32),
        vm((2, 128), F32), vm((NX, 2, 128), F32), vm((2, 128), F32), vm((NZ, 2, 128), F32),
        vm((NX - 1, VDIM, rows), BF16), vm((NX - 1, 2, rows), F32),
        vm((NX - 1, VDIM, rows), BF16), vm((NX - 1, 2, rows), F32),
        vm((rows, 128), BF16), vm((rows, 128), BF16), vm((2, rows), F32),
        vm((NT - 1, 2, rows), F32), vm((2, rows, 128), F32),
        vm((NY, mine, model), BF16), vm((NY, mine, model), BF16), vm((NY, mine, model), F32),
        vm((NY, mine, model), BF16), vm((NY, mine, model), BF16), vm((NY, mine, model), F32),
        vm((2, mine, model), F32), vm((mine, model), BF16), vm((mine, model), BF16),
        vm((2, mine, model), BF16), vm((2, mine, model), BF16),
        dma((len(LOADS),)), pltpu.SemaphoreType.REGULAR((4,)),
        dma((13,)), dma((13,)), dma((8 * PIECES,)), dma((8 * PIECES,)),
        dma((NX - 1,)), dma((NX - 1,)), dma((2,)), dma((NX - 1,)), dma((NX - 1,)),
        dma((8,)), dma((8,)), dma((NX - 1,)), dma((NX - 1,)), dma((NX - 1,)), dma((NX - 1,)),
        dma((NT - 1,)), dma((NT - 1,)), dma((NY,)), dma((NY,)), dma((NY,)), dma((NY,)),
        dma((2,)), dma((2,)), dma((4,)), dma((4,)),
    ]
    return pl.pallas_call(
        layer,
        name="layer",
        out_shape=jax.ShapeDtypeStruct((mine, model), BF16),
        in_specs=[pl.BlockSpec(memory_space=pl.ANY)] * len(LOADS),
        out_specs=pl.BlockSpec(memory_space=pltpu.VMEM),
        scratch_shapes=scratch,
        compiler_params=pltpu.CompilerParams(
            collective_id=0, has_side_effects=True, vmem_limit_bytes=63 * 1024 * 1024
        ),
    )(*operands)


def shards(
    tokens, pre_gain, rate_factor, w_rec_in, w_rec_gate, conv_taps, rate_maps, input_maps,
    decay_param, w_query, w_latent, w_rope_key, latent_gain, w_expand, rec_gain, att_gain,
    w_out_rec, w_out_att, post_gain,
):
    rows = tokens.shape[0]
    frequency = 1.0 / THETA ** (jnp.arange(0, ROPE, 2).astype(F32) / ROPE)
    places = (lax.axis_index("sp") * rows + jnp.arange(rows)).astype(F32)
    turned = places[None, :] * frequency[:, None]
    given = {
        "tok": tokens, "gain": pre_gain[None], "w_in": w_rec_in, "w_gate": w_rec_gate,
        "w_q": w_query.T, "w_rope": w_rope_key.T, "w_lat": w_latent, "w_exp": w_expand,
        "lat_gain": latent_gain[None], "cos": jnp.cos(turned), "sin": jnp.sin(turned),
        "rf": rate_factor[None], "taps": conv_taps, "rmap": rate_maps[0], "imap": input_maps[0],
        "decay": decay_param[None], "rgain": rec_gain[None], "again": att_gain[None],
        "w_rec": w_out_rec, "w_att": w_out_att, "post": post_gain[None],
    }
    return call_layer(*(given[name] for name in LOADS))


def solution(mesh):
    placed = (
        P("sp", "tp"), P(), P("sp"), P(None, "tp"), P(None, "tp"), P(None, "tp"),
        P("tp", None, None), P("tp", None, None), P("tp"), P(None, "tp"), P(), P(), P(),
        P(None, "tp"), P("tp"), P("tp"), P("tp", None), P("tp", None), P(),
    )
    return jax.shard_map(
        shards, mesh=mesh, in_specs=placed, out_specs=P(("sp", "tp"), None), check_vma=False
    )
```

```python
import math

import jax
import jax.numpy as jnp
from jax import lax
from jax.experimental import pallas as pl
from jax.experimental.pallas import tpu as pltpu
from jax.sharding import PartitionSpec as P

NOPE = 128
ROPE = 64
VDIM = 128
EPS = 1e-06
RATE_C = 8.0
THETA = 10000.0
NY, NX, NZ = 4, 4, 8
NT = 2 * NY
PIECES = 4
LOW = -1e30
MESH = pl.DeviceIdType.MESH
F32, BF16 = jnp.float32, jnp.bfloat16
QK = NOPE + ROPE


def remote(src, dst, send, recv, where):
    return pltpu.make_async_remote_copy(
        src_ref=src, dst_ref=dst, send_sem=send, recv_sem=recv, device_id=where, device_id_type=MESH
    )


def greet(partners):
    barrier = pltpu.get_barrier_semaphore()
    for where in partners:
        pl.semaphore_signal(barrier, inc=1, device_id=where, device_id_type=MESH)
    pl.semaphore_wait(barrier, len(partners))


def hello(sem, where):
    pl.semaphore_signal(sem, inc=1, device_id=where, device_id_type=MESH)


def mm(a, b):
    return jnp.dot(a, b, preferred_element_type=F32)


def mm_t(a, b):
    return lax.dot_general(a, b, (((1,), (1,)), ((), ())), preferred_element_type=F32)


def shifted(values, by, fill):
    row = lax.broadcasted_iota(jnp.int32, values.shape, 0)
    return jnp.where(row < by, fill, pltpu.roll(values, by, 0))


def minus_expm1(x):
    series = 1.0 + x * (1.0 / 7.0)
    for n in (6.0, 5.0, 4.0, 3.0, 2.0):
        series = 1.0 + (x * (1.0 / n)) * series
    return jnp.where(x > -0.25, -x * series, 1.0 - jnp.exp(x))


def softplus(x):
    small = jnp.exp(-jnp.abs(x))
    t = small / (2.0 + small)
    t2 = t * t
    series = 1.0 / 17.0
    for n in (15.0, 13.0, 11.0, 9.0, 7.0, 5.0, 3.0, 1.0):
        series = 1.0 / n + t2 * series
    return jnp.maximum(x, 0.0) + 2.0 * t * series


LOADS = (
    "tok", "gain", "w_in", "w_gate", "w_q", "w_rope", "w_lat", "w_exp", "lat_gain", "cos", "sin",
    "rf", "taps", "rmap", "imap", "decay", "rgain", "again", "w_rec", "w_att", "post",
)


def layer(*refs):
    n_in = len(LOADS)
    src = dict(zip(LOADS, refs[:n_in]))
    out_ref = refs[n_in]
    (
        tok, gain, v_ig, v_qr, v_lat, v_exp, lat_gain, cos_s, sin_s, rf, taps, rmap, imap, decay,
        rgain, again, w_rec, w_att, post,
        a_ig, a_qr, a_lat, sq,
        own_kv, own_q, rec_s, gate_s, kv, qs, halo, ext, m_s, l_s, o_s, cum_s, loc_s,
        mine_x, cx, mine_z, cz, po, ps, go, gs,
        act_r, act_t, sums, got_s, inv_s, part,
        lsem, hi, ass, ars, kss, krs, qss, qrs, hsem, xss, xrs, zss, zrs, oss, ors, tss, trs,
        sss, srs, *rest,
    ) = refs[n_in + 1 :]
    r_bufs, t_bufs = rest[0:7], rest[7:14]
    r_sems, t_sems = rest[14:20], rest[20:26]

    sp, tp = lax.axis_index("sp"), lax.axis_index("tp")
    z, x = sp // NX, sp % NX
    y, c = tp // 2, tp % 2

    def at_tp(yy, cc):
        return yy * 2 + cc

    sib = at_tp(y, 1 - c)
    up, dn, far = (at_tp((y + d) % NY, c) for d in (1, 3, 2))
    up_sib, dn_sib, far_sib = (at_tp((y + d) % NY, 1 - c) for d in (1, 3, 2))

    def at_zx(zz, xx):
        return {"sp": zz * NX + xx}

    zup, zdn = at_zx((z + 1) % NZ, x), at_zx((z + NZ - 1) % NZ, x)
    xs = {d: at_zx(z, (x + d) % NX) for d in range(1, NX)}

    rows, depth = tok.shape[1], tok.shape[2]
    model = depth * NT
    half = rows // 2

    where = {
        "tok": tok.at[tp], "gain": gain, "w_in": v_ig.at[:, pl.ds(0, 128)],
        "w_gate": v_ig.at[:, pl.ds(128, 128)], "w_q": v_qr.at[pl.ds(0, QK)],
        "w_rope": v_qr.at[pl.ds(QK, ROPE)], "w_lat": v_lat, "w_exp": v_exp, "lat_gain": lat_gain,
        "cos": cos_s, "sin": sin_s, "rf": rf, "taps": taps, "rmap": rmap, "imap": imap,
        "decay": decay, "rgain": rgain, "again": again, "w_rec": w_rec, "w_att": w_att, "post": post,
    }
    load = {
        name: pltpu.make_async_copy(src[name], where[name], lsem.at[k])
        for k, name in enumerate(LOADS)
    }
    load["tok"].start()
    greet([{"tp": sib}, {"tp": up}, {"tp": dn}, xs[1], xs[3], zup, zdn])
    hello(hi.at[0], xs[3])
    hello(hi.at[1], {"tp": dn})
    hello(hi.at[2], {"tp": sib})
    hello(hi.at[4], zdn)
    hello(hi.at[5], zup)

    sent = []

    def go_send(copy):
        copy.start()
        sent.append(copy)

    h0, h1, whole = pl.ds(0, half), pl.ds(half, half), pl.ds(0, rows)

    def tok_msg(k, slot, piece, to):
        at = tok.at[slot, piece]
        return remote(at, at, ass.at[k], ars.at[k], {"tp": to})

    def send(k, slot, piece, to):
        go_send(tok_msg(k, slot, piece, to))

    def arrived(k, slot, piece):
        tok_msg(k, slot, piece, sib).wait_recv()

    load["tok"].wait()
    send(1, tp, h0, up)
    send(3, tp, h1, dn)
    send(0, tp, whole, sib)
    send(2, tp, h1, up)
    send(4, tp, h0, dn)
    for name in LOADS[1:]:
        load[name].start()

    def chunk(source, first=False):
        wide = tok[source].astype(F32)
        square = wide * wide
        folded = square[:, 0:128]
        for k in range(1, depth // 128):
            folded = folded + square[:, k * 128 : (k + 1) * 128]
        at = pl.ds(pl.multiple_of(source * depth, depth), depth)
        low = (wide * gain[:, at]).astype(BF16)
        ig, qr, lat = mm(low, v_ig[at, :]), mm_t(low, v_qr[:, at]), mm(low, v_lat[at, :])
        if first:
            sq[...], a_ig[...], a_qr[...], a_lat[...] = folded, ig, qr, lat
        else:
            sq[...] += folded
            a_ig[...] += ig
            a_qr[...] += qr
            a_lat[...] += lat

    for name in ("gain", "w_in", "w_gate", "w_q", "w_rope", "w_lat"):
        load[name].wait()
    chunk(tp, True)
    pl.semaphore_wait(hi.at[2], 1)
    hello(hi.at[3], {"tp": dn})
    pl.semaphore_wait(hi.at[4], 1)
    hello(hi.at[6], zdn)
    pl.semaphore_wait(hi.at[5], 1)
    hello(hi.at[7], zup)
    arrived(0, sib, whole)
    chunk(sib)
    arrived(1, dn, h0)
    send(5, dn, h0, up)
    send(7, dn, h0, sib)
    arrived(3, up, h1)
    send(6, up, h1, dn)
    send(9, up, h1, sib)
    arrived(2, dn, h1)
    send(8, dn, h1, sib)
    arrived(4, up, h0)
    send(10, up, h0, sib)
    chunk(dn)
    pl.semaphore_wait(hi.at[6], 1)
    hello(hi.at[8], zdn)
    pl.semaphore_wait(hi.at[7], 1)
    chunk(up)
    arrived(7, dn_sib, h0)
    arrived(8, dn_sib, h1)
    chunk(dn_sib)
    arrived(9, up_sib, h1)
    arrived(10, up_sib, h0)
    chunk(up_sib)
    arrived(5, far, h0)
    send(11, far, h0, sib)
    arrived(6, far, h1)
    send(12, far, h1, sib)
    chunk(far)
    for name in LOADS[7:]:
        load[name].wait()
    arrived(11, far_sib, h0)
    arrived(12, far_sib, h1)
    chunk(far_sib)

    inverse = lax.rsqrt(jnp.sum(sq[...], axis=1, keepdims=True) / model + EPS)
    rec_s[...] = (inverse * a_ig[:, 0:128]).astype(BF16)
    succ = {"sp": (sp + 1) % (NX * NZ)}
    tail = rows - 16
    pl.semaphore_wait(hi.at[0], 1)
    mine_tail = remote(rec_s.at[pl.ds(tail, 16)], halo, hsem.at[0], hsem.at[1], succ)
    go_send(mine_tail)
    latent = inverse * a_lat[...]
    spread = lax.rsqrt(jnp.mean(latent * latent, axis=1, keepdims=True) + EPS)
    latent = (latent * spread * lat_gain[...]).astype(BF16)
    expanded = mm(latent, v_exp[...]).T
    turned = (inverse * a_qr[:, NOPE:]).T
    cosine, sine = cos_s[...], sin_s[...]
    hr = ROPE // 2
    u, w = turned[ROPE : ROPE + hr], turned[ROPE + hr :]
    own_kv[0:NOPE, :] = expanded[0:NOPE].astype(BF16)
    own_kv[NOPE : NOPE + hr, :] = (u * cosine - w * sine).astype(BF16)
    own_kv[NOPE + hr : QK, :] = (w * cosine + u * sine).astype(BF16)
    own_kv[QK:, :] = expanded[NOPE:].astype(BF16)

    size = (QK + VDIM) // PIECES

    def piece_at(p):
        return pl.ds(p * size, size)

    def kv_msg(source, direction, hop, p):
        k = (direction * 4 + hop - 1) * PIECES + p
        slot = (z + (NZ - hop + 1 if direction == 0 else hop - 1)) % NZ
        return remote(
            source, kv.at[slot, piece_at(p)], kss.at[k], krs.at[k], zup if direction == 0 else zdn
        )

    def kv_goes(direction, hop, p):
        return hop < 4 or (hop == 4 and (direction == 0) == (p < PIECES // 2))

    for p in range(PIECES):
        for direction in (0, 1):
            go_send(kv_msg(own_kv.at[piece_at(p)], direction, 1, p))

    u, w = turned[0:hr], turned[hr:ROPE]
    own_q[0:NOPE, :] = (inverse * a_qr[:, 0:NOPE]).T.astype(BF16)
    own_q[NOPE : NOPE + hr, :] = (u * cosine - w * sine).astype(BF16)
    own_q[NOPE + hr :, :] = (w * cosine + u * sine).astype(BF16)

    def q_msg(d, slot):
        return remote(own_q, qs.at[slot], qss.at[d - 1], qrs.at[d - 1], xs[d])

    go_send(q_msg(1, x))
    go_send(q_msg(3, x))
    gate_s[...] = inverse * a_ig[:, 128:256]
    pl.semaphore_wait(hi.at[1], 1)
    pl.semaphore_wait(hi.at[8], 1)

    for xx in range(NX):
        m_s[xx] = jnp.full((1, rows), LOW, F32)
        l_s[xx] = jnp.zeros((1, rows), F32)
        o_s[xx] = jnp.zeros((VDIM, rows), F32)

    scale = math.log2(math.e) / math.sqrt(QK)

    def attend(slots, queries, keys, values, masked):
        scores = [mm(keys, query) * scale for query in queries]
        if masked:
            key = lax.broadcasted_iota(jnp.int32, scores[0].shape, 0)
            place = lax.broadcasted_iota(jnp.int32, scores[0].shape, 1)
            scores = [jnp.where(key <= place, s, LOW) for s in scores]
        before = [m_s[k] for k in slots]
        most = [jnp.maximum(b, jnp.max(s, axis=0, keepdims=True)) for b, s in zip(before, scores)]
        weights = [jnp.exp2(s - m) for s, m in zip(scores, most)]
        shrink = [jnp.exp2(b - m) for b, m in zip(before, most)]
        for k, m, s, wt in zip(slots, most, shrink, weights):
            m_s[k] = m
            l_s[k] = l_s[k] * s + jnp.sum(wt, axis=0, keepdims=True)
        for k, s, wt in zip(slots, shrink, weights):
            o_s[k] = o_s[k] * s + mm(values, wt.astype(BF16))

    def unit(slot):
        attend(
            range(NX), [qs[k] for k in range(NX)], kv[slot, 0:QK, :].T, kv[slot, QK:, :], False
        )

    def poll(hop, pieces):
        for p in pieces:
            for direction in (0, 1):
                if kv_goes(direction, hop, p):
                    slot = (z + (NZ - hop if direction == 0 else hop)) % NZ
                    here = kv.at[slot, piece_at(p)]
                    k = (direction * 4 + hop - 1) * PIECES + p
                    remote(here, here, kss.at[k], krs.at[k], zup).wait_recv()
                    if kv_goes(direction, hop + 1, p):
                        go_send(kv_msg(here, direction, hop + 1, p))

    first_half, second_half = (0, 1), (2, 3)

    def against(slot):
        @pl.when(slot < z)
        def _():
            unit(slot)

    def below(hop):
        against((z + NZ - hop) % NZ)

    def above(hop):
        against((z + hop) % NZ)

    order = [(y + 2) % NY, (y + 1) % NY, (y + 3) % NY, y]
    mine = out_ref.shape[0]
    middle = model // 2
    left, right = pl.ds(0, middle), pl.ds(middle, middle)

    def rows_of(yy, cc):
        return pl.ds(pl.multiple_of((yy * 2 + cc) * mine, mine), mine)

    class Branch:
        def __init__(self, act, weight, bufs, sems):
            self.act, self.weight = act, weight
            self.out, self.got, self.own, self.f_out, self.f_in, self.n_out, self.n_in = bufs
            self.ps, self.pr, self.fs, self.fr, self.ns, self.nr = sems

        def pair(self, k):
            return remote(self.out.at[k], self.got.at[k], self.ps.at[k], self.pr.at[k], {"tp": sib})

        def far(self, k):
            cols, to = ((left, up), (right, dn))[k]
            return remote(
                self.f_out.at[:, cols], self.f_in.at[:, cols], self.fs.at[k], self.fr.at[k], {"tp": to}
            )

        def near(self, k):
            side, cols = ((0, right), (1, left), (0, left), (1, right))[k]
            at = (side, slice(None), cols)
            return remote(
                self.n_out.at[at], self.n_in.at[at], self.ns.at[k], self.nr.at[k],
                {"tp": (up, dn)[side]},
            )

        def product(self, k):
            yy = order[k]
            both = jnp.concatenate(
                [self.act[rows_of(yy, 1 - c), :], self.act[rows_of(yy, c), :]], axis=0
            )
            value = mm(both, self.weight[...])
            self.out[k] = value[0:mine].astype(BF16)
            go_send(self.pair(k))
            self.own[k] = value[mine:]

        def chip(self, k):
            self.pair(k).wait_recv()
            return self.own[k] + self.got[k].astype(F32)

        def send_far(self):
            self.f_out[...] = self.chip(0).astype(BF16)
            go_send(self.far(0))
            go_send(self.far(1))

        def send_pure(self):
            up_sum = self.chip(1)
            self.n_out[0, :, middle:] = up_sum[:, middle:].astype(BF16)
            go_send(self.near(0))
            self.own[1, :, 0:middle] = up_sum[:, 0:middle]
            dn_sum = self.chip(2)
            self.n_out[1, :, 0:middle] = dn_sum[:, 0:middle].astype(BF16)
            go_send(self.near(1))
            self.own[2, :, middle:] = dn_sum[:, middle:]
            self.own[3] = self.chip(3)

        def send_joined(self):
            self.far(0).wait_recv()
            joined = self.own[1, :, 0:middle] + self.f_in[:, 0:middle].astype(F32)
            self.n_out[0, :, 0:middle] = joined.astype(BF16)
            go_send(self.near(2))
            self.far(1).wait_recv()
            joined = self.own[2, :, middle:] + self.f_in[:, middle:].astype(F32)
            self.n_out[1, :, middle:] = joined.astype(BF16)
            go_send(self.near(3))

        def total(self):
            for k in range(4):
                self.near(k).wait_recv()
            return self.own[3] + self.n_in[0].astype(F32) + self.n_in[1].astype(F32)

    branch_r = Branch(act_r, w_rec, r_bufs, r_sems)
    branch_t = Branch(act_t, w_att, t_bufs, t_sems)

    ext[16:, :] = rec_s[...].astype(F32)
    attend((x,), [own_q[...]], own_kv[0:QK, :].T, own_kv[QK:, :], True)
    mine_tail.wait_recv()
    ext[0:16, :] = jnp.where(sp == 0, 0.0, halo[...].astype(F32))
    convolved = taps[0:1, :] * ext[13 : 13 + rows, :]
    for k in range(1, 4):
        convolved = convolved + taps[k : k + 1, :] * ext[13 + k : 13 + k + rows, :]
    conv_low = convolved.astype(BF16)
    rate = jax.nn.sigmoid(mm(conv_low, rmap[...]))
    entry = jax.nn.sigmoid(mm(conv_low, imap[...]))
    factor = jnp.broadcast_to(rf[...], (128, rows)).T
    log_keep = (-RATE_C) * factor * rate * softplus(-decay[...])
    cum = jnp.exp(log_keep)
    local = jnp.sqrt(minus_expm1(2.0 * log_keep)) * entry * convolved
    step = 1
    while step < rows:
        local = local + cum * shifted(local, step, 0.0)
        cum = cum * shifted(cum, step, 1.0)
        step *= 2
    cum_s[...] = cum
    loc_s[...] = local
    mine_x[0:1, :] = cum[rows - 1 :]
    mine_x[1:2, :] = local[rows - 1 :]

    def x_msg(d, slot):
        return remote(mine_x, cx.at[slot], xss.at[d - 1], xrs.at[d - 1], xs[d])

    for d in (2, 1, 3):
        go_send(x_msg(d, x))
    go_send(q_msg(2, x))
    poll(1, first_half)
    poll(1, second_half)

    cx[x] = mine_x[...]
    for d in range(1, NX):
        x_msg(d, (x + NX - d) % NX).wait_recv()
    pa, pb = jnp.ones((1, 128), F32), jnp.zeros((1, 128), F32)
    ta, tb = pa, pb
    for i in range(NX):
        a, b = cx[i, 0:1, :], cx[i, 1:2, :]
        ta, tb = ta * a, a * tb + b
        pa = jnp.where(i < x, pa * a, pa)
        pb = jnp.where(i < x, a * pb + b, pb)
    mine_z[0:1, :] = ta
    mine_z[1:2, :] = tb

    def z_msg(d, slot):
        to = at_zx((z + d) % NZ, x)
        return remote(mine_z, cz.at[slot], zss.at[d - 1], zrs.at[d - 1], to)

    for d in (4, 3, 5, 2, 6, 1, 7):
        go_send(z_msg(d, z))

    poll(2, first_half)
    qs[x] = own_q[...]
    for d in (1, 3, 2):
        q_msg(d, (x + NX - d) % NX).wait_recv()
    for xx in range(1, NX):

        @pl.when(x < xx)
        def _():
            attend((xx,), [qs[xx]], own_kv[0:QK, :].T, own_kv[QK:, :], False)

    poll(2, second_half)
    below(1)
    poll(3, first_half)
    above(1)

    cz[z] = mine_z[...]
    for d in range(1, NZ):
        z_msg(d, (z + NZ - d) % NZ).wait_recv()
    entering = jnp.zeros((1, 128), F32)
    for i in range(NZ):
        entering = jnp.where(i < z, cz[i, 0:1, :] * entering + cz[i, 1:2, :], entering)
    entering = pa * entering + pb
    state = loc_s[...] + cum_s[...] * entering
    rec = state * jax.nn.gelu(gate_s[...])
    act_r[...] = (rec * rgain[...]).astype(BF16)
    square = (rec * rec).T
    sums[0:1, :] = jnp.sum(square, axis=0, keepdims=True)
    for k in (0, 1):
        branch_r.product(k)
    poll(3, second_half)
    for k in (2, 3):
        branch_r.product(k)
    branch_r.send_far()
    below(2)
    poll(4, first_half)
    branch_r.send_pure()
    above(2)
    below(3)
    poll(4, second_half)
    above(3)
    below(4)

    def o_msg(d):
        return remote(po.at[d - 1], go.at[d - 1], oss.at[d - 1], ors.at[d - 1], xs[d])

    def s_msg(d):
        return remote(ps.at[d - 1], gs.at[d - 1], tss.at[d - 1], trs.at[d - 1], xs[d])

    for d in (2, 1, 3):
        xx = (x + d) % NX
        total = l_s[xx]
        ps[d - 1, 0:1, :] = m_s[xx]
        ps[d - 1, 1:2, :] = total
        po[d - 1] = (o_s[xx] / jnp.where(total > 0.0, total, 1.0)).astype(BF16)
        go_send(s_msg(d))
        go_send(o_msg(d))

    branch_r.send_joined()

    most = m_s[x]
    for d in range(1, NX):
        s_msg(d).wait_recv()
        most = jnp.maximum(most, gs[d - 1, 0:1, :])
    share = jnp.exp2(m_s[x] - most)
    total = l_s[x] * share
    out = o_s[x] * share
    for d in range(1, NX):
        o_msg(d).wait_recv()
        share = gs[d - 1, 1:2, :] * jnp.exp2(gs[d - 1, 0:1, :] - most)
        total = total + share
        out = out + go[d - 1].astype(F32) * share
    out = out / total
    sums[1:2, :] = jnp.sum(out * out, axis=0, keepdims=True)

    def sum_msg(d):
        return remote(sums, got_s.at[d - 1], sss.at[d - 1], srs.at[d - 1], {"tp": (tp + d) % NT})

    pl.semaphore_wait(hi.at[3], 1)
    for d in (4, 3, 5, 2, 6, 1, 7):
        go_send(sum_msg(d))
    act_t[...] = (out.T * again[...]).astype(BF16)
    branch_t.product(0)
    branch_t.product(1)
    branch_t.send_far()
    branch_t.product(2)
    branch_t.product(3)
    branch_t.send_pure()
    total = sums[...]
    for d in range(1, NT):
        sum_msg(d).wait_recv()
        total = total + got_s[d - 1]
    inverse = lax.rsqrt(total / (128 * NT) + EPS)
    inv_s[0] = jnp.broadcast_to(inverse[0:1, :], (128, rows)).T
    inv_s[1] = jnp.broadcast_to(inverse[1:2, :], (128, rows)).T
    at = rows_of(y, c)
    part[0] = branch_r.total() * inv_s[0, at, :][:, 0:1]
    branch_t.send_joined()
    mixed = part[0] + branch_t.total() * inv_s[1, at, :][:, 0:1]
    spread = lax.rsqrt(jnp.mean(mixed * mixed, axis=1, keepdims=True) + EPS)
    out_ref[...] = (mixed * spread * post[...]).astype(BF16)
    for copy in sent:
        copy.wait_send()


def call_layer(*operands):
    rows, depth = operands[0].shape
    model = depth * NT
    mine = rows // NT
    dma = pltpu.SemaphoreType.DMA
    vm = pltpu.VMEM
    scratch = [
        vm((NT, rows, depth), BF16), vm((1, model), F32), vm((model, 256), BF16),
        vm((QK + ROPE, model), BF16), vm((model, 512), BF16), vm((512, NOPE + VDIM), BF16),
        vm((1, 512), F32), vm((ROPE // 2, rows), F32), vm((ROPE // 2, rows), F32),
        vm((1, rows), F32), vm((4, 128), F32), vm((128, 128), BF16), vm((128, 128), BF16),
        vm((1, 128), F32), vm((1, 128), F32), vm((1, 128), F32), vm((128, model), BF16),
        vm((128, model), BF16), vm((1, model), F32),
        vm((rows, 256), F32), vm((rows, 256), F32), vm((rows, 512), F32), vm((rows, 128), F32),
        vm((QK + VDIM, rows), BF16), vm((QK, rows), BF16), vm((rows, 128), BF16),
        vm((rows, 128), F32), vm((NZ, QK + VDIM, rows), BF16), vm((NX, QK, rows), BF16),
        vm((16, 128), BF16), vm((16 + rows, 128), F32), vm((NX, 1, rows), F32),
        vm((NX, 1, rows), F32), vm((NX, VDIM, rows), F32), vm((rows, 128), F32),
        vm((rows, 128), F32),
        vm((2, 128), F32), vm((NX, 2, 128), F32), vm((2, 128), F32), vm((NZ, 2, 128), F32),
        vm((NX - 1, VDIM, rows), BF16), vm((NX - 1, 2, rows), F32),
        vm((NX - 1, VDIM, rows), BF16), vm((NX - 1, 2, rows), F32),
        vm((rows, 128), BF16), vm((rows, 128), BF16), vm((2, rows), F32),
        vm((NT - 1, 2, rows), F32), vm((2, rows, 128), F32),
        vm((1, mine, model), F32),
        dma((len(LOADS),)), pltpu.SemaphoreType.REGULAR((9,)),
        dma((13,)), dma((13,)), dma((8 * PIECES,)), dma((8 * PIECES,)),
        dma((NX - 1,)), dma((NX - 1,)), dma((2,)), dma((NX - 1,)), dma((NX - 1,)),
        dma((8,)), dma((8,)), dma((NX - 1,)), dma((NX - 1,)), dma((NX - 1,)), dma((NX - 1,)),
        dma((NT - 1,)), dma((NT - 1,)),
    ]
    for _ in range(2):
        scratch += [
            vm((NY, mine, model), BF16), vm((NY, mine, model), BF16), vm((NY, mine, model), F32),
            vm((mine, model), BF16), vm((mine, model), BF16),
            vm((2, mine, model), BF16), vm((2, mine, model), BF16),
        ]
    for _ in range(2):
        scratch += [dma((NY,)), dma((NY,)), dma((2,)), dma((2,)), dma((4,)), dma((4,))]
    return pl.pallas_call(
        layer,
        name="layer",
        out_shape=jax.ShapeDtypeStruct((mine, model), BF16),
        in_specs=[pl.BlockSpec(memory_space=pl.ANY)] * len(LOADS),
        out_specs=pl.BlockSpec(memory_space=pltpu.VMEM),
        scratch_shapes=scratch,
        compiler_params=pltpu.CompilerParams(
            collective_id=0, has_side_effects=True, vmem_limit_bytes=63 * 1024 * 1024
        ),
    )(*operands)


def shards(
    tokens, pre_gain, rate_factor, w_rec_in, w_rec_gate, conv_taps, rate_maps, input_maps,
    decay_param, w_query, w_latent, w_rope_key, latent_gain, w_expand, rec_gain, att_gain,
    w_out_rec, w_out_att, post_gain,
):
    rows = tokens.shape[0]
    frequency = 1.0 / THETA ** (jnp.arange(0, ROPE, 2).astype(F32) / ROPE)
    places = (lax.axis_index("sp") * rows + jnp.arange(rows)).astype(F32)
    turned = places[None, :] * frequency[:, None]
    given = {
        "tok": tokens, "gain": pre_gain[None], "w_in": w_rec_in, "w_gate": w_rec_gate,
        "w_q": w_query.T, "w_rope": w_rope_key.T, "w_lat": w_latent, "w_exp": w_expand,
        "lat_gain": latent_gain[None], "cos": jnp.cos(turned), "sin": jnp.sin(turned),
        "rf": rate_factor[None], "taps": conv_taps, "rmap": rate_maps[0], "imap": input_maps[0],
        "decay": decay_param[None], "rgain": rec_gain[None], "again": att_gain[None],
        "w_rec": w_out_rec, "w_att": w_out_att, "post": post_gain[None],
    }
    return call_layer(*(given[name] for name in LOADS))


def solution(mesh):
    placed = (
        P("sp", "tp"), P(), P("sp"), P(None, "tp"), P(None, "tp"), P(None, "tp"),
        P("tp", None, None), P("tp", None, None), P("tp"), P(None, "tp"), P(), P(), P(),
        P(None, "tp"), P("tp"), P("tp"), P("tp", None), P("tp", None), P(),
    )
    return jax.shard_map(
        shards, mesh=mesh, in_specs=placed, out_specs=P(("sp", "tp"), None), check_vma=False
    )
```

```python
import math

import jax
import jax.numpy as jnp
import numpy as np
from jax import lax
from jax.experimental import pallas as pl
from jax.experimental.pallas import tpu as pltpu
from jax.sharding import PartitionSpec as P

NOPE = 128
ROPE = 64
VDIM = 128
EPS = 1e-06
RATE_C = 8.0
THETA = 10000.0
NY, NX, NZ = 4, 4, 8
NT = 2 * NY
PIECES = 4
LOW = -1e30
MESH = pl.DeviceIdType.MESH
F32, BF16 = jnp.float32, jnp.bfloat16
QK = NOPE + ROPE


def remote(src, dst, send, recv, where):
    return pltpu.make_async_remote_copy(
        src_ref=src, dst_ref=dst, send_sem=send, recv_sem=recv, device_id=where, device_id_type=MESH
    )


def greet(partners):
    barrier = pltpu.get_barrier_semaphore()
    for where in partners:
        pl.semaphore_signal(barrier, inc=1, device_id=where, device_id_type=MESH)
    pl.semaphore_wait(barrier, len(partners))


def hello(sem, where):
    pl.semaphore_signal(sem, inc=1, device_id=where, device_id_type=MESH)


def mm(a, b):
    return jnp.dot(a, b, preferred_element_type=F32)


def mm_t(a, b):
    return lax.dot_general(a, b, (((1,), (1,)), ((), ())), preferred_element_type=F32)


def shifted(values, by, fill):
    row = lax.broadcasted_iota(jnp.int32, values.shape, 0)
    return jnp.where(row < by, fill, pltpu.roll(values, by, 0))


def minus_expm1(x):
    series = 1.0 + x * (1.0 / 7.0)
    for n in (6.0, 5.0, 4.0, 3.0, 2.0):
        series = 1.0 + (x * (1.0 / n)) * series
    return jnp.where(x > -0.25, -x * series, 1.0 - jnp.exp(x))


def softplus(x):
    small = jnp.exp(-jnp.abs(x))
    t = small / (2.0 + small)
    t2 = t * t
    series = 1.0 / 17.0
    for n in (15.0, 13.0, 11.0, 9.0, 7.0, 5.0, 3.0, 1.0):
        series = 1.0 / n + t2 * series
    return jnp.maximum(x, 0.0) + 2.0 * t * series


LOADS = (
    "tok", "gain", "w_in", "w_gate", "w_q", "w_rope", "w_lat", "w_exp", "lat_gain", "freq",
    "rf", "taps", "rmap", "imap", "decay", "rgain", "again", "w_rec", "w_att", "post",
)


def layer(*refs):
    n_in = len(LOADS)
    src = dict(zip(LOADS, refs[:n_in]))
    out_ref = refs[n_in]
    (
        tok, gain, v_ig, v_qr, v_lat, v_exp, lat_gain, freq, cos_s, sin_s, rf, taps, rmap, imap, decay,
        rgain, again, w_rec, w_att, post,
        a_ig, a_qr, a_lat, sq,
        own_kv, own_q, rec_s, gate_s, kv, qs, halo, ext, m_s, l_s, o_s, cum_s, loc_s,
        mine_x, cx, mine_z, cz, po, ps, go, gs,
        sums, got_s, inv_s, part,
        lsem, hi, ass, ars, kss, krs, qss, qrs, hsem, xss, xrs, zss, zrs, oss, ors, tss, trs,
        sss, srs, wss, wrs, *rest,
    ) = refs[n_in + 1 :]
    r_bufs, t_bufs = rest[0:8], rest[8:16]
    r_sems, t_sems = rest[16:22], rest[22:28]

    sp, tp = lax.axis_index("sp"), lax.axis_index("tp")
    z, x = sp // NX, sp % NX
    y, c = tp // 2, tp % 2

    def at_tp(yy, cc):
        return yy * 2 + cc

    sib = at_tp(y, 1 - c)
    up, dn, far = (at_tp((y + d) % NY, c) for d in (1, 3, 2))
    up_sib, dn_sib, far_sib = (at_tp((y + d) % NY, 1 - c) for d in (1, 3, 2))

    def at_zx(zz, xx):
        return {"sp": zz * NX + xx}

    zup, zdn = at_zx((z + 1) % NZ, x), at_zx((z + NZ - 1) % NZ, x)
    xs = {d: at_zx(z, (x + d) % NX) for d in range(1, NX)}

    rows, depth = tok.shape[1], tok.shape[2]
    model = depth * NT
    half = rows // 2

    mine_rows = pl.ds(pl.multiple_of(c * 128, 128), 128)
    where = {
        "tok": tok.at[tp], "gain": gain, "w_in": v_ig.at[:, pl.ds(0, 128)],
        "w_gate": v_ig.at[:, pl.ds(128, 128)], "w_q": v_qr.at[pl.ds(0, QK)],
        "w_rope": v_qr.at[pl.ds(QK, ROPE)], "w_lat": v_lat, "w_exp": v_exp, "lat_gain": lat_gain,
        "freq": freq, "rf": rf, "taps": taps, "rmap": rmap, "imap": imap,
        "decay": decay, "rgain": rgain, "again": again, "w_rec": w_rec.at[mine_rows], "w_att": w_att.at[mine_rows], "post": post,
    }
    load = {
        name: pltpu.make_async_copy(src[name], where[name], lsem.at[k])
        for k, name in enumerate(LOADS)
    }
    load["tok"].start()
    greet([{"tp": sib}, {"tp": up}, {"tp": dn}, xs[1], xs[3], zup, zdn])
    hello(hi.at[0], xs[3])
    hello(hi.at[1], {"tp": dn})
    hello(hi.at[2], {"tp": sib})
    hello(hi.at[4], zdn)
    hello(hi.at[5], zup)

    sent = []

    def go_send(copy):
        copy.start()
        sent.append(copy)

    h0, h1, whole = pl.ds(0, half), pl.ds(half, half), pl.ds(0, rows)

    def tok_msg(k, slot, piece, to):
        at = tok.at[slot, piece]
        return remote(at, at, ass.at[k], ars.at[k], {"tp": to})

    def send(k, slot, piece, to):
        go_send(tok_msg(k, slot, piece, to))

    def arrived(k, slot, piece):
        tok_msg(k, slot, piece, sib).wait_recv()

    load["tok"].wait()
    send(1, tp, h0, up)
    send(3, tp, h1, dn)
    send(0, tp, whole, sib)
    send(2, tp, h1, up)
    send(4, tp, h0, dn)
    for name in LOADS[1:]:
        load[name].start()

    def chunk(source, first=False):
        wide = tok[source].astype(F32)
        square = wide * wide
        folded = square[:, 0:128]
        for k in range(1, depth // 128):
            folded = folded + square[:, k * 128 : (k + 1) * 128]
        at = pl.ds(pl.multiple_of(source * depth, depth), depth)
        low = (wide * gain[:, at]).astype(BF16)
        ig, qr, lat = mm(low, v_ig[at, :]), mm_t(low, v_qr[:, at]), mm(low, v_lat[at, :])
        if first:
            sq[...], a_ig[...], a_qr[...], a_lat[...] = folded, ig, qr, lat
        else:
            sq[...] += folded
            a_ig[...] += ig
            a_qr[...] += qr
            a_lat[...] += lat

    for name in ("gain", "w_in", "w_gate", "w_q", "w_rope", "w_lat"):
        load[name].wait()
    chunk(tp, True)
    pl.semaphore_wait(hi.at[2], 1)
    hello(hi.at[3], {"tp": dn})
    pl.semaphore_wait(hi.at[4], 1)
    hello(hi.at[6], zdn)
    pl.semaphore_wait(hi.at[5], 1)
    hello(hi.at[7], zup)
    arrived(0, sib, whole)
    chunk(sib)
    for name in LOADS[7:]:
        load[name].wait()
    places = lax.broadcasted_iota(jnp.int32, (ROPE // 2, rows), 1) + sp * rows
    angle = places.astype(F32) * freq[...]
    cos_s[...] = jnp.cos(angle)
    sin_s[...] = jnp.sin(angle)
    arrived(1, dn, h0)
    send(5, dn, h0, up)
    send(7, dn, h0, sib)
    arrived(3, up, h1)
    send(6, up, h1, dn)
    send(9, up, h1, sib)
    arrived(2, dn, h1)
    send(8, dn, h1, sib)
    arrived(4, up, h0)
    send(10, up, h0, sib)
    chunk(dn)
    pl.semaphore_wait(hi.at[6], 1)
    hello(hi.at[8], zdn)
    pl.semaphore_wait(hi.at[7], 1)
    chunk(up)
    arrived(7, dn_sib, h0)
    arrived(8, dn_sib, h1)
    chunk(dn_sib)
    arrived(9, up_sib, h1)
    arrived(10, up_sib, h0)
    chunk(up_sib)
    arrived(5, far, h0)
    send(11, far, h0, sib)
    arrived(6, far, h1)
    send(12, far, h1, sib)
    chunk(far)
    arrived(11, far_sib, h0)
    arrived(12, far_sib, h1)
    chunk(far_sib)

    inverse = lax.rsqrt(jnp.sum(sq[...], axis=1, keepdims=True) / model + EPS)
    rec_s[...] = (inverse * a_ig[:, 0:128]).astype(BF16)
    succ = {"sp": (sp + 1) % (NX * NZ)}
    tail = rows - 16
    pl.semaphore_wait(hi.at[0], 1)
    mine_tail = remote(rec_s.at[pl.ds(tail, 16)], halo, hsem.at[0], hsem.at[1], succ)
    go_send(mine_tail)
    latent = inverse * a_lat[...]
    spread = lax.rsqrt(jnp.mean(latent * latent, axis=1, keepdims=True) + EPS)
    latent = (latent * spread * lat_gain[...]).astype(BF16)
    expanded = mm(latent, v_exp[...]).T
    turned = (inverse * a_qr[:, NOPE:]).T
    cosine, sine = cos_s[...], sin_s[...]
    hr = ROPE // 2
    u, w = turned[ROPE : ROPE + hr], turned[ROPE + hr :]
    own_kv[0:NOPE, :] = expanded[0:NOPE].astype(BF16)
    own_kv[NOPE : NOPE + hr, :] = (u * cosine - w * sine).astype(BF16)
    own_kv[NOPE + hr : QK, :] = (w * cosine + u * sine).astype(BF16)
    own_kv[QK:, :] = expanded[NOPE:].astype(BF16)

    size = (QK + VDIM) // PIECES

    def piece_at(p):
        return pl.ds(p * size, size)

    def kv_msg(source, direction, hop, p):
        k = (direction * 4 + hop - 1) * PIECES + p
        slot = (z + (NZ - hop + 1 if direction == 0 else hop - 1)) % NZ
        return remote(
            source, kv.at[slot, piece_at(p)], kss.at[k], krs.at[k], zup if direction == 0 else zdn
        )

    def kv_goes(direction, hop, p):
        return hop < 4 or (hop == 4 and (direction == 0) == (p < PIECES // 2))

    def piece(direction, i):
        return (i + 2 * direction) % PIECES

    for i in range(PIECES):
        for direction in (0, 1):
            p = piece(direction, i)
            go_send(kv_msg(own_kv.at[piece_at(p)], direction, 1, p))

    def w_msg(weight, k):
        at = weight.at[mine_rows]
        return remote(at, at, wss.at[k], wrs.at[k], {"tp": sib})

    go_send(w_msg(w_rec, 0))
    go_send(w_msg(w_att, 1))

    u, w = turned[0:hr], turned[hr:ROPE]
    own_q[0:NOPE, :] = (inverse * a_qr[:, 0:NOPE]).T.astype(BF16)
    own_q[NOPE : NOPE + hr, :] = (u * cosine - w * sine).astype(BF16)
    own_q[NOPE + hr :, :] = (w * cosine + u * sine).astype(BF16)

    def q_msg(d, slot):
        return remote(own_q, qs.at[slot], qss.at[d - 1], qrs.at[d - 1], xs[d])

    go_send(q_msg(1, x))
    go_send(q_msg(3, x))
    gate_s[...] = inverse * a_ig[:, 128:256]
    pl.semaphore_wait(hi.at[1], 1)
    pl.semaphore_wait(hi.at[8], 1)

    for xx in range(NX):
        m_s[xx] = jnp.full((1, rows), LOW, F32)
        l_s[xx] = jnp.zeros((1, rows), F32)
        o_s[xx] = jnp.zeros((VDIM, rows), F32)

    scale = math.log2(math.e) / math.sqrt(QK)

    def attend(slots, queries, keys, values, masked):
        scores = [mm(keys, query) * scale for query in queries]
        if masked:
            key = lax.broadcasted_iota(jnp.int32, scores[0].shape, 0)
            place = lax.broadcasted_iota(jnp.int32, scores[0].shape, 1)
            scores = [jnp.where(key <= place, s, LOW) for s in scores]
        before = [m_s[k] for k in slots]
        most = [jnp.maximum(b, jnp.max(s, axis=0, keepdims=True)) for b, s in zip(before, scores)]
        weights = [jnp.exp2(s - m) for s, m in zip(scores, most)]
        shrink = [jnp.exp2(b - m) for b, m in zip(before, most)]
        for k, m, s, wt in zip(slots, most, shrink, weights):
            m_s[k] = m
            l_s[k] = l_s[k] * s + jnp.sum(wt, axis=0, keepdims=True)
        for k, s, wt in zip(slots, shrink, weights):
            o_s[k] = o_s[k] * s + mm(values, wt.astype(BF16))

    def unit(slot):
        attend(
            range(NX), [qs[k] for k in range(NX)], kv[slot, 0:QK, :].T, kv[slot, QK:, :], False
        )

    def poll(hop, pieces):
        for i in pieces:
            for direction in (0, 1):
                p = piece(direction, i)
                if kv_goes(direction, hop, p):
                    slot = (z + (NZ - hop if direction == 0 else hop)) % NZ
                    here = kv.at[slot, piece_at(p)]
                    k = (direction * 4 + hop - 1) * PIECES + p
                    remote(here, here, kss.at[k], krs.at[k], zup).wait_recv()
                    if kv_goes(direction, hop + 1, p):
                        go_send(kv_msg(here, direction, hop + 1, p))

    first_half, second_half = (0, 1), (2, 3)

    def against(slot):
        @pl.when(slot < z)
        def _():
            unit(slot)

    def below(hop):
        against((z + NZ - hop) % NZ)

    def above(hop):
        against((z + hop) % NZ)

    order = [(y + 2) % NY, (y + 1) % NY, (y + 3) % NY, y]
    mine = out_ref.shape[0]
    middle = model // 2
    left, right = pl.ds(0, middle), pl.ds(middle, middle)

    def rows_of(yy, cc):
        return pl.ds(pl.multiple_of((yy * 2 + cc) * mine, mine), mine)

    class Branch:
        def __init__(self, weight, k, bufs, sems):
            self.weight, self.k = weight, k
            self.natural, self.out, self.act, self.own, self.f_out, self.f_in, self.n_out, self.n_in = bufs
            self.ps, self.pr, self.fs, self.fr, self.ns, self.nr = sems

        def pair(self):
            at = self.act.at[:, mine_rows]
            return remote(self.out, at, self.ps.at[0], self.pr.at[0], {"tp": sib})

        def far(self, k):
            cols, to = ((left, up), (right, dn))[k]
            return remote(
                self.f_out.at[:, cols], self.f_in.at[:, cols], self.fs.at[k], self.fr.at[k], {"tp": to}
            )

        def near(self, k):
            side, cols = ((0, right), (1, left), (0, left), (1, right))[k]
            at = (side, slice(None), cols)
            return remote(
                self.n_out.at[at], self.n_in.at[at], self.ns.at[k], self.nr.at[k],
                {"tp": (up, dn)[side]},
            )

        def begin(self, value):
            self.natural[...] = value
            for k, yy in enumerate(order):
                at = slice(k * mine, (k + 1) * mine)
                self.out[at, :] = self.natural[rows_of(yy, 1 - c), :]
                self.act[at, mine_rows] = self.natural[rows_of(yy, c), :]
            go_send(self.pair())

        def send_far(self):
            w_msg(self.weight, self.k).wait_recv()
            self.pair().wait_recv()
            self.f_out[...] = mm(self.act[0:mine, :], self.weight[...]).astype(BF16)
            go_send(self.far(0))
            go_send(self.far(1))

        def send_pure(self):
            self.own[...] = mm(self.act[mine:, :], self.weight[...])
            self.n_out[0, :, middle:] = self.own[0:mine, middle:].astype(BF16)
            go_send(self.near(0))
            self.n_out[1, :, 0:middle] = self.own[mine : 2 * mine, 0:middle].astype(BF16)
            go_send(self.near(1))

        def send_joined(self):
            self.far(0).wait_recv()
            joined = self.own[0:mine, 0:middle] + self.f_in[:, 0:middle].astype(F32)
            self.n_out[0, :, 0:middle] = joined.astype(BF16)
            go_send(self.near(2))
            self.far(1).wait_recv()
            joined = self.own[mine : 2 * mine, middle:] + self.f_in[:, middle:].astype(F32)
            self.n_out[1, :, middle:] = joined.astype(BF16)
            go_send(self.near(3))

        def total(self):
            for k in range(4):
                self.near(k).wait_recv()
            return self.own[2 * mine :, :] + self.n_in[0].astype(F32) + self.n_in[1].astype(F32)

    branch_r = Branch(w_rec, 0, r_bufs, r_sems)
    branch_t = Branch(w_att, 1, t_bufs, t_sems)

    ext[16:, :] = rec_s[...].astype(F32)
    attend((x,), [own_q[...]], own_kv[0:QK, :].T, own_kv[QK:, :], True)
    mine_tail.wait_recv()
    ext[0:16, :] = jnp.where(sp == 0, 0.0, halo[...].astype(F32))
    convolved = taps[0:1, :] * ext[13 : 13 + rows, :]
    for k in range(1, 4):
        convolved = convolved + taps[k : k + 1, :] * ext[13 + k : 13 + k + rows, :]
    conv_low = convolved.astype(BF16)
    rate = jax.nn.sigmoid(mm(conv_low, rmap[...]))
    entry = jax.nn.sigmoid(mm(conv_low, imap[...]))
    factor = jnp.broadcast_to(rf[...], (128, rows)).T
    log_keep = (-RATE_C) * factor * rate * softplus(-decay[...])
    cum = jnp.exp(log_keep)
    local = jnp.sqrt(minus_expm1(2.0 * log_keep)) * entry * convolved
    step = 1
    while step < rows:
        local = local + cum * shifted(local, step, 0.0)
        cum = cum * shifted(cum, step, 1.0)
        step *= 2
    cum_s[...] = cum
    loc_s[...] = local
    mine_x[0:1, :] = cum[rows - 1 :]
    mine_x[1:2, :] = local[rows - 1 :]

    def x_msg(d, slot):
        return remote(mine_x, cx.at[slot], xss.at[d - 1], xrs.at[d - 1], xs[d])

    for d in (2, 1, 3):
        go_send(x_msg(d, x))
    go_send(q_msg(2, x))
    poll(1, first_half)

    cx[x] = mine_x[...]
    for d in range(1, NX):
        x_msg(d, (x + NX - d) % NX).wait_recv()
    pa, pb = jnp.ones((1, 128), F32), jnp.zeros((1, 128), F32)
    ta, tb = pa, pb
    for i in range(NX):
        a, b = cx[i, 0:1, :], cx[i, 1:2, :]
        ta, tb = ta * a, a * tb + b
        pa = jnp.where(i < x, pa * a, pa)
        pb = jnp.where(i < x, a * pb + b, pb)
    mine_z[0:1, :] = ta
    mine_z[1:2, :] = tb

    def z_msg(d, slot):
        to = at_zx((z + d) % NZ, x)
        return remote(mine_z, cz.at[slot], zss.at[d - 1], zrs.at[d - 1], to)

    for d in (4, 3, 5, 2, 6, 1, 7):
        go_send(z_msg(d, z))

    poll(1, second_half)
    poll(2, first_half)
    qs[x] = own_q[...]
    for d in (1, 3, 2):
        q_msg(d, (x + NX - d) % NX).wait_recv()
    for xx in range(1, NX):

        @pl.when(x < xx)
        def _():
            attend((xx,), [qs[xx]], own_kv[0:QK, :].T, own_kv[QK:, :], False)

    cz[z] = mine_z[...]
    for d in range(1, NZ):
        z_msg(d, (z + NZ - d) % NZ).wait_recv()
    entering = jnp.zeros((1, 128), F32)
    for i in range(NZ):
        entering = jnp.where(i < z, cz[i, 0:1, :] * entering + cz[i, 1:2, :], entering)
    entering = pa * entering + pb
    state = loc_s[...] + cum_s[...] * entering
    rec = state * jax.nn.gelu(gate_s[...])
    branch_r.begin((rec * rgain[...]).astype(BF16))
    square = (rec * rec).T
    sums[0:1, :] = jnp.sum(square, axis=0, keepdims=True)
    poll(2, second_half)
    below(1)
    branch_r.send_far()
    poll(3, first_half)
    branch_r.send_pure()
    above(1)
    poll(3, second_half)
    below(2)
    above(2)
    below(3)
    above(3)
    poll(4, first_half)
    poll(4, second_half)
    below(4)

    def o_msg(d):
        return remote(po.at[d - 1], go.at[d - 1], oss.at[d - 1], ors.at[d - 1], xs[d])

    def s_msg(d):
        return remote(ps.at[d - 1], gs.at[d - 1], tss.at[d - 1], trs.at[d - 1], xs[d])

    for d in (2, 1, 3):
        xx = (x + d) % NX
        total = l_s[xx]
        ps[d - 1, 0:1, :] = m_s[xx]
        ps[d - 1, 1:2, :] = total
        po[d - 1] = (o_s[xx] / jnp.where(total > 0.0, total, 1.0)).astype(BF16)
        go_send(s_msg(d))
        go_send(o_msg(d))

    branch_r.send_joined()

    most = m_s[x]
    for d in range(1, NX):
        s_msg(d).wait_recv()
        most = jnp.maximum(most, gs[d - 1, 0:1, :])
    share = jnp.exp2(m_s[x] - most)
    total = l_s[x] * share
    out = o_s[x] * share
    for d in range(1, NX):
        o_msg(d).wait_recv()
        share = gs[d - 1, 1:2, :] * jnp.exp2(gs[d - 1, 0:1, :] - most)
        total = total + share
        out = out + go[d - 1].astype(F32) * share
    out = out / total
    sums[1:2, :] = jnp.sum(out * out, axis=0, keepdims=True)

    def sum_msg(d):
        return remote(sums, got_s.at[d - 1], sss.at[d - 1], srs.at[d - 1], {"tp": (tp + d) % NT})

    pl.semaphore_wait(hi.at[3], 1)
    for d in (4, 3, 5, 2, 6, 1, 7):
        go_send(sum_msg(d))
    branch_t.begin((out.T * again[...]).astype(BF16))
    branch_t.send_far()
    branch_t.send_pure()
    total = sums[...]
    for d in range(1, NT):
        sum_msg(d).wait_recv()
        total = total + got_s[d - 1]
    inverse = lax.rsqrt(total / (128 * NT) + EPS)
    inv_s[0] = jnp.broadcast_to(inverse[0:1, :], (128, rows)).T
    inv_s[1] = jnp.broadcast_to(inverse[1:2, :], (128, rows)).T
    at = rows_of(y, c)
    part[0] = branch_r.total() * inv_s[0, at, :][:, 0:1]
    branch_t.send_joined()
    mixed = part[0] + branch_t.total() * inv_s[1, at, :][:, 0:1]
    spread = lax.rsqrt(jnp.mean(mixed * mixed, axis=1, keepdims=True) + EPS)
    out_ref[...] = (mixed * spread * post[...]).astype(BF16)
    for copy in sent:
        copy.wait_send()


def call_layer(*operands):
    rows, depth = operands[0].shape
    model = depth * NT
    mine = rows // NT
    dma = pltpu.SemaphoreType.DMA
    vm = pltpu.VMEM
    scratch = [
        vm((NT, rows, depth), BF16), vm((1, model), F32), vm((model, 256), BF16),
        vm((QK + ROPE, model), BF16), vm((model, 512), BF16), vm((512, NOPE + VDIM), BF16),
        vm((1, 512), F32), vm((ROPE // 2, rows), F32), vm((ROPE // 2, rows), F32), vm((ROPE // 2, rows), F32),
        vm((1, rows), F32), vm((4, 128), F32), vm((128, 128), BF16), vm((128, 128), BF16),
        vm((1, 128), F32), vm((1, 128), F32), vm((1, 128), F32), vm((256, model), BF16),
        vm((256, model), BF16), vm((1, model), F32),
        vm((rows, 256), F32), vm((rows, 256), F32), vm((rows, 512), F32), vm((rows, 128), F32),
        vm((QK + VDIM, rows), BF16), vm((QK, rows), BF16), vm((rows, 128), BF16),
        vm((rows, 128), F32), vm((NZ, QK + VDIM, rows), BF16), vm((NX, QK, rows), BF16),
        vm((16, 128), BF16), vm((16 + rows, 128), F32), vm((NX, 1, rows), F32),
        vm((NX, 1, rows), F32), vm((NX, VDIM, rows), F32), vm((rows, 128), F32),
        vm((rows, 128), F32),
        vm((2, 128), F32), vm((NX, 2, 128), F32), vm((2, 128), F32), vm((NZ, 2, 128), F32),
        vm((NX - 1, VDIM, rows), BF16), vm((NX - 1, 2, rows), F32),
        vm((NX - 1, VDIM, rows), BF16), vm((NX - 1, 2, rows), F32),
        vm((2, rows), F32),
        vm((NT - 1, 2, rows), F32), vm((2, rows, 128), F32),
        vm((1, mine, model), F32),
        dma((len(LOADS),)), pltpu.SemaphoreType.REGULAR((9,)),
        dma((13,)), dma((13,)), dma((8 * PIECES,)), dma((8 * PIECES,)),
        dma((NX - 1,)), dma((NX - 1,)), dma((2,)), dma((NX - 1,)), dma((NX - 1,)),
        dma((8,)), dma((8,)), dma((NX - 1,)), dma((NX - 1,)), dma((NX - 1,)), dma((NX - 1,)),
        dma((NT - 1,)), dma((NT - 1,)), dma((2,)), dma((2,)),
    ]
    for _ in range(2):
        scratch += [
            vm((rows, 128), BF16), vm((NY * mine, 128), BF16), vm((NY * mine, 256), BF16),
            vm((3 * mine, model), F32),
            vm((mine, model), BF16), vm((mine, model), BF16),
            vm((2, mine, model), BF16), vm((2, mine, model), BF16),
        ]
    for _ in range(2):
        scratch += [dma((1,)), dma((1,)), dma((2,)), dma((2,)), dma((4,)), dma((4,))]
    return pl.pallas_call(
        layer,
        name="layer",
        out_shape=pltpu.VMEM((mine, model), BF16),
        in_specs=[pl.BlockSpec(memory_space=pl.ANY)] * len(LOADS),
        out_specs=pl.BlockSpec(memory_space=pltpu.VMEM),
        scratch_shapes=scratch,
        compiler_params=pltpu.CompilerParams(
            collective_id=0, has_side_effects=True, vmem_limit_bytes=63 * 1024 * 1024
        ),
    )(*operands)


def shards(
    tokens, pre_gain, rate_factor, w_rec_in, w_rec_gate, conv_taps, rate_maps, input_maps,
    decay_param, w_query, w_latent, w_rope_key, latent_gain, w_expand, rec_gain, att_gain,
    w_out_rec, w_out_att, post_gain,
):
    rows = tokens.shape[0]
    power = np.arange(0, ROPE, 2).astype(np.float32) / np.float32(ROPE)
    frequency = np.float32(1.0) / np.float32(THETA) ** power
    frequency = np.repeat(frequency[:, None], rows, axis=1)
    given = {
        "tok": tokens, "gain": pre_gain[None], "w_in": w_rec_in, "w_gate": w_rec_gate,
        "w_q": w_query.T, "w_rope": w_rope_key.T, "w_lat": w_latent, "w_exp": w_expand,
        "lat_gain": latent_gain[None], "freq": jnp.asarray(frequency),
        "rf": rate_factor[None], "taps": conv_taps, "rmap": rate_maps[0], "imap": input_maps[0],
        "decay": decay_param[None], "rgain": rec_gain[None], "again": att_gain[None],
        "w_rec": w_out_rec, "w_att": w_out_att, "post": post_gain[None],
    }
    return call_layer(*(given[name] for name in LOADS))


def solution(mesh):
    placed = (
        P("sp", "tp"), P(), P("sp"), P(None, "tp"), P(None, "tp"), P(None, "tp"),
        P("tp", None, None), P("tp", None, None), P("tp"), P(None, "tp"), P(), P(), P(),
        P(None, "tp"), P("tp"), P("tp"), P("tp", None), P("tp", None), P(),
    )
    return jax.shard_map(
        shards, mesh=mesh, in_specs=placed, out_specs=P(("sp", "tp"), None), check_vma=False
    )
```

```python
import math

import jax
import jax.numpy as jnp
import numpy as np
from jax import lax
from jax.experimental import pallas as pl
from jax.experimental.pallas import tpu as pltpu
from jax.sharding import PartitionSpec as P

NOPE = 128
ROPE = 64
VDIM = 128
EPS = 1e-06
RATE_C = 8.0
THETA = 10000.0
NY, NX, NZ = 4, 4, 8
NT = 2 * NY
PIECES = 4
LOW = -1e30
MESH = pl.DeviceIdType.MESH
F32, BF16 = jnp.float32, jnp.bfloat16
QK = NOPE + ROPE


def remote(src, dst, send, recv, where):
    return pltpu.make_async_remote_copy(
        src_ref=src, dst_ref=dst, send_sem=send, recv_sem=recv, device_id=where, device_id_type=MESH
    )


def greet(partners):
    barrier = pltpu.get_barrier_semaphore()
    for where in partners:
        pl.semaphore_signal(barrier, inc=1, device_id=where, device_id_type=MESH)
    pl.semaphore_wait(barrier, len(partners))


def hello(sem, where):
    pl.semaphore_signal(sem, inc=1, device_id=where, device_id_type=MESH)


def mm(a, b):
    return jnp.dot(a, b, preferred_element_type=F32)


def mm_t(a, b):
    return lax.dot_general(a, b, (((1,), (1,)), ((), ())), preferred_element_type=F32)


def shifted(values, by, fill):
    row = lax.broadcasted_iota(jnp.int32, values.shape, 0)
    return jnp.where(row < by, fill, pltpu.roll(values, by, 0))


def minus_expm1(x):
    series = 1.0 + x * (1.0 / 7.0)
    for n in (6.0, 5.0, 4.0, 3.0, 2.0):
        series = 1.0 + (x * (1.0 / n)) * series
    return jnp.where(x > -0.25, -x * series, 1.0 - jnp.exp(x))


def softplus(x):
    small = jnp.exp(-jnp.abs(x))
    t = small / (2.0 + small)
    t2 = t * t
    series = 1.0 / 17.0
    for n in (15.0, 13.0, 11.0, 9.0, 7.0, 5.0, 3.0, 1.0):
        series = 1.0 / n + t2 * series
    return jnp.maximum(x, 0.0) + 2.0 * t * series


LOADS = (
    "tok", "gain", "w_in", "w_gate", "w_q", "w_rope", "w_lat", "w_exp", "lat_gain", "freq",
    "rf", "taps", "rmap", "imap", "decay", "rgain", "again", "w_rec", "w_att", "post",
)


def layer(*refs):
    n_in = len(LOADS)
    src = dict(zip(LOADS, refs[:n_in]))
    out_ref = refs[n_in]
    (
        tok, gain, v_ig, v_qr, v_lat, v_exp, lat_gain, freq, cos_s, sin_s, cos_q, sin_q, rf, taps, rmap, imap, decay,
        rgain, again, w_rec, w_att, post,
        a_ig, a_qr, a_lat, sq,
        own_kv, own_q, rec_s, gate_s, kv, qs, halo, ext, m_s, l_s, o_s, cum_s, loc_s,
        mine_x, cx, mine_z, cz, po, ps, go, gs,
        sums, got_s, inv_s, sums_t, got_t, inv_t, both, part,
        lsem, hi, ass, ars, kss, krs, qss, qrs, hsem, xss, xrs, zss, zrs, oss, ors, tss, trs,
        sss, srs, wss, wrs, uss, urs, *rest,
    ) = refs[n_in + 1 :]
    r_bufs, t_bufs = rest[0:8], rest[8:16]
    r_sems, t_sems = rest[16:22], rest[22:28]

    sp, tp = lax.axis_index("sp"), lax.axis_index("tp")
    z, x = sp // NX, sp % NX
    y, c = tp // 2, tp % 2

    def at_tp(yy, cc):
        return yy * 2 + cc

    sib = at_tp(y, 1 - c)
    up, dn, far = (at_tp((y + d) % NY, c) for d in (1, 3, 2))
    up_sib, dn_sib, far_sib = (at_tp((y + d) % NY, 1 - c) for d in (1, 3, 2))

    def at_zx(zz, xx):
        return {"sp": zz * NX + xx}

    zup, zdn = at_zx((z + 1) % NZ, x), at_zx((z + NZ - 1) % NZ, x)
    xs = {d: at_zx(z, (x + d) % NX) for d in range(1, NX)}

    rows, depth = tok.shape[1], tok.shape[2]
    model = depth * NT
    half = rows // 2

    mine_rows = pl.ds(pl.multiple_of(c * 128, 128), 128)
    where = {
        "tok": tok.at[tp], "gain": gain, "w_in": v_ig.at[:, pl.ds(0, 128)],
        "w_gate": v_ig.at[:, pl.ds(128, 128)], "w_q": v_qr.at[pl.ds(0, QK)],
        "w_rope": v_qr.at[pl.ds(QK, ROPE)], "w_lat": v_lat, "w_exp": v_exp, "lat_gain": lat_gain,
        "freq": freq, "rf": rf, "taps": taps, "rmap": rmap, "imap": imap,
        "decay": decay, "rgain": rgain, "again": again.at[c], "w_rec": w_rec.at[mine_rows], "w_att": w_att.at[mine_rows], "post": post,
    }
    load = {
        name: pltpu.make_async_copy(src[name], where[name], lsem.at[k])
        for k, name in enumerate(LOADS)
    }
    load["tok"].start()
    greet([{"tp": sib}, {"tp": up}, {"tp": dn}, xs[1], xs[3], zup, zdn])
    hello(hi.at[0], xs[3])
    hello(hi.at[1], {"tp": dn})
    hello(hi.at[2], {"tp": sib})
    hello(hi.at[4], zdn)
    hello(hi.at[5], zup)

    sent = []

    def go_send(copy):
        copy.start()
        sent.append(copy)

    h0, h1, whole = pl.ds(0, half), pl.ds(half, half), pl.ds(0, rows)

    def tok_msg(k, slot, piece, to):
        at = tok.at[slot, piece]
        return remote(at, at, ass.at[k], ars.at[k], {"tp": to})

    def send(k, slot, piece, to):
        go_send(tok_msg(k, slot, piece, to))

    def arrived(k, slot, piece):
        tok_msg(k, slot, piece, sib).wait_recv()

    mine = out_ref.shape[0]

    def query_place(shape):
        lane = lax.broadcasted_iota(jnp.int32, shape, 1)
        inner = lane % (NY * mine)
        return (inner // mine) * (2 * mine) + (lane // (NY * mine)) * mine + inner % mine

    def query_order(value):
        starts = [(2 * yy + cc) * mine for cc in (0, 1) for yy in range(NY)]
        return jnp.concatenate([value[k : k + mine] for k in starts], axis=0)

    load["tok"].wait()
    send(1, tp, h0, up)
    send(3, tp, h1, dn)
    send(0, tp, whole, sib)
    send(2, tp, h1, up)
    send(4, tp, h0, dn)
    for name in LOADS[1:]:
        load[name].start()

    def chunk(source, first=False):
        wide = tok[source].astype(F32)
        square = wide * wide
        folded = square[:, 0:128]
        for k in range(1, depth // 128):
            folded = folded + square[:, k * 128 : (k + 1) * 128]
        at = pl.ds(pl.multiple_of(source * depth, depth), depth)
        low = (wide * gain[:, at]).astype(BF16)
        ig, qr, lat = mm(low, v_ig[at, :]), mm_t(low, v_qr[:, at]), mm(low, v_lat[at, :])
        if first:
            sq[...], a_ig[...], a_qr[...], a_lat[...] = folded, ig, qr, lat
        else:
            sq[...] += folded
            a_ig[...] += ig
            a_qr[...] += qr
            a_lat[...] += lat

    for name in ("gain", "w_in", "w_gate", "w_q", "w_rope", "w_lat"):
        load[name].wait()
    chunk(tp, True)
    pl.semaphore_wait(hi.at[2], 1)
    hello(hi.at[3], {"tp": dn})
    hello(hi.at[9], xs[3])
    pl.semaphore_wait(hi.at[4], 1)
    hello(hi.at[6], zdn)
    pl.semaphore_wait(hi.at[5], 1)
    hello(hi.at[7], zup)
    arrived(0, sib, whole)
    chunk(sib)
    for name in LOADS[7:]:
        load[name].wait()
    places = lax.broadcasted_iota(jnp.int32, (ROPE // 2, rows), 1) + sp * rows
    angle = places.astype(F32) * freq[...]
    cos_s[...] = jnp.cos(angle)
    sin_s[...] = jnp.sin(angle)
    angle = (query_place((ROPE // 2, rows)) + sp * rows).astype(F32) * freq[...]
    cos_q[...] = jnp.cos(angle)
    sin_q[...] = jnp.sin(angle)
    arrived(1, dn, h0)
    send(5, dn, h0, up)
    send(7, dn, h0, sib)
    arrived(3, up, h1)
    send(6, up, h1, dn)
    send(9, up, h1, sib)
    arrived(2, dn, h1)
    send(8, dn, h1, sib)
    arrived(4, up, h0)
    send(10, up, h0, sib)
    chunk(dn)
    pl.semaphore_wait(hi.at[6], 1)
    hello(hi.at[8], zdn)
    pl.semaphore_wait(hi.at[7], 1)
    chunk(up)
    arrived(7, dn_sib, h0)
    arrived(8, dn_sib, h1)
    chunk(dn_sib)
    arrived(9, up_sib, h1)
    arrived(10, up_sib, h0)
    chunk(up_sib)
    arrived(5, far, h0)
    send(11, far, h0, sib)
    arrived(6, far, h1)
    send(12, far, h1, sib)
    chunk(far)
    arrived(11, far_sib, h0)
    arrived(12, far_sib, h1)
    chunk(far_sib)

    inverse = lax.rsqrt(jnp.sum(sq[...], axis=1, keepdims=True) / model + EPS)
    rec_s[...] = (inverse * a_ig[:, 0:128]).astype(BF16)
    succ = {"sp": (sp + 1) % (NX * NZ)}
    tail = rows - 16
    pl.semaphore_wait(hi.at[0], 1)
    mine_tail = remote(rec_s.at[pl.ds(tail, 16)], halo, hsem.at[0], hsem.at[1], succ)
    go_send(mine_tail)
    latent = inverse * a_lat[...]
    spread = lax.rsqrt(jnp.mean(latent * latent, axis=1, keepdims=True) + EPS)
    latent = (latent * spread * lat_gain[...]).astype(BF16)
    expanded = mm(latent, v_exp[...]).T
    turned = (inverse * a_qr[:, NOPE:]).T
    cosine, sine = cos_s[...], sin_s[...]
    hr = ROPE // 2
    u, w = turned[ROPE : ROPE + hr], turned[ROPE + hr :]
    own_kv[0:NOPE, :] = expanded[0:NOPE].astype(BF16)
    own_kv[NOPE : NOPE + hr, :] = (u * cosine - w * sine).astype(BF16)
    own_kv[NOPE + hr : QK, :] = (w * cosine + u * sine).astype(BF16)
    own_kv[QK:, :] = expanded[NOPE:].astype(BF16)

    size = (QK + VDIM) // PIECES

    def piece_at(p):
        return pl.ds(p * size, size)

    def kv_msg(source, direction, hop, p):
        k = (direction * 4 + hop - 1) * PIECES + p
        slot = (z + (NZ - hop + 1 if direction == 0 else hop - 1)) % NZ
        return remote(
            source, kv.at[slot, piece_at(p)], kss.at[k], krs.at[k], zup if direction == 0 else zdn
        )

    def kv_goes(direction, hop, p):
        return hop < 4 or (hop == 4 and (direction == 0) == (p < PIECES // 2))

    def piece(direction, i):
        return (i + 2 * direction) % PIECES

    for i in range(PIECES):
        for direction in (0, 1):
            p = piece(direction, i)
            go_send(kv_msg(own_kv.at[piece_at(p)], direction, 1, p))

    def w_msg(weight, k):
        at = weight.at[mine_rows]
        return remote(at, at, wss.at[k], wrs.at[k], {"tp": sib})

    go_send(w_msg(w_rec, 0))
    go_send(w_msg(w_att, 1))

    def gain_msg():
        return remote(again.at[c], again.at[c], wss.at[2], wrs.at[2], {"tp": sib})

    go_send(gain_msg())

    query = query_order(inverse * a_qr[...])
    turned = query[:, NOPE:].T
    cosine, sine = cos_q[...], sin_q[...]
    u, w = turned[0:hr], turned[hr:ROPE]
    own_q[0:NOPE, :] = query[:, 0:NOPE].T.astype(BF16)
    own_q[NOPE : NOPE + hr, :] = (u * cosine - w * sine).astype(BF16)
    own_q[NOPE + hr :, :] = (w * cosine + u * sine).astype(BF16)

    def q_msg(d, slot):
        return remote(own_q, qs.at[slot], qss.at[d - 1], qrs.at[d - 1], xs[d])

    go_send(q_msg(1, x))
    go_send(q_msg(3, x))
    gate_s[...] = inverse * a_ig[:, 128:256]
    pl.semaphore_wait(hi.at[1], 1)
    pl.semaphore_wait(hi.at[8], 1)

    for xx in range(NX):
        m_s[xx] = jnp.full((1, rows), LOW, F32)
        l_s[xx] = jnp.zeros((1, rows), F32)
        o_s[xx] = jnp.zeros((VDIM, rows), F32)

    scale = math.log2(math.e) / math.sqrt(QK)

    def attend(slots, queries, keys, values, masked):
        scores = [mm(keys, query) * scale for query in queries]
        if masked:
            key = lax.broadcasted_iota(jnp.int32, scores[0].shape, 0)
            place = query_place(scores[0].shape)
            scores = [jnp.where(key <= place, s, LOW) for s in scores]
        before = [m_s[k] for k in slots]
        most = [jnp.maximum(b, jnp.max(s, axis=0, keepdims=True)) for b, s in zip(before, scores)]
        weights = [jnp.exp2(s - m) for s, m in zip(scores, most)]
        shrink = [jnp.exp2(b - m) for b, m in zip(before, most)]
        for k, m, s, wt in zip(slots, most, shrink, weights):
            m_s[k] = m
            l_s[k] = l_s[k] * s + jnp.sum(wt, axis=0, keepdims=True)
        for k, s, wt in zip(slots, shrink, weights):
            o_s[k] = o_s[k] * s + mm(values, wt.astype(BF16))

    def unit(slot):
        attend(
            range(NX), [qs[k] for k in range(NX)], kv[slot, 0:QK, :].T, kv[slot, QK:, :], False
        )

    def poll(hop, pieces):
        for i in pieces:
            for direction in (0, 1):
                p = piece(direction, i)
                if kv_goes(direction, hop, p):
                    slot = (z + (NZ - hop if direction == 0 else hop)) % NZ
                    here = kv.at[slot, piece_at(p)]
                    k = (direction * 4 + hop - 1) * PIECES + p
                    remote(here, here, kss.at[k], krs.at[k], zup).wait_recv()
                    if kv_goes(direction, hop + 1, p):
                        go_send(kv_msg(here, direction, hop + 1, p))

    first_half, second_half = (0, 1), (2, 3)

    def against(slot):
        @pl.when(slot < z)
        def _():
            unit(slot)

    def below(hop):
        against((z + NZ - hop) % NZ)

    def above(hop):
        against((z + hop) % NZ)

    order = [(y + 2) % NY, (y + 1) % NY, (y + 3) % NY, y]
    middle = model // 2
    left, right = pl.ds(0, middle), pl.ds(middle, middle)

    def rows_of(yy, cc):
        return pl.ds(pl.multiple_of((yy * 2 + cc) * mine, mine), mine)

    class Branch:
        def __init__(self, weight, k, bufs, sems):
            self.weight, self.k = weight, k
            self.natural, self.out, self.act, self.own, self.f_out, self.f_in, self.n_out, self.n_in = bufs
            self.ps, self.pr, self.fs, self.fr, self.ns, self.nr = sems

        def pair(self):
            at = self.act.at[:, mine_rows]
            return remote(self.out, at, self.ps.at[0], self.pr.at[0], {"tp": sib})

        def far(self, k):
            cols, to = ((left, up), (right, dn))[k]
            return remote(
                self.f_out.at[:, cols], self.f_in.at[:, cols], self.fs.at[k], self.fr.at[k], {"tp": to}
            )

        def near(self, k):
            side, cols = ((0, right), (1, left), (0, left), (1, right))[k]
            at = (side, slice(None), cols)
            return remote(
                self.n_out.at[at], self.n_in.at[at], self.ns.at[k], self.nr.at[k],
                {"tp": (up, dn)[side]},
            )

        def begin(self, value):
            self.natural[...] = value
            for k, yy in enumerate(order):
                at = slice(k * mine, (k + 1) * mine)
                self.out[at, :] = self.natural[rows_of(yy, 1 - c), :]
                self.act[at, mine_rows] = self.natural[rows_of(yy, c), :]
            go_send(self.pair())

        def send_far(self):
            w_msg(self.weight, self.k).wait_recv()
            self.f_out[...] = mm(self.act[0:mine, :], self.weight[...]).astype(BF16)
            go_send(self.far(0))
            go_send(self.far(1))

        def send_pure(self):
            self.own[...] = mm(self.act[mine:, :], self.weight[...])
            self.n_out[0, :, middle:] = self.own[0:mine, middle:].astype(BF16)
            go_send(self.near(0))
            self.n_out[1, :, 0:middle] = self.own[mine : 2 * mine, 0:middle].astype(BF16)
            go_send(self.near(1))

        def send_joined(self):
            self.far(0).wait_recv()
            joined = self.own[0:mine, 0:middle] + self.f_in[:, 0:middle].astype(F32)
            self.n_out[0, :, 0:middle] = joined.astype(BF16)
            go_send(self.near(2))
            self.far(1).wait_recv()
            joined = self.own[mine : 2 * mine, middle:] + self.f_in[:, middle:].astype(F32)
            self.n_out[1, :, middle:] = joined.astype(BF16)
            go_send(self.near(3))

        def total(self):
            for k in range(4):
                self.near(k).wait_recv()
            return self.own[2 * mine :, :] + self.n_in[0].astype(F32) + self.n_in[1].astype(F32)

    branch_r = Branch(w_rec, 0, r_bufs, r_sems)
    branch_t = Branch(w_att, 1, t_bufs, t_sems)

    ext[16:, :] = rec_s[...].astype(F32)
    attend((x,), [own_q[...]], own_kv[0:QK, :].T, own_kv[QK:, :], True)
    mine_tail.wait_recv()
    ext[0:16, :] = jnp.where(sp == 0, 0.0, halo[...].astype(F32))
    convolved = taps[0:1, :] * ext[13 : 13 + rows, :]
    for k in range(1, 4):
        convolved = convolved + taps[k : k + 1, :] * ext[13 + k : 13 + k + rows, :]
    conv_low = convolved.astype(BF16)
    rate = jax.nn.sigmoid(mm(conv_low, rmap[...]))
    entry = jax.nn.sigmoid(mm(conv_low, imap[...]))
    factor = jnp.broadcast_to(rf[...], (128, rows)).T
    log_keep = (-RATE_C) * factor * rate * softplus(-decay[...])
    cum = jnp.exp(log_keep)
    local = jnp.sqrt(minus_expm1(2.0 * log_keep)) * entry * convolved
    step = 1
    while step < rows:
        local = local + cum * shifted(local, step, 0.0)
        cum = cum * shifted(cum, step, 1.0)
        step *= 2
    cum_s[...] = cum
    loc_s[...] = local
    mine_x[0:1, :] = cum[rows - 1 :]
    mine_x[1:2, :] = local[rows - 1 :]

    def x_msg(d, slot):
        return remote(mine_x, cx.at[slot], xss.at[d - 1], xrs.at[d - 1], xs[d])

    for d in (2, 1, 3):
        go_send(x_msg(d, x))
    go_send(q_msg(2, x))
    poll(1, first_half)
    poll(1, second_half)

    cx[x] = mine_x[...]
    for d in range(1, NX):
        x_msg(d, (x + NX - d) % NX).wait_recv()
    pa, pb = jnp.ones((1, 128), F32), jnp.zeros((1, 128), F32)
    ta, tb = pa, pb
    for i in range(NX):
        a, b = cx[i, 0:1, :], cx[i, 1:2, :]
        ta, tb = ta * a, a * tb + b
        pa = jnp.where(i < x, pa * a, pa)
        pb = jnp.where(i < x, a * pb + b, pb)
    mine_z[0:1, :] = ta
    mine_z[1:2, :] = tb

    def z_msg(d, slot):
        to = at_zx((z + d) % NZ, x)
        return remote(mine_z, cz.at[slot], zss.at[d - 1], zrs.at[d - 1], to)

    for d in (4, 3, 5, 2, 6, 1, 7):
        go_send(z_msg(d, z))

    poll(2, first_half)
    qs[x] = own_q[...]
    for d in (1, 3, 2):
        q_msg(d, (x + NX - d) % NX).wait_recv()
    for xx in range(1, NX):

        @pl.when(x < xx)
        def _():
            attend((xx,), [qs[xx]], own_kv[0:QK, :].T, own_kv[QK:, :], False)

    poll(2, second_half)
    below(1)
    poll(3, first_half)

    cz[z] = mine_z[...]
    for d in range(1, NZ):
        z_msg(d, (z + NZ - d) % NZ).wait_recv()
    entering = jnp.zeros((1, 128), F32)
    for i in range(NZ):
        entering = jnp.where(i < z, cz[i, 0:1, :] * entering + cz[i, 1:2, :], entering)
    entering = pa * entering + pb
    state = loc_s[...] + cum_s[...] * entering
    rec = state * jax.nn.gelu(gate_s[...])
    branch_r.begin((rec * rgain[...]).astype(BF16))
    square = (rec * rec).T
    sums[...] = jnp.sum(square, axis=0, keepdims=True)

    def sum_msg(d):
        return remote(sums, got_s.at[d - 1], sss.at[d - 1], srs.at[d - 1], {"tp": (tp + d) % NT})

    pl.semaphore_wait(hi.at[3], 1)
    for d in (4, 3, 5, 2, 6, 1, 7):
        go_send(sum_msg(d))
    above(1)
    branch_r.pair().wait_recv()
    branch_r.send_far()
    branch_r.send_pure()
    below(2)
    above(2)
    poll(3, second_half)
    below(3)
    above(3)
    poll(4, first_half)
    poll(4, second_half)
    below(4)

    lanes = NY * mine

    def part_to(d, e):
        return {"sp": z * NX + (x + d) % NX, "tp": sib if e else tp}

    def o_msg(d, e):
        k = d * 2 + e
        return remote(po.at[k], go.at[k], oss.at[k], ors.at[k], part_to(d, e))

    def s_msg(d, e):
        k = d * 2 + e
        return remote(ps.at[k], gs.at[k], tss.at[k], trs.at[k], part_to(d, e))

    pl.semaphore_wait(hi.at[9], 1)
    for d, e in ((2, 0), (2, 1), (1, 0), (3, 0), (1, 1), (3, 1), (0, 1)):
        k, xx = d * 2 + e, (x + d) % NX
        at = pl.ds(pl.multiple_of((c + e - 2 * c * e) * lanes, lanes), lanes)
        total = l_s[xx, :, at]
        ps[k, 0:1, :] = m_s[xx, :, at]
        ps[k, 1:2, :] = total
        po[k] = (o_s[xx, :, at] / jnp.where(total > 0.0, total, 1.0)).astype(BF16)
        go_send(s_msg(d, e))
        go_send(o_msg(d, e))
    branch_r.send_joined()

    mine_lanes = pl.ds(pl.multiple_of(c * lanes, lanes), lanes)
    gain_msg().wait_recv()
    squares = jnp.zeros((1, lanes), F32)
    for e in (0, 1):
        if e == 0:
            most = m_s[x, :, mine_lanes]
        else:
            s_msg(0, 1).wait_recv()
            most = gs[1, 0:1, :]
        for d in range(1, NX):
            s_msg(d, e).wait_recv()
            most = jnp.maximum(most, gs[d * 2 + e, 0:1, :])
        total, out = jnp.zeros((1, lanes), F32), jnp.zeros((VDIM, lanes), F32)
        for d in range(NX):
            k = d * 2 + e
            if k == 0:
                share = jnp.exp2(m_s[x, :, mine_lanes] - most)
                total = l_s[x, :, mine_lanes] * share
                out = o_s[x, :, mine_lanes] * share
            else:
                o_msg(d, e).wait_recv()
                share = gs[k, 1:2, :] * jnp.exp2(gs[k, 0:1, :] - most)
                total = total + share
                out = out + go[k].astype(F32) * share
        out = out / total
        squares = squares + jnp.sum(out * out, axis=0, keepdims=True)
        head = c + e - 2 * c * e
        at = pl.ds(pl.multiple_of(head * 128, 128), 128)
        both[:, at] = (out.T * again[head]).astype(BF16)
    sums_t[...] = squares

    def t_msg(k):
        to = (up, dn, far)[k]
        return remote(sums_t, got_t.at[k], uss.at[k], urs.at[k], {"tp": to})

    for k in (2, 0, 1):
        go_send(t_msg(k))
    for k, yy in enumerate(order):
        at = pl.ds(pl.multiple_of(yy * mine, mine), mine)
        branch_t.act[k * mine : (k + 1) * mine, :] = both[at, :]
    branch_t.send_far()
    branch_t.send_pure()
    total = sums[...]
    for d in range(1, NT):
        sum_msg(d).wait_recv()
        total = total + got_s[d - 1]
    inv_s[...] = jnp.broadcast_to(lax.rsqrt(total / (128 * NT) + EPS), (128, rows)).T
    part[0] = branch_r.total() * inv_s[rows_of(y, c), :][:, 0:1]
    total = sums_t[...]
    for k in range(NY - 1):
        t_msg(k).wait_recv()
        total = total + got_t[k]
    inv_t[...] = jnp.broadcast_to(lax.rsqrt(total / (128 * NT) + EPS), (128, lanes)).T
    branch_t.send_joined()
    at = pl.ds(pl.multiple_of(y * mine, mine), mine)
    mixed = part[0] + branch_t.total() * inv_t[at, :][:, 0:1]
    spread = lax.rsqrt(jnp.mean(mixed * mixed, axis=1, keepdims=True) + EPS)
    out_ref[...] = (mixed * spread * post[...]).astype(BF16)
    for copy in sent:
        copy.wait_send()


def call_layer(*operands):
    rows, depth = operands[0].shape
    model = depth * NT
    mine = rows // NT
    dma = pltpu.SemaphoreType.DMA
    vm = pltpu.VMEM
    scratch = [
        vm((NT, rows, depth), BF16), vm((1, model), F32), vm((model, 256), BF16),
        vm((QK + ROPE, model), BF16), vm((model, 512), BF16), vm((512, NOPE + VDIM), BF16),
        vm((1, 512), F32), *[vm((ROPE // 2, rows), F32) for _ in range(5)],
        vm((1, rows), F32), vm((4, 128), F32), vm((128, 128), BF16), vm((128, 128), BF16),
        vm((1, 128), F32), vm((1, 128), F32), vm((2, 1, 128), F32), vm((256, model), BF16),
        vm((256, model), BF16), vm((1, model), F32),
        vm((rows, 256), F32), vm((rows, 256), F32), vm((rows, 512), F32), vm((rows, 128), F32),
        vm((QK + VDIM, rows), BF16), vm((QK, rows), BF16), vm((rows, 128), BF16),
        vm((rows, 128), F32), vm((NZ, QK + VDIM, rows), BF16), vm((NX, QK, rows), BF16),
        vm((16, 128), BF16), vm((16 + rows, 128), F32), vm((NX, 1, rows), F32),
        vm((NX, 1, rows), F32), vm((NX, VDIM, rows), F32), vm((rows, 128), F32),
        vm((rows, 128), F32),
        vm((2, 128), F32), vm((NX, 2, 128), F32), vm((2, 128), F32), vm((NZ, 2, 128), F32),
        vm((2 * NX, VDIM, NY * mine), BF16), vm((2 * NX, 2, NY * mine), F32),
        vm((2 * NX, VDIM, NY * mine), BF16), vm((2 * NX, 2, NY * mine), F32),
        vm((1, rows), F32), vm((NT - 1, 1, rows), F32), vm((rows, 128), F32),
        vm((1, NY * mine), F32), vm((NY - 1, 1, NY * mine), F32), vm((NY * mine, 128), F32),
        vm((NY * mine, 256), BF16),
        vm((1, mine, model), F32),
        dma((len(LOADS),)), pltpu.SemaphoreType.REGULAR((10,)),
        dma((13,)), dma((13,)), dma((8 * PIECES,)), dma((8 * PIECES,)),
        dma((NX - 1,)), dma((NX - 1,)), dma((2,)), dma((NX - 1,)), dma((NX - 1,)),
        dma((8,)), dma((8,)), dma((2 * NX,)), dma((2 * NX,)), dma((2 * NX,)), dma((2 * NX,)),
        dma((NT - 1,)), dma((NT - 1,)), dma((3,)), dma((3,)), dma((NY - 1,)), dma((NY - 1,)),
    ]
    for _ in range(2):
        scratch += [
            vm((rows, 128), BF16), vm((NY * mine, 128), BF16), vm((NY * mine, 256), BF16),
            vm((3 * mine, model), F32),
            vm((mine, model), BF16), vm((mine, model), BF16),
            vm((2, mine, model), BF16), vm((2, mine, model), BF16),
        ]
    for _ in range(2):
        scratch += [dma((1,)), dma((1,)), dma((2,)), dma((2,)), dma((4,)), dma((4,))]
    return pl.pallas_call(
        layer,
        name="layer",
        out_shape=pltpu.VMEM((mine, model), BF16),
        in_specs=[pl.BlockSpec(memory_space=pl.ANY)] * len(LOADS),
        out_specs=pl.BlockSpec(memory_space=pltpu.VMEM),
        scratch_shapes=scratch,
        compiler_params=pltpu.CompilerParams(
            collective_id=0, has_side_effects=True, vmem_limit_bytes=63 * 1024 * 1024
        ),
    )(*operands)


def shards(
    tokens, pre_gain, rate_factor, w_rec_in, w_rec_gate, conv_taps, rate_maps, input_maps,
    decay_param, w_query, w_latent, w_rope_key, latent_gain, w_expand, rec_gain, att_gain,
    w_out_rec, w_out_att, post_gain,
):
    rows = tokens.shape[0]
    power = np.arange(0, ROPE, 2).astype(np.float32) / np.float32(ROPE)
    frequency = np.float32(1.0) / np.float32(THETA) ** power
    frequency = np.repeat(frequency[:, None], rows, axis=1)
    given = {
        "tok": tokens, "gain": pre_gain[None], "w_in": w_rec_in, "w_gate": w_rec_gate,
        "w_q": w_query.T, "w_rope": w_rope_key.T, "w_lat": w_latent, "w_exp": w_expand,
        "lat_gain": latent_gain[None], "freq": jnp.asarray(frequency),
        "rf": rate_factor[None], "taps": conv_taps, "rmap": rate_maps[0], "imap": input_maps[0],
        "decay": decay_param[None], "rgain": rec_gain[None], "again": att_gain[None],
        "w_rec": w_out_rec, "w_att": w_out_att, "post": post_gain[None],
    }
    return call_layer(*(given[name] for name in LOADS))


def solution(mesh):
    placed = (
        P("sp", "tp"), P(), P("sp"), P(None, "tp"), P(None, "tp"), P(None, "tp"),
        P("tp", None, None), P("tp", None, None), P("tp"), P(None, "tp"), P(), P(), P(),
        P(None, "tp"), P("tp"), P("tp"), P("tp", None), P("tp", None), P(),
    )
    return jax.shard_map(
        shards, mesh=mesh, in_specs=placed, out_specs=P(("sp", "tp"), None), check_vma=False
    )
```

```python
import math

import jax
import jax.numpy as jnp
import numpy as np
from jax import lax
from jax.experimental import pallas as pl
from jax.experimental.pallas import tpu as pltpu
from jax.sharding import PartitionSpec as P

NOPE = 128
ROPE = 64
VDIM = 128
EPS = 1e-06
RATE_C = 8.0
THETA = 10000.0
NY, NX, NZ = 4, 4, 8
NT = 2 * NY
PIECES = 4
LOW = -1e30
MESH = pl.DeviceIdType.MESH
F32, BF16 = jnp.float32, jnp.bfloat16
QK = NOPE + ROPE


def remote(src, dst, send, recv, where):
    return pltpu.make_async_remote_copy(
        src_ref=src, dst_ref=dst, send_sem=send, recv_sem=recv, device_id=where, device_id_type=MESH
    )


def greet(partners):
    barrier = pltpu.get_barrier_semaphore()
    for where in partners:
        pl.semaphore_signal(barrier, inc=1, device_id=where, device_id_type=MESH)
    pl.semaphore_wait(barrier, len(partners))


def hello(sem, where):
    pl.semaphore_signal(sem, inc=1, device_id=where, device_id_type=MESH)


def mm(a, b):
    return jnp.dot(a, b, preferred_element_type=F32)


def mm_t(a, b):
    return lax.dot_general(a, b, (((1,), (1,)), ((), ())), preferred_element_type=F32)


def shifted(values, by, fill):
    row = lax.broadcasted_iota(jnp.int32, values.shape, 0)
    return jnp.where(row < by, fill, pltpu.roll(values, by, 0))


def minus_expm1(x):
    series = 1.0 + x * (1.0 / 7.0)
    for n in (6.0, 5.0, 4.0, 3.0, 2.0):
        series = 1.0 + (x * (1.0 / n)) * series
    return jnp.where(x > -0.25, -x * series, 1.0 - jnp.exp(x))


def softplus(x):
    small = jnp.exp(-jnp.abs(x))
    t = small / (2.0 + small)
    t2 = t * t
    series = 1.0 / 17.0
    for n in (15.0, 13.0, 11.0, 9.0, 7.0, 5.0, 3.0, 1.0):
        series = 1.0 / n + t2 * series
    return jnp.maximum(x, 0.0) + 2.0 * t * series


LOADS = (
    "tok", "gain", "w_in", "w_gate", "w_q", "w_rope", "w_lat", "w_exp", "lat_gain", "freq",
    "rf", "taps", "rmap", "imap", "decay", "rgain", "again", "w_rec", "w_att", "post",
)


def layer(*refs):
    n_in = len(LOADS)
    src = dict(zip(LOADS, refs[:n_in]))
    out_ref = refs[n_in]
    (
        tok, gain, v_ig, v_qr, v_lat, v_exp, lat_gain, freq, cos_s, sin_s, cos_q, sin_q, rf, taps, rmap, imap, decay,
        rgain, again, w_rec, w_att, post,
        a_ig, a_qr, a_lat, sq,
        own_kv, own_q, rec_s, gate_s, kv, qs, halo, ext, m_s, l_s, o_s, cum_s, loc_s,
        mine_x, cx, mine_z, cz, pre_x, ent_s, po, ps, go, gs,
        sums, got_s, inv_s, sums_t, got_t, inv_t, both, part,
        lsem, hi, ass, ars, kss, krs, qss, qrs, hsem, xss, xrs, zss, zrs, oss, ors, tss, trs,
        sss, srs, wss, wrs, uss, urs, *rest,
    ) = refs[n_in + 1 :]
    r_bufs, t_bufs = rest[0:8], rest[8:16]
    r_sems, t_sems = rest[16:22], rest[22:28]

    sp, tp = lax.axis_index("sp"), lax.axis_index("tp")
    z, x = sp // NX, sp % NX
    y, c = tp // 2, tp % 2

    def at_tp(yy, cc):
        return yy * 2 + cc

    sib = at_tp(y, 1 - c)
    up, dn, far = (at_tp((y + d) % NY, c) for d in (1, 3, 2))
    up_sib, dn_sib, far_sib = (at_tp((y + d) % NY, 1 - c) for d in (1, 3, 2))

    def at_zx(zz, xx):
        return {"sp": zz * NX + xx}

    zup, zdn = at_zx((z + 1) % NZ, x), at_zx((z + NZ - 1) % NZ, x)
    xs = {d: at_zx(z, (x + d) % NX) for d in range(1, NX)}

    rows, depth = tok.shape[1], tok.shape[2]
    model = depth * NT
    half = rows // 2

    mine_rows = pl.ds(pl.multiple_of(c * 128, 128), 128)
    where = {
        "tok": tok.at[tp], "gain": gain, "w_in": v_ig.at[:, pl.ds(0, 128)],
        "w_gate": v_ig.at[:, pl.ds(128, 128)], "w_q": v_qr.at[pl.ds(0, QK)],
        "w_rope": v_qr.at[pl.ds(QK, ROPE)], "w_lat": v_lat, "w_exp": v_exp, "lat_gain": lat_gain,
        "freq": freq, "rf": rf, "taps": taps, "rmap": rmap, "imap": imap,
        "decay": decay, "rgain": rgain, "again": again.at[c], "w_rec": w_rec.at[mine_rows], "w_att": w_att.at[mine_rows], "post": post,
    }
    load = {
        name: pltpu.make_async_copy(src[name], where[name], lsem.at[k])
        for k, name in enumerate(LOADS)
    }
    load["tok"].start()
    greet([{"tp": sib}, {"tp": up}, {"tp": dn}, xs[1], xs[3], zup, zdn])
    hello(hi.at[0], xs[3])
    hello(hi.at[1], {"tp": dn})
    hello(hi.at[2], {"tp": sib})
    hello(hi.at[4], zdn)
    hello(hi.at[5], zup)

    sent = []

    def go_send(copy):
        copy.start()
        sent.append(copy)

    h0, h1, whole = pl.ds(0, half), pl.ds(half, half), pl.ds(0, rows)

    def tok_msg(k, slot, piece, to):
        at = tok.at[slot, piece]
        return remote(at, at, ass.at[k], ars.at[k], {"tp": to})

    def send(k, slot, piece, to):
        go_send(tok_msg(k, slot, piece, to))

    def arrived(k, slot, piece):
        tok_msg(k, slot, piece, sib).wait_recv()

    mine = out_ref.shape[0]

    def query_place(shape):
        lane = lax.broadcasted_iota(jnp.int32, shape, 1)
        inner = lane % (NY * mine)
        return (inner // mine) * (2 * mine) + (lane // (NY * mine)) * mine + inner % mine

    def query_order(value):
        starts = [(2 * yy + cc) * mine for cc in (0, 1) for yy in range(NY)]
        return jnp.concatenate([value[k : k + mine] for k in starts], axis=0)

    load["tok"].wait()
    send(1, tp, h0, up)
    send(3, tp, h1, dn)
    send(0, tp, whole, sib)
    send(2, tp, h1, up)
    send(4, tp, h0, dn)
    for name in LOADS[1:]:
        load[name].start()

    def chunk(source, first=False):
        wide = tok[source].astype(F32)
        square = wide * wide
        folded = square[:, 0:128]
        for k in range(1, depth // 128):
            folded = folded + square[:, k * 128 : (k + 1) * 128]
        at = pl.ds(pl.multiple_of(source * depth, depth), depth)
        low = (wide * gain[:, at]).astype(BF16)
        ig, qr, lat = mm(low, v_ig[at, :]), mm_t(low, v_qr[:, at]), mm(low, v_lat[at, :])
        if first:
            sq[...], a_ig[...], a_qr[...], a_lat[...] = folded, ig, qr, lat
        else:
            sq[...] += folded
            a_ig[...] += ig
            a_qr[...] += qr
            a_lat[...] += lat

    for name in ("gain", "w_in", "w_gate", "w_q", "w_rope", "w_lat"):
        load[name].wait()
    chunk(tp, True)
    pl.semaphore_wait(hi.at[2], 1)
    hello(hi.at[3], {"tp": dn})
    hello(hi.at[9], xs[3])
    pl.semaphore_wait(hi.at[4], 1)
    hello(hi.at[6], zdn)
    pl.semaphore_wait(hi.at[5], 1)
    hello(hi.at[7], zup)
    arrived(0, sib, whole)
    chunk(sib)
    for name in LOADS[7:]:
        load[name].wait()
    places = lax.broadcasted_iota(jnp.int32, (ROPE // 2, rows), 1) + sp * rows
    angle = places.astype(F32) * freq[...]
    cos_s[...] = jnp.cos(angle)
    sin_s[...] = jnp.sin(angle)
    angle = (query_place((ROPE // 2, rows)) + sp * rows).astype(F32) * freq[...]
    cos_q[...] = jnp.cos(angle)
    sin_q[...] = jnp.sin(angle)
    arrived(1, dn, h0)
    send(5, dn, h0, up)
    send(7, dn, h0, sib)
    arrived(3, up, h1)
    send(6, up, h1, dn)
    send(9, up, h1, sib)
    arrived(2, dn, h1)
    send(8, dn, h1, sib)
    arrived(4, up, h0)
    send(10, up, h0, sib)
    chunk(dn)
    pl.semaphore_wait(hi.at[6], 1)
    hello(hi.at[8], zdn)
    pl.semaphore_wait(hi.at[7], 1)
    chunk(up)
    arrived(7, dn_sib, h0)
    arrived(8, dn_sib, h1)
    chunk(dn_sib)
    arrived(9, up_sib, h1)
    arrived(10, up_sib, h0)
    chunk(up_sib)
    arrived(5, far, h0)
    send(11, far, h0, sib)
    arrived(6, far, h1)
    send(12, far, h1, sib)
    chunk(far)
    arrived(11, far_sib, h0)
    arrived(12, far_sib, h1)
    chunk(far_sib)

    inverse = lax.rsqrt(jnp.sum(sq[...], axis=1, keepdims=True) / model + EPS)
    rec_s[...] = (inverse * a_ig[:, 0:128]).astype(BF16)
    succ = {"sp": (sp + 1) % (NX * NZ)}
    tail = rows - 16
    pl.semaphore_wait(hi.at[0], 1)
    mine_tail = remote(rec_s.at[pl.ds(tail, 16)], halo, hsem.at[0], hsem.at[1], succ)
    go_send(mine_tail)
    latent = inverse * a_lat[...]
    spread = lax.rsqrt(jnp.mean(latent * latent, axis=1, keepdims=True) + EPS)
    latent = (latent * spread * lat_gain[...]).astype(BF16)
    expanded = mm(latent, v_exp[...]).T
    turned = (inverse * a_qr[:, NOPE:]).T
    cosine, sine = cos_s[...], sin_s[...]
    hr = ROPE // 2
    u, w = turned[ROPE : ROPE + hr], turned[ROPE + hr :]
    own_kv[0:NOPE, :] = expanded[0:NOPE].astype(BF16)
    own_kv[NOPE : NOPE + hr, :] = (u * cosine - w * sine).astype(BF16)
    own_kv[NOPE + hr : QK, :] = (w * cosine + u * sine).astype(BF16)
    own_kv[QK:, :] = expanded[NOPE:].astype(BF16)

    size = (QK + VDIM) // PIECES

    def piece_at(p):
        return pl.ds(p * size, size)

    def kv_msg(source, direction, hop, p):
        k = (direction * 4 + hop - 1) * PIECES + p
        slot = (z + (NZ - hop + 1 if direction == 0 else hop - 1)) % NZ
        return remote(
            source, kv.at[slot, piece_at(p)], kss.at[k], krs.at[k], zup if direction == 0 else zdn
        )

    def kv_goes(direction, hop, p):
        return hop < 4 or (hop == 4 and (direction == 0) == (p < PIECES // 2))

    def piece(direction, i):
        return (i + 2 * direction) % PIECES

    for i in range(PIECES):
        for direction in (0, 1):
            p = piece(direction, i)
            go_send(kv_msg(own_kv.at[piece_at(p)], direction, 1, p))

    def w_msg(weight, k):
        at = weight.at[mine_rows]
        return remote(at, at, wss.at[k], wrs.at[k], {"tp": sib})

    go_send(w_msg(w_rec, 0))
    go_send(w_msg(w_att, 1))

    def gain_msg():
        return remote(again.at[c], again.at[c], wss.at[2], wrs.at[2], {"tp": sib})

    go_send(gain_msg())

    query = query_order(inverse * a_qr[...])
    turned = query[:, NOPE:].T
    cosine, sine = cos_q[...], sin_q[...]
    u, w = turned[0:hr], turned[hr:ROPE]
    own_q[0:NOPE, :] = query[:, 0:NOPE].T.astype(BF16)
    own_q[NOPE : NOPE + hr, :] = (u * cosine - w * sine).astype(BF16)
    own_q[NOPE + hr :, :] = (w * cosine + u * sine).astype(BF16)

    def q_msg(d, slot):
        return remote(own_q, qs.at[slot], qss.at[d - 1], qrs.at[d - 1], xs[d])

    go_send(q_msg(1, x))
    go_send(q_msg(3, x))
    gate_s[...] = inverse * a_ig[:, 128:256]
    pl.semaphore_wait(hi.at[1], 1)
    pl.semaphore_wait(hi.at[8], 1)

    for xx in range(NX):
        m_s[xx] = jnp.full((1, rows), LOW, F32)
        l_s[xx] = jnp.zeros((1, rows), F32)
        o_s[xx] = jnp.zeros((VDIM, rows), F32)

    scale = math.log2(math.e) / math.sqrt(QK)

    def attend(slots, queries, keys, values, masked):
        scores = [mm(keys, query) * scale for query in queries]
        if masked:
            key = lax.broadcasted_iota(jnp.int32, scores[0].shape, 0)
            place = query_place(scores[0].shape)
            scores = [jnp.where(key <= place, s, LOW) for s in scores]
        before = [m_s[k] for k in slots]
        most = [jnp.maximum(b, jnp.max(s, axis=0, keepdims=True)) for b, s in zip(before, scores)]
        weights = [jnp.exp2(s - m) for s, m in zip(scores, most)]
        shrink = [jnp.exp2(b - m) for b, m in zip(before, most)]
        for k, m, s, wt in zip(slots, most, shrink, weights):
            m_s[k] = m
            l_s[k] = l_s[k] * s + jnp.sum(wt, axis=0, keepdims=True)
        for k, s, wt in zip(slots, shrink, weights):
            o_s[k] = o_s[k] * s + mm(values, wt.astype(BF16))

    def unit(slot):
        attend(
            range(NX), [qs[k] for k in range(NX)], kv[slot, 0:QK, :].T, kv[slot, QK:, :], False
        )

    def poll(hop, pieces):
        for i in pieces:
            for direction in (0, 1):
                p = piece(direction, i)
                if kv_goes(direction, hop, p):
                    slot = (z + (NZ - hop if direction == 0 else hop)) % NZ
                    here = kv.at[slot, piece_at(p)]
                    k = (direction * 4 + hop - 1) * PIECES + p
                    remote(here, here, kss.at[k], krs.at[k], zup).wait_recv()
                    if kv_goes(direction, hop + 1, p):
                        go_send(kv_msg(here, direction, hop + 1, p))

    first_half, second_half = (0, 1), (2, 3)

    def against(slot):
        @pl.when(slot < z)
        def _():
            unit(slot)

    def below(hop):
        against((z + NZ - hop) % NZ)

    def above(hop):
        against((z + hop) % NZ)

    order = [(y + 2) % NY, (y + 1) % NY, (y + 3) % NY, y]
    middle = model // 2
    left, right = pl.ds(0, middle), pl.ds(middle, middle)

    def rows_of(yy, cc):
        return pl.ds(pl.multiple_of((yy * 2 + cc) * mine, mine), mine)

    class Branch:
        def __init__(self, weight, k, bufs, sems, go):
            self.weight, self.k, self.go = weight, k, go
            self.natural, self.out, self.act, self.own, self.f_out, self.f_in, self.n_out, self.n_in = bufs
            self.ps, self.pr, self.fs, self.fr, self.ns, self.nr = sems

        def pair(self):
            at = self.act.at[:, mine_rows]
            return remote(self.out, at, self.ps.at[0], self.pr.at[0], {"tp": sib})

        def far(self, k):
            cols, to = ((left, up), (right, dn))[k]
            return remote(
                self.f_out.at[:, cols], self.f_in.at[:, cols], self.fs.at[k], self.fr.at[k], {"tp": to}
            )

        def near(self, k):
            side, cols = ((0, right), (1, left), (0, left), (1, right))[k]
            at = (side, slice(None), cols)
            return remote(
                self.n_out.at[at], self.n_in.at[at], self.ns.at[k], self.nr.at[k],
                {"tp": (up, dn)[side]},
            )

        def begin(self, value):
            self.natural[...] = value
            for k, yy in enumerate(order):
                at = slice(k * mine, (k + 1) * mine)
                self.out[at, :] = self.natural[rows_of(yy, 1 - c), :]
                self.act[at, mine_rows] = self.natural[rows_of(yy, c), :]
            self.go(self.pair())

        def send_far(self):
            w_msg(self.weight, self.k).wait_recv()
            self.f_out[...] = mm(self.act[0:mine, :], self.weight[...]).astype(BF16)
            self.go(self.far(0))
            self.go(self.far(1))

        def send_pure(self):
            self.own[...] = mm(self.act[mine:, :], self.weight[...])
            self.n_out[0, :, middle:] = self.own[0:mine, middle:].astype(BF16)
            self.go(self.near(0))
            self.n_out[1, :, 0:middle] = self.own[mine : 2 * mine, 0:middle].astype(BF16)
            self.go(self.near(1))

        def send_joined(self):
            self.far(0).wait_recv()
            joined = self.own[0:mine, 0:middle] + self.f_in[:, 0:middle].astype(F32)
            self.n_out[0, :, 0:middle] = joined.astype(BF16)
            go_send(self.near(2))
            self.far(1).wait_recv()
            joined = self.own[mine : 2 * mine, middle:] + self.f_in[:, middle:].astype(F32)
            self.n_out[1, :, middle:] = joined.astype(BF16)
            go_send(self.near(3))

        def total(self):
            for k in range(4):
                self.near(k).wait_recv()
            return self.own[2 * mine :, :] + self.n_in[0].astype(F32) + self.n_in[1].astype(F32)

    branch_r = Branch(w_rec, 0, r_bufs, r_sems, lambda copy: copy.start())
    branch_t = Branch(w_att, 1, t_bufs, t_sems, go_send)

    ext[16:, :] = rec_s[...].astype(F32)
    attend((x,), [own_q[...]], own_kv[0:QK, :].T, own_kv[QK:, :], True)
    mine_tail.wait_recv()
    ext[0:16, :] = jnp.where(sp == 0, 0.0, halo[...].astype(F32))
    convolved = taps[0:1, :] * ext[13 : 13 + rows, :]
    for k in range(1, 4):
        convolved = convolved + taps[k : k + 1, :] * ext[13 + k : 13 + k + rows, :]
    conv_low = convolved.astype(BF16)
    rate = jax.nn.sigmoid(mm(conv_low, rmap[...]))
    entry = jax.nn.sigmoid(mm(conv_low, imap[...]))
    factor = jnp.broadcast_to(rf[...], (128, rows)).T
    log_keep = (-RATE_C) * factor * rate * softplus(-decay[...])
    cum = jnp.exp(log_keep)
    local = jnp.sqrt(minus_expm1(2.0 * log_keep)) * entry * convolved
    step = 1
    while step < rows:
        local = local + cum * shifted(local, step, 0.0)
        cum = cum * shifted(cum, step, 1.0)
        step *= 2
    cum_s[...] = cum
    loc_s[...] = local
    mine_x[0:1, :] = cum[rows - 1 :]
    mine_x[1:2, :] = local[rows - 1 :]

    def x_msg(d, slot):
        return remote(mine_x, cx.at[slot], xss.at[d - 1], xrs.at[d - 1], xs[d])

    for d in (2, 1, 3):
        go_send(x_msg(d, x))
    go_send(q_msg(2, x))
    poll(1, first_half)
    poll(1, second_half)

    cx[x] = mine_x[...]
    for d in range(1, NX):
        x_msg(d, (x + NX - d) % NX).wait_recv()
    pa, pb = jnp.ones((1, 128), F32), jnp.zeros((1, 128), F32)
    ta, tb = pa, pb
    for i in range(NX):
        a, b = cx[i, 0:1, :], cx[i, 1:2, :]
        ta, tb = ta * a, a * tb + b
        pa = jnp.where(i < x, pa * a, pa)
        pb = jnp.where(i < x, a * pb + b, pb)
    pre_x[0:1, :] = pa
    pre_x[1:2, :] = pb
    mine_z[0:1, :] = ta
    mine_z[1:2, :] = tb

    def z_msg(d, slot):
        to = at_zx((z + d) % NZ, x)
        return remote(mine_z, cz.at[slot], zss.at[d - 1], zrs.at[d - 1], to)

    for d in (4, 3, 5, 2, 6, 1, 7):
        go_send(z_msg(d, z))

    poll(2, first_half)
    qs[x] = own_q[...]
    for d in (1, 3, 2):
        q_msg(d, (x + NX - d) % NX).wait_recv()
    for xx in range(1, NX):

        @pl.when(x < xx)
        def _():
            attend((xx,), [qs[xx]], own_kv[0:QK, :].T, own_kv[QK:, :], False)

    def carried(d):
        z_msg(d, (z + NZ - d) % NZ).wait_recv()

    def whole_recurrence():
        for d in range(1, NZ):

            @pl.when(d <= z)
            def _():
                carried(d)

        ent_s[...] = jnp.zeros((1, 128), F32)
        for i in range(NZ - 1):

            @pl.when(i < z)
            def _():
                ent_s[...] = cz[i, 0:1, :] * ent_s[...] + cz[i, 1:2, :]

        entering = pre_x[0:1, :] * ent_s[...] + pre_x[1:2, :]
        state = loc_s[...] + cum_s[...] * entering
        rec = state * jax.nn.gelu(gate_s[...])
        branch_r.begin((rec * rgain[...]).astype(BF16))
        square = (rec * rec).T
        sums[...] = jnp.sum(square, axis=0, keepdims=True)

    def reduce_r():
        branch_r.pair().wait_recv()
        branch_r.send_far()
        branch_r.send_pure()

    early = z < NZ // 2
    late = z >= NZ // 2
    poll(2, second_half)
    pl.when(early)(whole_recurrence)
    below(1)
    pl.when(early)(reduce_r)
    poll(3, first_half)
    pl.when(late)(whole_recurrence)

    def sum_msg(d):
        return remote(sums, got_s.at[d - 1], sss.at[d - 1], srs.at[d - 1], {"tp": (tp + d) % NT})

    pl.semaphore_wait(hi.at[3], 1)
    for d in (4, 3, 5, 2, 6, 1, 7):
        go_send(sum_msg(d))
    above(1)
    pl.when(late)(reduce_r)
    sent.append(branch_r.pair())
    for k in (0, 1):
        sent.append(branch_r.far(k))
        sent.append(branch_r.near(k))
    below(2)
    above(2)
    poll(3, second_half)
    below(3)

    lanes = NY * mine

    def part_to(d, e):
        return {"sp": z * NX + (x + d) % NX, "tp": sib if e else tp}

    def o_msg(d, e):
        k = d * 2 + e
        return remote(po.at[k], go.at[k], oss.at[k], ors.at[k], part_to(d, e))

    def s_msg(d, e):
        k = d * 2 + e
        return remote(ps.at[k], gs.at[k], tss.at[k], trs.at[k], part_to(d, e))

    pl.semaphore_wait(hi.at[9], 1)
    others = ((2, 0), (2, 1), (1, 0), (3, 0), (1, 1), (3, 1), (0, 1))

    def send_outputs():
        for d, e in others:
            k, xx = d * 2 + e, (x + d) % NX
            at = pl.ds(pl.multiple_of((c + e - 2 * c * e) * lanes, lanes), lanes)
            total = l_s[xx, :, at]
            ps[k, 0:1, :] = m_s[xx, :, at]
            ps[k, 1:2, :] = total
            po[k] = (o_s[xx, :, at] / jnp.where(total > 0.0, total, 1.0)).astype(BF16)
            s_msg(d, e).start()
            o_msg(d, e).start()

    pl.when(early)(send_outputs)
    above(3)
    poll(4, first_half)
    poll(4, second_half)
    below(4)
    pl.when(late)(send_outputs)
    for d, e in others:
        sent.append(s_msg(d, e))
        sent.append(o_msg(d, e))
    branch_r.send_joined()

    mine_lanes = pl.ds(pl.multiple_of(c * lanes, lanes), lanes)
    gain_msg().wait_recv()
    squares = jnp.zeros((1, lanes), F32)
    for e in (0, 1):
        if e == 0:
            most = m_s[x, :, mine_lanes]
        else:
            s_msg(0, 1).wait_recv()
            most = gs[1, 0:1, :]
        for d in range(1, NX):
            s_msg(d, e).wait_recv()
            most = jnp.maximum(most, gs[d * 2 + e, 0:1, :])
        total, out = jnp.zeros((1, lanes), F32), jnp.zeros((VDIM, lanes), F32)
        for d in range(NX):
            k = d * 2 + e
            if k == 0:
                share = jnp.exp2(m_s[x, :, mine_lanes] - most)
                total = l_s[x, :, mine_lanes] * share
                out = o_s[x, :, mine_lanes] * share
            else:
                o_msg(d, e).wait_recv()
                share = gs[k, 1:2, :] * jnp.exp2(gs[k, 0:1, :] - most)
                total = total + share
                out = out + go[k].astype(F32) * share
        out = out / total
        squares = squares + jnp.sum(out * out, axis=0, keepdims=True)
        head = c + e - 2 * c * e
        at = pl.ds(pl.multiple_of(head * 128, 128), 128)
        both[:, at] = (out.T * again[head]).astype(BF16)
    sums_t[...] = squares

    def t_msg(k):
        to = (up, dn, far)[k]
        return remote(sums_t, got_t.at[k], uss.at[k], urs.at[k], {"tp": to})

    for k in (2, 0, 1):
        go_send(t_msg(k))
    for k, yy in enumerate(order):
        at = pl.ds(pl.multiple_of(yy * mine, mine), mine)
        branch_t.act[k * mine : (k + 1) * mine, :] = both[at, :]
    branch_t.send_far()
    branch_t.send_pure()
    total = sums[...]
    for d in range(1, NT):
        sum_msg(d).wait_recv()
        total = total + got_s[d - 1]
    inv_s[...] = jnp.broadcast_to(lax.rsqrt(total / (128 * NT) + EPS), (128, rows)).T
    part[0] = branch_r.total() * inv_s[rows_of(y, c), :][:, 0:1]
    total = sums_t[...]
    for k in range(NY - 1):
        t_msg(k).wait_recv()
        total = total + got_t[k]
    inv_t[...] = jnp.broadcast_to(lax.rsqrt(total / (128 * NT) + EPS), (128, lanes)).T
    branch_t.send_joined()
    at = pl.ds(pl.multiple_of(y * mine, mine), mine)
    mixed = part[0] + branch_t.total() * inv_t[at, :][:, 0:1]
    spread = lax.rsqrt(jnp.mean(mixed * mixed, axis=1, keepdims=True) + EPS)
    out_ref[...] = (mixed * spread * post[...]).astype(BF16)
    for d in range(1, NZ):

        @pl.when(d > z)
        def _():
            carried(d)

    for copy in sent:
        copy.wait_send()


def call_layer(*operands):
    rows, depth = operands[0].shape
    model = depth * NT
    mine = rows // NT
    dma = pltpu.SemaphoreType.DMA
    vm = pltpu.VMEM
    scratch = [
        vm((NT, rows, depth), BF16), vm((1, model), F32), vm((model, 256), BF16),
        vm((QK + ROPE, model), BF16), vm((model, 512), BF16), vm((512, NOPE + VDIM), BF16),
        vm((1, 512), F32), *[vm((ROPE // 2, rows), F32) for _ in range(5)],
        vm((1, rows), F32), vm((4, 128), F32), vm((128, 128), BF16), vm((128, 128), BF16),
        vm((1, 128), F32), vm((1, 128), F32), vm((2, 1, 128), F32), vm((256, model), BF16),
        vm((256, model), BF16), vm((1, model), F32),
        vm((rows, 256), F32), vm((rows, 256), F32), vm((rows, 512), F32), vm((rows, 128), F32),
        vm((QK + VDIM, rows), BF16), vm((QK, rows), BF16), vm((rows, 128), BF16),
        vm((rows, 128), F32), vm((NZ, QK + VDIM, rows), BF16), vm((NX, QK, rows), BF16),
        vm((16, 128), BF16), vm((16 + rows, 128), F32), vm((NX, 1, rows), F32),
        vm((NX, 1, rows), F32), vm((NX, VDIM, rows), F32), vm((rows, 128), F32),
        vm((rows, 128), F32),
        vm((2, 128), F32), vm((NX, 2, 128), F32), vm((2, 128), F32), vm((NZ, 2, 128), F32),
        vm((2, 128), F32), vm((1, 128), F32),
        vm((2 * NX, VDIM, NY * mine), BF16), vm((2 * NX, 2, NY * mine), F32),
        vm((2 * NX, VDIM, NY * mine), BF16), vm((2 * NX, 2, NY * mine), F32),
        vm((1, rows), F32), vm((NT - 1, 1, rows), F32), vm((rows, 128), F32),
        vm((1, NY * mine), F32), vm((NY - 1, 1, NY * mine), F32), vm((NY * mine, 128), F32),
        vm((NY * mine, 256), BF16),
        vm((1, mine, model), F32),
        dma((len(LOADS),)), pltpu.SemaphoreType.REGULAR((10,)),
        dma((13,)), dma((13,)), dma((8 * PIECES,)), dma((8 * PIECES,)),
        dma((NX - 1,)), dma((NX - 1,)), dma((2,)), dma((NX - 1,)), dma((NX - 1,)),
        dma((8,)), dma((8,)), dma((2 * NX,)), dma((2 * NX,)), dma((2 * NX,)), dma((2 * NX,)),
        dma((NT - 1,)), dma((NT - 1,)), dma((3,)), dma((3,)), dma((NY - 1,)), dma((NY - 1,)),
    ]
    for _ in range(2):
        scratch += [
            vm((rows, 128), BF16), vm((NY * mine, 128), BF16), vm((NY * mine, 256), BF16),
            vm((3 * mine, model), F32),
            vm((mine, model), BF16), vm((mine, model), BF16),
            vm((2, mine, model), BF16), vm((2, mine, model), BF16),
        ]
    for _ in range(2):
        scratch += [dma((1,)), dma((1,)), dma((2,)), dma((2,)), dma((4,)), dma((4,))]
    return pl.pallas_call(
        layer,
        name="layer",
        out_shape=pltpu.VMEM((mine, model), BF16),
        in_specs=[pl.BlockSpec(memory_space=pl.ANY)] * len(LOADS),
        out_specs=pl.BlockSpec(memory_space=pltpu.VMEM),
        scratch_shapes=scratch,
        compiler_params=pltpu.CompilerParams(
            collective_id=0, has_side_effects=True, vmem_limit_bytes=63 * 1024 * 1024
        ),
    )(*operands)


def shards(
    tokens, pre_gain, rate_factor, w_rec_in, w_rec_gate, conv_taps, rate_maps, input_maps,
    decay_param, w_query, w_latent, w_rope_key, latent_gain, w_expand, rec_gain, att_gain,
    w_out_rec, w_out_att, post_gain,
):
    rows = tokens.shape[0]
    power = np.arange(0, ROPE, 2).astype(np.float32) / np.float32(ROPE)
    frequency = np.float32(1.0) / np.float32(THETA) ** power
    frequency = np.repeat(frequency[:, None], rows, axis=1)
    given = {
        "tok": tokens, "gain": pre_gain[None], "w_in": w_rec_in, "w_gate": w_rec_gate,
        "w_q": w_query.T, "w_rope": w_rope_key.T, "w_lat": w_latent, "w_exp": w_expand,
        "lat_gain": latent_gain[None], "freq": jnp.asarray(frequency),
        "rf": rate_factor[None], "taps": conv_taps, "rmap": rate_maps[0], "imap": input_maps[0],
        "decay": decay_param[None], "rgain": rec_gain[None], "again": att_gain[None],
        "w_rec": w_out_rec, "w_att": w_out_att, "post": post_gain[None],
    }
    return call_layer(*(given[name] for name in LOADS))


def solution(mesh):
    placed = (
        P("sp", "tp"), P(), P("sp"), P(None, "tp"), P(None, "tp"), P(None, "tp"),
        P("tp", None, None), P("tp", None, None), P("tp"), P(None, "tp"), P(), P(), P(),
        P(None, "tp"), P("tp"), P("tp"), P("tp", None), P("tp", None), P(),
    )
    return jax.shard_map(
        shards, mesh=mesh, in_specs=placed, out_specs=P(("sp", "tp"), None), check_vma=False
    )
```

```python
import math

import jax
import jax.numpy as jnp
import numpy as np
from jax import lax
from jax.experimental import pallas as pl
from jax.experimental.pallas import tpu as pltpu
from jax.sharding import PartitionSpec as P

NOPE = 128
ROPE = 64
VDIM = 128
EPS = 1e-06
RATE_C = 8.0
THETA = 10000.0
NY, NX, NZ = 4, 4, 8
NT = 2 * NY
PIECES = 4
LOW = -1e30
MESH = pl.DeviceIdType.MESH
F32, BF16 = jnp.float32, jnp.bfloat16
QK = NOPE + ROPE


def remote(src, dst, send, recv, where):
    return pltpu.make_async_remote_copy(
        src_ref=src, dst_ref=dst, send_sem=send, recv_sem=recv, device_id=where, device_id_type=MESH
    )


def greet(partners):
    barrier = pltpu.get_barrier_semaphore()
    for where in partners:
        pl.semaphore_signal(barrier, inc=1, device_id=where, device_id_type=MESH)
    pl.semaphore_wait(barrier, len(partners))


def hello(sem, where):
    pl.semaphore_signal(sem, inc=1, device_id=where, device_id_type=MESH)


def mm(a, b):
    return jnp.dot(a, b, preferred_element_type=F32)


def mm_t(a, b):
    return lax.dot_general(a, b, (((1,), (1,)), ((), ())), preferred_element_type=F32)


def shifted(values, by, fill):
    row = lax.broadcasted_iota(jnp.int32, values.shape, 0)
    return jnp.where(row < by, fill, pltpu.roll(values, by, 0))


def minus_expm1(x):
    series = 1.0 + x * (1.0 / 7.0)
    for n in (6.0, 5.0, 4.0, 3.0, 2.0):
        series = 1.0 + (x * (1.0 / n)) * series
    return jnp.where(x > -0.25, -x * series, 1.0 - jnp.exp(x))


def softplus(x):
    small = jnp.exp(-jnp.abs(x))
    t = small / (2.0 + small)
    t2 = t * t
    series = 1.0 / 17.0
    for n in (15.0, 13.0, 11.0, 9.0, 7.0, 5.0, 3.0, 1.0):
        series = 1.0 / n + t2 * series
    return jnp.maximum(x, 0.0) + 2.0 * t * series


LOADS = (
    "tok", "gain", "w_in", "w_gate", "w_q", "w_rope", "w_lat", "w_exp", "lat_gain", "freq",
    "rf", "taps", "rmap", "imap", "decay", "rgain", "again", "w_rec", "w_att", "post",
)


def layer(*refs):
    n_in = len(LOADS)
    src = dict(zip(LOADS, refs[:n_in]))
    out_ref = refs[n_in]
    (
        tok, gain, v_ig, v_qr, v_lat, v_exp, lat_gain, freq, cos_s, sin_s, cos_q, sin_q, rf, taps, rmap, imap, decay,
        rgain, again, w_rec, w_att, post,
        a_ig, a_qr, a_lat, sq,
        own_kv, own_q, rec_s, gate_s, kv, qs, halo, ext, m_s, l_s, o_s, cum_s, loc_s,
        mine_x, cx, mine_z, cz, pre_x, ent_s, po, ps, go, gs,
        sums, got_s, inv_s, sums_t, got_t, inv_t, both, part,
        lsem, hi, ass, ars, kss, krs, qss, qrs, hsem, xss, xrs, zss, zrs, oss, ors, tss, trs,
        sss, srs, wss, wrs, uss, urs, *rest,
    ) = refs[n_in + 1 :]
    r_bufs, t_bufs = rest[0:8], rest[8:16]
    r_sems, t_sems = rest[16:22], rest[22:28]

    sp, tp = lax.axis_index("sp"), lax.axis_index("tp")
    z, x = sp // NX, sp % NX
    y, c = tp // 2, tp % 2

    def at_tp(yy, cc):
        return yy * 2 + cc

    sib = at_tp(y, 1 - c)
    up, dn, far = (at_tp((y + d) % NY, c) for d in (1, 3, 2))
    up_sib, dn_sib, far_sib = (at_tp((y + d) % NY, 1 - c) for d in (1, 3, 2))

    def at_zx(zz, xx):
        return {"sp": zz * NX + xx}

    zup, zdn = at_zx((z + 1) % NZ, x), at_zx((z + NZ - 1) % NZ, x)
    xs = {d: at_zx(z, (x + d) % NX) for d in range(1, NX)}

    rows, depth = tok.shape[1], tok.shape[2]
    model = depth * NT
    half = rows // 2

    mine_rows = pl.ds(pl.multiple_of(c * 128, 128), 128)
    where = {
        "tok": tok.at[tp], "gain": gain, "w_in": v_ig.at[:, pl.ds(0, 128)],
        "w_gate": v_ig.at[:, pl.ds(128, 128)], "w_q": v_qr.at[pl.ds(0, QK)],
        "w_rope": v_qr.at[pl.ds(QK, ROPE)], "w_lat": v_lat, "w_exp": v_exp, "lat_gain": lat_gain,
        "freq": freq, "rf": rf, "taps": taps, "rmap": rmap, "imap": imap,
        "decay": decay, "rgain": rgain, "again": again.at[c], "w_rec": w_rec.at[mine_rows], "w_att": w_att.at[mine_rows], "post": post,
    }
    load = {
        name: pltpu.make_async_copy(src[name], where[name], lsem.at[k])
        for k, name in enumerate(LOADS)
    }
    load["tok"].start()
    greet([{"tp": sib}, {"tp": up}, {"tp": dn}, xs[1], xs[3], zup, zdn])
    hello(hi.at[0], xs[3])
    hello(hi.at[1], {"tp": dn})
    hello(hi.at[2], {"tp": sib})
    hello(hi.at[4], zdn)
    hello(hi.at[5], zup)

    sent = []

    def go_send(copy):
        copy.start()
        sent.append(copy)

    h0, h1, whole = pl.ds(0, half), pl.ds(half, half), pl.ds(0, rows)

    def tok_msg(k, slot, piece, to):
        at = tok.at[slot, piece]
        return remote(at, at, ass.at[k], ars.at[k], {"tp": to})

    def send(k, slot, piece, to):
        go_send(tok_msg(k, slot, piece, to))

    def arrived(k, slot, piece):
        tok_msg(k, slot, piece, sib).wait_recv()

    mine = out_ref.shape[0]

    def query_place(shape):
        lane = lax.broadcasted_iota(jnp.int32, shape, 1)
        inner = lane % (NY * mine)
        return (inner // mine) * (2 * mine) + (lane // (NY * mine)) * mine + inner % mine

    def query_order(value):
        starts = [(2 * yy + cc) * mine for cc in (0, 1) for yy in range(NY)]
        return jnp.concatenate([value[k : k + mine] for k in starts], axis=0)

    load["tok"].wait()
    send(1, tp, h0, up)
    send(3, tp, h1, dn)
    send(0, tp, whole, sib)
    send(2, tp, h1, up)
    send(4, tp, h0, dn)
    for name in LOADS[1:]:
        load[name].start()

    def chunk(source, first=False):
        wide = tok[source].astype(F32)
        square = wide * wide
        folded = square[:, 0:128]
        for k in range(1, depth // 128):
            folded = folded + square[:, k * 128 : (k + 1) * 128]
        at = pl.ds(pl.multiple_of(source * depth, depth), depth)
        low = (wide * gain[:, at]).astype(BF16)
        ig, qr, lat = mm(low, v_ig[at, :]), mm_t(low, v_qr[:, at]), mm(low, v_lat[at, :])
        if first:
            sq[...], a_ig[...], a_qr[...], a_lat[...] = folded, ig, qr, lat
        else:
            sq[...] += folded
            a_ig[...] += ig
            a_qr[...] += qr
            a_lat[...] += lat

    for name in ("gain", "w_in", "w_gate", "w_q", "w_rope", "w_lat"):
        load[name].wait()
    chunk(tp, True)
    pl.semaphore_wait(hi.at[2], 1)
    hello(hi.at[3], {"tp": dn})
    hello(hi.at[9], xs[3])
    pl.semaphore_wait(hi.at[4], 1)
    hello(hi.at[6], zdn)
    pl.semaphore_wait(hi.at[5], 1)
    hello(hi.at[7], zup)
    arrived(0, sib, whole)
    chunk(sib)
    for name in LOADS[7:]:
        load[name].wait()
    places = lax.broadcasted_iota(jnp.int32, (ROPE // 2, rows), 1) + sp * rows
    angle = places.astype(F32) * freq[...]
    cos_s[...] = jnp.cos(angle)
    sin_s[...] = jnp.sin(angle)
    angle = (query_place((ROPE // 2, rows)) + sp * rows).astype(F32) * freq[...]
    cos_q[...] = jnp.cos(angle)
    sin_q[...] = jnp.sin(angle)
    arrived(1, dn, h0)
    send(5, dn, h0, up)
    send(7, dn, h0, sib)
    arrived(3, up, h1)
    send(6, up, h1, dn)
    send(9, up, h1, sib)
    arrived(2, dn, h1)
    send(8, dn, h1, sib)
    arrived(4, up, h0)
    send(10, up, h0, sib)
    chunk(dn)
    pl.semaphore_wait(hi.at[6], 1)
    hello(hi.at[8], zdn)
    pl.semaphore_wait(hi.at[7], 1)
    chunk(up)
    arrived(7, dn_sib, h0)
    arrived(8, dn_sib, h1)
    chunk(dn_sib)
    arrived(9, up_sib, h1)
    arrived(10, up_sib, h0)
    chunk(up_sib)
    arrived(5, far, h0)
    send(11, far, h0, sib)
    arrived(6, far, h1)
    send(12, far, h1, sib)
    chunk(far)
    arrived(11, far_sib, h0)
    arrived(12, far_sib, h1)
    chunk(far_sib)

    inverse = lax.rsqrt(jnp.sum(sq[...], axis=1, keepdims=True) / model + EPS)
    rec_s[...] = (inverse * a_ig[:, 0:128]).astype(BF16)
    succ = {"sp": (sp + 1) % (NX * NZ)}
    tail = rows - 16
    pl.semaphore_wait(hi.at[0], 1)
    mine_tail = remote(rec_s.at[pl.ds(tail, 16)], halo, hsem.at[0], hsem.at[1], succ)
    go_send(mine_tail)
    latent = inverse * a_lat[...]
    spread = lax.rsqrt(jnp.mean(latent * latent, axis=1, keepdims=True) + EPS)
    latent = (latent * spread * lat_gain[...]).astype(BF16)
    expanded = mm(latent, v_exp[...]).T
    turned = (inverse * a_qr[:, NOPE:]).T
    cosine, sine = cos_s[...], sin_s[...]
    hr = ROPE // 2
    u, w = turned[ROPE : ROPE + hr], turned[ROPE + hr :]
    own_kv[0:NOPE, :] = expanded[0:NOPE].astype(BF16)
    own_kv[NOPE : NOPE + hr, :] = (u * cosine - w * sine).astype(BF16)
    own_kv[NOPE + hr : QK, :] = (w * cosine + u * sine).astype(BF16)
    own_kv[QK:, :] = expanded[NOPE:].astype(BF16)

    size = (QK + VDIM) // PIECES

    def piece_at(p):
        return pl.ds(p * size, size)

    def kv_msg(source, direction, hop, p):
        k = (direction * 4 + hop - 1) * PIECES + p
        slot = (z + (NZ - hop + 1 if direction == 0 else hop - 1)) % NZ
        return remote(
            source, kv.at[slot, piece_at(p)], kss.at[k], krs.at[k], zup if direction == 0 else zdn
        )

    def kv_goes(direction, hop, p):
        return hop < 4 or (hop == 4 and (direction == 0) == (p < PIECES // 2))

    def piece(direction, i):
        return (i + 2 * direction) % PIECES

    for i in range(PIECES):
        for direction in (0, 1):
            p = piece(direction, i)
            go_send(kv_msg(own_kv.at[piece_at(p)], direction, 1, p))

    def w_msg(weight, k):
        at = weight.at[mine_rows]
        return remote(at, at, wss.at[k], wrs.at[k], {"tp": sib})

    go_send(w_msg(w_rec, 0))
    go_send(w_msg(w_att, 1))

    def gain_msg():
        return remote(again.at[c], again.at[c], wss.at[2], wrs.at[2], {"tp": sib})

    go_send(gain_msg())

    query = query_order(inverse * a_qr[...])
    turned = query[:, NOPE:].T
    cosine, sine = cos_q[...], sin_q[...]
    u, w = turned[0:hr], turned[hr:ROPE]
    own_q[0:NOPE, :] = query[:, 0:NOPE].T.astype(BF16)
    own_q[NOPE : NOPE + hr, :] = (u * cosine - w * sine).astype(BF16)
    own_q[NOPE + hr :, :] = (w * cosine + u * sine).astype(BF16)

    def q_msg(d, slot):
        return remote(own_q, qs.at[slot], qss.at[d - 1], qrs.at[d - 1], xs[d])

    go_send(q_msg(1, x))
    go_send(q_msg(3, x))
    gate_s[...] = inverse * a_ig[:, 128:256]
    pl.semaphore_wait(hi.at[1], 1)
    pl.semaphore_wait(hi.at[8], 1)

    for xx in range(NX):
        m_s[xx] = jnp.full((1, rows), LOW, F32)
        l_s[xx] = jnp.zeros((1, rows), F32)
        o_s[xx] = jnp.zeros((VDIM, rows), F32)

    scale = math.log2(math.e) / math.sqrt(QK)

    def attend(slots, queries, keys, values, masked):
        scores = [mm(keys, query) * scale for query in queries]
        if masked:
            key = lax.broadcasted_iota(jnp.int32, scores[0].shape, 0)
            place = query_place(scores[0].shape)
            scores = [jnp.where(key <= place, s, LOW) for s in scores]
        before = [m_s[k] for k in slots]
        most = [jnp.maximum(b, jnp.max(s, axis=0, keepdims=True)) for b, s in zip(before, scores)]
        weights = [jnp.exp2(s - m) for s, m in zip(scores, most)]
        shrink = [jnp.exp2(b - m) for b, m in zip(before, most)]
        for k, m, s, wt in zip(slots, most, shrink, weights):
            m_s[k] = m
            l_s[k] = l_s[k] * s + jnp.sum(wt, axis=0, keepdims=True)
        for k, s, wt in zip(slots, shrink, weights):
            o_s[k] = o_s[k] * s + mm(values, wt.astype(BF16))

    def unit(slot):
        attend(
            range(NX), [qs[k] for k in range(NX)], kv[slot, 0:QK, :].T, kv[slot, QK:, :], False
        )

    def poll(hop, pieces):
        for i in pieces:
            for direction in (0, 1):
                p = piece(direction, i)
                if kv_goes(direction, hop, p):
                    slot = (z + (NZ - hop if direction == 0 else hop)) % NZ
                    here = kv.at[slot, piece_at(p)]
                    k = (direction * 4 + hop - 1) * PIECES + p
                    remote(here, here, kss.at[k], krs.at[k], zup).wait_recv()
                    if kv_goes(direction, hop + 1, p):
                        go_send(kv_msg(here, direction, hop + 1, p))

    first_half, second_half = (0, 1), (2, 3)

    def against(slot):
        @pl.when(slot < z)
        def _():
            unit(slot)

    def below(hop):
        against((z + NZ - hop) % NZ)

    def above(hop):
        against((z + hop) % NZ)

    order = [(y + 2) % NY, (y + 1) % NY, (y + 3) % NY, y]
    middle = model // 2
    left, right = pl.ds(0, middle), pl.ds(middle, middle)

    def rows_of(yy, cc):
        return pl.ds(pl.multiple_of((yy * 2 + cc) * mine, mine), mine)

    class Branch:
        def __init__(self, weight, k, bufs, sems, go):
            self.weight, self.k, self.go = weight, k, go
            self.natural, self.out, self.act, self.own, self.f_out, self.f_in, self.n_out, self.n_in = bufs
            self.ps, self.pr, self.fs, self.fr, self.ns, self.nr = sems

        def pair(self):
            at = self.act.at[:, mine_rows]
            return remote(self.out, at, self.ps.at[0], self.pr.at[0], {"tp": sib})

        def far(self, k):
            cols, to = ((left, up), (right, dn))[k]
            return remote(
                self.f_out.at[:, cols], self.f_in.at[:, cols], self.fs.at[k], self.fr.at[k], {"tp": to}
            )

        def near(self, k):
            side, cols = ((0, right), (1, left), (0, left), (1, right))[k]
            at = (side, slice(None), cols)
            return remote(
                self.n_out.at[at], self.n_in.at[at], self.ns.at[k], self.nr.at[k],
                {"tp": (up, dn)[side]},
            )

        def begin(self, value):
            self.natural[...] = value
            for k, yy in enumerate(order):
                at = slice(k * mine, (k + 1) * mine)
                self.out[at, :] = self.natural[rows_of(yy, 1 - c), :]
                self.act[at, mine_rows] = self.natural[rows_of(yy, c), :]
            self.go(self.pair())

        def send_far(self):
            w_msg(self.weight, self.k).wait_recv()
            self.f_out[...] = mm(self.act[0:mine, :], self.weight[...]).astype(BF16)
            self.go(self.far(0))
            self.go(self.far(1))

        def send_pure(self):
            self.own[...] = mm(self.act[mine:, :], self.weight[...])
            self.n_out[0, :, middle:] = self.own[0:mine, middle:].astype(BF16)
            self.go(self.near(0))
            self.n_out[1, :, 0:middle] = self.own[mine : 2 * mine, 0:middle].astype(BF16)
            self.go(self.near(1))

        def send_joined(self):
            self.far(0).wait_recv()
            joined = self.own[0:mine, 0:middle] + self.f_in[:, 0:middle].astype(F32)
            self.n_out[0, :, 0:middle] = joined.astype(BF16)
            go_send(self.near(2))
            self.far(1).wait_recv()
            joined = self.own[mine : 2 * mine, middle:] + self.f_in[:, middle:].astype(F32)
            self.n_out[1, :, middle:] = joined.astype(BF16)
            go_send(self.near(3))

        def total(self):
            for k in range(4):
                self.near(k).wait_recv()
            return self.own[2 * mine :, :] + self.n_in[0].astype(F32) + self.n_in[1].astype(F32)

    branch_r = Branch(w_rec, 0, r_bufs, r_sems, lambda copy: copy.start())
    branch_t = Branch(w_att, 1, t_bufs, t_sems, go_send)

    ext[16:, :] = rec_s[...].astype(F32)
    attend((x,), [own_q[...]], own_kv[0:QK, :].T, own_kv[QK:, :], True)
    mine_tail.wait_recv()
    ext[0:16, :] = jnp.where(sp == 0, 0.0, halo[...].astype(F32))
    convolved = taps[0:1, :] * ext[13 : 13 + rows, :]
    for k in range(1, 4):
        convolved = convolved + taps[k : k + 1, :] * ext[13 + k : 13 + k + rows, :]
    conv_low = convolved.astype(BF16)
    rate = jax.nn.sigmoid(mm(conv_low, rmap[...]))
    entry = jax.nn.sigmoid(mm(conv_low, imap[...]))
    factor = jnp.broadcast_to(rf[...], (128, rows)).T
    log_keep = (-RATE_C) * factor * rate * softplus(-decay[...])
    cum = jnp.exp(log_keep)
    local = jnp.sqrt(minus_expm1(2.0 * log_keep)) * entry * convolved
    step = 1
    while step < rows:
        local = local + cum * shifted(local, step, 0.0)
        cum = cum * shifted(cum, step, 1.0)
        step *= 2
    cum_s[...] = cum
    loc_s[...] = local
    mine_x[0:1, :] = cum[rows - 1 :]
    mine_x[1:2, :] = local[rows - 1 :]

    def x_msg(d, slot):
        return remote(mine_x, cx.at[slot], xss.at[d - 1], xrs.at[d - 1], xs[d])

    for d in (2, 1, 3):
        go_send(x_msg(d, x))
    go_send(q_msg(2, x))
    poll(1, first_half)
    poll(1, second_half)

    cx[x] = mine_x[...]
    for d in range(1, NX):
        x_msg(d, (x + NX - d) % NX).wait_recv()
    pa, pb = jnp.ones((1, 128), F32), jnp.zeros((1, 128), F32)
    ta, tb = pa, pb
    for i in range(NX):
        a, b = cx[i, 0:1, :], cx[i, 1:2, :]
        ta, tb = ta * a, a * tb + b
        pa = jnp.where(i < x, pa * a, pa)
        pb = jnp.where(i < x, a * pb + b, pb)
    pre_x[0:1, :] = pa
    pre_x[1:2, :] = pb
    mine_z[0:1, :] = ta
    mine_z[1:2, :] = tb

    def z_msg(d, slot):
        to = at_zx((z + d) % NZ, x)
        return remote(mine_z, cz.at[slot], zss.at[d - 1], zrs.at[d - 1], to)

    for d in (4, 3, 5, 2, 6, 1, 7):
        go_send(z_msg(d, z))

    lanes = NY * mine

    def part_to(d, e):
        return {"sp": z * NX + (x + d) % NX, "tp": sib if e else tp}

    def o_msg(d, e):
        k = d * 2 + e
        return remote(po.at[k], go.at[k], oss.at[k], ors.at[k], part_to(d, e))

    def s_msg(d, e):
        k = d * 2 + e
        return remote(ps.at[k], gs.at[k], tss.at[k], trs.at[k], part_to(d, e))

    pl.semaphore_wait(hi.at[9], 1)
    others = ((2, 0), (2, 1), (1, 0), (3, 0), (1, 1), (3, 1), (0, 1))

    def send_outputs():
        for d, e in others:
            k, xx = d * 2 + e, (x + d) % NX
            at = pl.ds(pl.multiple_of((c + e - 2 * c * e) * lanes, lanes), lanes)
            total = l_s[xx, :, at]
            ps[k, 0:1, :] = m_s[xx, :, at]
            ps[k, 1:2, :] = total
            po[k] = (o_s[xx, :, at] / jnp.where(total > 0.0, total, 1.0)).astype(BF16)
            s_msg(d, e).start()
            o_msg(d, e).start()

    def carried(d):
        z_msg(d, (z + NZ - d) % NZ).wait_recv()

    def whole_recurrence():
        for d in range(1, NZ):

            @pl.when(d <= z)
            def _():
                carried(d)

        ent_s[...] = jnp.zeros((1, 128), F32)
        for i in range(NZ - 1):

            @pl.when(i < z)
            def _():
                ent_s[...] = cz[i, 0:1, :] * ent_s[...] + cz[i, 1:2, :]

        entering = pre_x[0:1, :] * ent_s[...] + pre_x[1:2, :]
        state = loc_s[...] + cum_s[...] * entering
        rec = state * jax.nn.gelu(gate_s[...])
        branch_r.begin((rec * rgain[...]).astype(BF16))
        square = (rec * rec).T
        sums[...] = jnp.sum(square, axis=0, keepdims=True)

    def reduce_r():
        branch_r.pair().wait_recv()
        branch_r.send_far()
        branch_r.send_pure()

    pl.when(z == 0)(whole_recurrence)
    poll(2, first_half)
    pl.when(z == 0)(reduce_r)
    qs[x] = own_q[...]
    for d in (1, 3, 2):
        q_msg(d, (x + NX - d) % NX).wait_recv()
    for xx in range(1, NX):

        @pl.when(x < xx)
        def _():
            attend((xx,), [qs[xx]], own_kv[0:QK, :].T, own_kv[QK:, :], False)

    early = z < NZ // 2
    late = z >= NZ // 2
    pl.when(z == 0)(send_outputs)
    below(1)
    pl.when(z == 1)(send_outputs)
    pl.when(z == 1)(whole_recurrence)
    poll(2, second_half)
    pl.when(jnp.logical_and(z >= 2, early))(whole_recurrence)
    above(1)
    pl.when(jnp.logical_and(z >= 1, early))(reduce_r)
    poll(3, first_half)
    pl.when(late)(whole_recurrence)

    def sum_msg(d):
        return remote(sums, got_s.at[d - 1], sss.at[d - 1], srs.at[d - 1], {"tp": (tp + d) % NT})

    pl.semaphore_wait(hi.at[3], 1)
    for d in (4, 3, 5, 2, 6, 1, 7):
        go_send(sum_msg(d))
    below(2)
    pl.when(z == 2)(send_outputs)
    pl.when(late)(reduce_r)
    sent.append(branch_r.pair())
    for k in (0, 1):
        sent.append(branch_r.far(k))
        sent.append(branch_r.near(k))
    above(2)
    poll(3, second_half)
    below(3)
    pl.when(z == 3)(send_outputs)
    above(3)
    poll(4, first_half)
    poll(4, second_half)
    below(4)
    pl.when(late)(send_outputs)
    for d, e in others:
        sent.append(s_msg(d, e))
        sent.append(o_msg(d, e))
    branch_r.send_joined()

    mine_lanes = pl.ds(pl.multiple_of(c * lanes, lanes), lanes)
    gain_msg().wait_recv()
    squares = jnp.zeros((1, lanes), F32)
    for e in (0, 1):
        if e == 0:
            most = m_s[x, :, mine_lanes]
        else:
            s_msg(0, 1).wait_recv()
            most = gs[1, 0:1, :]
        for d in range(1, NX):
            s_msg(d, e).wait_recv()
            most = jnp.maximum(most, gs[d * 2 + e, 0:1, :])
        total, out = jnp.zeros((1, lanes), F32), jnp.zeros((VDIM, lanes), F32)
        for d in range(NX):
            k = d * 2 + e
            if k == 0:
                share = jnp.exp2(m_s[x, :, mine_lanes] - most)
                total = l_s[x, :, mine_lanes] * share
                out = o_s[x, :, mine_lanes] * share
            else:
                o_msg(d, e).wait_recv()
                share = gs[k, 1:2, :] * jnp.exp2(gs[k, 0:1, :] - most)
                total = total + share
                out = out + go[k].astype(F32) * share
        out = out / total
        squares = squares + jnp.sum(out * out, axis=0, keepdims=True)
        head = c + e - 2 * c * e
        at = pl.ds(pl.multiple_of(head * 128, 128), 128)
        both[:, at] = (out.T * again[head]).astype(BF16)
    sums_t[...] = squares

    def t_msg(k):
        to = (up, dn, far)[k]
        return remote(sums_t, got_t.at[k], uss.at[k], urs.at[k], {"tp": to})

    for k in (2, 0, 1):
        go_send(t_msg(k))
    for k, yy in enumerate(order):
        at = pl.ds(pl.multiple_of(yy * mine, mine), mine)
        branch_t.act[k * mine : (k + 1) * mine, :] = both[at, :]
    branch_t.send_far()
    branch_t.send_pure()
    total = sums[...]
    for d in range(1, NT):
        sum_msg(d).wait_recv()
        total = total + got_s[d - 1]
    inv_s[...] = jnp.broadcast_to(lax.rsqrt(total / (128 * NT) + EPS), (128, rows)).T
    part[0] = branch_r.total() * inv_s[rows_of(y, c), :][:, 0:1]
    total = sums_t[...]
    for k in range(NY - 1):
        t_msg(k).wait_recv()
        total = total + got_t[k]
    inv_t[...] = jnp.broadcast_to(lax.rsqrt(total / (128 * NT) + EPS), (128, lanes)).T
    branch_t.send_joined()
    at = pl.ds(pl.multiple_of(y * mine, mine), mine)
    mixed = part[0] + branch_t.total() * inv_t[at, :][:, 0:1]
    spread = lax.rsqrt(jnp.mean(mixed * mixed, axis=1, keepdims=True) + EPS)
    out_ref[...] = (mixed * spread * post[...]).astype(BF16)
    for d in range(1, NZ):

        @pl.when(d > z)
        def _():
            carried(d)

    for copy in sent:
        copy.wait_send()


def call_layer(*operands):
    rows, depth = operands[0].shape
    model = depth * NT
    mine = rows // NT
    dma = pltpu.SemaphoreType.DMA
    vm = pltpu.VMEM
    scratch = [
        vm((NT, rows, depth), BF16), vm((1, model), F32), vm((model, 256), BF16),
        vm((QK + ROPE, model), BF16), vm((model, 512), BF16), vm((512, NOPE + VDIM), BF16),
        vm((1, 512), F32), *[vm((ROPE // 2, rows), F32) for _ in range(5)],
        vm((1, rows), F32), vm((4, 128), F32), vm((128, 128), BF16), vm((128, 128), BF16),
        vm((1, 128), F32), vm((1, 128), F32), vm((2, 1, 128), F32), vm((256, model), BF16),
        vm((256, model), BF16), vm((1, model), F32),
        vm((rows, 256), F32), vm((rows, 256), F32), vm((rows, 512), F32), vm((rows, 128), F32),
        vm((QK + VDIM, rows), BF16), vm((QK, rows), BF16), vm((rows, 128), BF16),
        vm((rows, 128), F32), vm((NZ, QK + VDIM, rows), BF16), vm((NX, QK, rows), BF16),
        vm((16, 128), BF16), vm((16 + rows, 128), F32), vm((NX, 1, rows), F32),
        vm((NX, 1, rows), F32), vm((NX, VDIM, rows), F32), vm((rows, 128), F32),
        vm((rows, 128), F32),
        vm((2, 128), F32), vm((NX, 2, 128), F32), vm((2, 128), F32), vm((NZ, 2, 128), F32),
        vm((2, 128), F32), vm((1, 128), F32),
        vm((2 * NX, VDIM, NY * mine), BF16), vm((2 * NX, 2, NY * mine), F32),
        vm((2 * NX, VDIM, NY * mine), BF16), vm((2 * NX, 2, NY * mine), F32),
        vm((1, rows), F32), vm((NT - 1, 1, rows), F32), vm((rows, 128), F32),
        vm((1, NY * mine), F32), vm((NY - 1, 1, NY * mine), F32), vm((NY * mine, 128), F32),
        vm((NY * mine, 256), BF16),
        vm((1, mine, model), F32),
        dma((len(LOADS),)), pltpu.SemaphoreType.REGULAR((10,)),
        dma((13,)), dma((13,)), dma((8 * PIECES,)), dma((8 * PIECES,)),
        dma((NX - 1,)), dma((NX - 1,)), dma((2,)), dma((NX - 1,)), dma((NX - 1,)),
        dma((8,)), dma((8,)), dma((2 * NX,)), dma((2 * NX,)), dma((2 * NX,)), dma((2 * NX,)),
        dma((NT - 1,)), dma((NT - 1,)), dma((3,)), dma((3,)), dma((NY - 1,)), dma((NY - 1,)),
    ]
    for _ in range(2):
        scratch += [
            vm((rows, 128), BF16), vm((NY * mine, 128), BF16), vm((NY * mine, 256), BF16),
            vm((3 * mine, model), F32),
            vm((mine, model), BF16), vm((mine, model), BF16),
            vm((2, mine, model), BF16), vm((2, mine, model), BF16),
        ]
    for _ in range(2):
        scratch += [dma((1,)), dma((1,)), dma((2,)), dma((2,)), dma((4,)), dma((4,))]
    return pl.pallas_call(
        layer,
        name="layer",
        out_shape=pltpu.VMEM((mine, model), BF16),
        in_specs=[pl.BlockSpec(memory_space=pl.ANY)] * len(LOADS),
        out_specs=pl.BlockSpec(memory_space=pltpu.VMEM),
        scratch_shapes=scratch,
        compiler_params=pltpu.CompilerParams(
            collective_id=0, has_side_effects=True, vmem_limit_bytes=63 * 1024 * 1024
        ),
    )(*operands)


def shards(
    tokens, pre_gain, rate_factor, w_rec_in, w_rec_gate, conv_taps, rate_maps, input_maps,
    decay_param, w_query, w_latent, w_rope_key, latent_gain, w_expand, rec_gain, att_gain,
    w_out_rec, w_out_att, post_gain,
):
    rows = tokens.shape[0]
    power = np.arange(0, ROPE, 2).astype(np.float32) / np.float32(ROPE)
    frequency = np.float32(1.0) / np.float32(THETA) ** power
    frequency = np.repeat(frequency[:, None], rows, axis=1)
    given = {
        "tok": tokens, "gain": pre_gain[None], "w_in": w_rec_in, "w_gate": w_rec_gate,
        "w_q": w_query.T, "w_rope": w_rope_key.T, "w_lat": w_latent, "w_exp": w_expand,
        "lat_gain": latent_gain[None], "freq": jnp.asarray(frequency),
        "rf": rate_factor[None], "taps": conv_taps, "rmap": rate_maps[0], "imap": input_maps[0],
        "decay": decay_param[None], "rgain": rec_gain[None], "again": att_gain[None],
        "w_rec": w_out_rec, "w_att": w_out_att, "post": post_gain[None],
    }
    return call_layer(*(given[name] for name in LOADS))


def solution(mesh):
    placed = (
        P("sp", "tp"), P(), P("sp"), P(None, "tp"), P(None, "tp"), P(None, "tp"),
        P("tp", None, None), P("tp", None, None), P("tp"), P(None, "tp"), P(), P(), P(),
        P(None, "tp"), P("tp"), P("tp"), P("tp", None), P("tp", None), P(),
    )
    return jax.shard_map(
        shards, mesh=mesh, in_specs=placed, out_specs=P(("sp", "tp"), None), check_vma=False
    )
```
